32 devices in a mesh: sp: 8 (over z, y), tp: 4 (over x, core).
Axes of the slice: x: 2, y: 2, z: 4, core: 2. Of those that a mesh axis runs over, the one named last changes fastest.
Arguments:
- resid_stream: bfloat16 [3072, 2048], P('sp'), may hold values from -6 to 6
- q_latent: bfloat16 [3072, 512], P('sp'), may hold values from -6 to 6
- kv_latent: bfloat16 [3072, 256], P('sp'), may hold values from -6 to 6
- rope_key: bfloat16 [3072, 64], P('sp'), may hold values from -6 to 6
- doc_ids: int32 [3072], P('sp'), may hold values from 0 to 3, as said below
- q_gain: float32 [512], replicated, may hold values from 1.5 to 64
- kv_gain: float32 [256], replicated, may hold values from 0.1 to 1.9
- w_query: bfloat16 [512, 3072], P(None, 'tp'), may hold values from -0.25 to 0.25
- w_key: bfloat16 [256, 2048], P(None, 'tp'), may hold values from -0.375 to 0.375
- w_value: bfloat16 [256, 2048], P(None, 'tp'), may hold values from -0.375 to 0.375
- w_out: bfloat16 [2048, 2048], replicated, may hold values from -0.5 to 0.5
- mix_gain: float32 [2048], replicated, may hold values from 0.1 to 1.9
- w_gate: bfloat16 [2048, 5632], P('sp', 'tp'), may hold values from -0.125 to 0.125
- w_up: bfloat16 [2048, 5632], P('sp', 'tp'), may hold values from -0.125 to 0.125
- w_down: bfloat16 [5632, 2048], P('tp', 'sp'), may hold values from -0.3125 to 0.3125
- out_gain: float32 [2048], replicated, may hold values from 0.1 to 1.9
Outputs:
- layer_out: bfloat16 [3072, 2048], P(('sp', 'tp'))
The draws below stay inside these ranges and needn't reach their ends.
Inputs may be any that keep to these rules, and one draw needn't show every extreme that they name: `doc_ids`: document numbers never fall along the sequence; every document has 1 to 2304 positions and one has exactly 2304.
All inputs are finite; a program needn't handle non-finite values.
Results may differ from the reference program's by a relative error of at most 0.02.
The reference program's roundings to bfloat16 on the way count: a program that leaves them out, or rounds other values in their place, can miss the bound.
Values may be sent and summed in bfloat16 or wider, within the bound.
A program may use at most 128 MiB of HBM per device.

```python
import math
import jax
import jax.numpy as jnp
from jax import lax

D = 2048
FF = 5632
HEADS = 16
NOPE = 128
RD = 64
VD = 128
QR = 512
KR = 256
TOK_DEV = 384
TOKENS = 3072
DOC_MOST = 2304
N_TP = 4


def draw_q_gain(key, part):
    return jnp.exp(jax.random.uniform(key, (QR,), jnp.float32, math.log(1.5), math.log(4.0)))


def draw_doc_ids(key, part):
    rest = TOKENS - DOC_MOST
    margin = max(1, rest // 6)
    key_slot = jax.random.fold_in(key, 11)
    key_first = jax.random.fold_in(key, 23)
    key_second = jax.random.fold_in(key, 37)
    big_slot = jax.random.randint(key_slot, (), 0, 4, dtype=jnp.int32)
    first_cut = jax.random.randint(key_first, (), margin, rest // 2, dtype=jnp.int32)
    second_cut = jax.random.randint(key_second, (), rest // 2 + margin, rest - margin + 1, dtype=jnp.int32)
    smaller = jnp.stack([first_cut, second_cut - first_cut, rest - second_cut]).astype(jnp.int32)
    slots = jnp.arange(4, dtype=jnp.int32)
    pick = slots - (slots > big_slot).astype(jnp.int32)
    pick = jnp.clip(pick, 0, 2)
    lengths = jnp.where(slots == big_slot, jnp.int32(DOC_MOST), jnp.take(smaller, pick))
    starts = jnp.cumsum(lengths).astype(jnp.int32)[:3]
    positions = jnp.arange(TOKENS, dtype=jnp.int32)
    return jnp.sum((positions[:, None] >= starts[None, :]).astype(jnp.int32), axis=1).astype(jnp.int32)


def shard_levels(stream_key, shape, split, low, largest):
    def one(axis_at, blocks):
        steps = jax.random.uniform(jax.random.fold_in(jax.random.fold_in(stream_key, 6), axis_at), (blocks,), jnp.float32, low / len(split), largest / len(split))
        return jnp.repeat(jnp.exp(steps), shape[axis_at] // blocks).reshape((-1,) + (1,) * (len(shape) - axis_at - 1))

    loudness = one(*split[0])
    for cut in split[1:]:
        loudness = loudness * one(*cut)
    return loudness


def normal_values(rng, dims, deviation, limit, shards=(), kind=jnp.bfloat16):
    values = jax.random.normal(rng, dims, jnp.float32) * deviation
    if len(shards) > 0:
        values = shard_levels(rng, dims, shards, -0.22, 0.18) * values
    return jnp.clip(values, min=-limit, max=limit).astype(kind)


def setup_inputs(seed: int = 0) -> dict:
    arg_keys = jax.random.split(jax.random.key(seed), 17)
    resid_stream = normal_values(arg_keys[0], (TOKENS, D), 1.0, 6.0, ((0, 8),))
    q_latent = normal_values(arg_keys[1], (TOKENS, QR), 1.0, 6.0, ((0, 8),))
    kv_latent = normal_values(arg_keys[2], (TOKENS, KR), 1.0, 6.0, ((0, 8),))
    rope_key = normal_values(arg_keys[3], (TOKENS, RD), 1.0, 6.0, ((0, 8),))
    doc_ids = draw_doc_ids(jax.random.fold_in(arg_keys[16], 71), 0)
    q_gain = draw_q_gain(jax.random.fold_in(arg_keys[16], 71), 0)
    kv_gain = jnp.clip(1.0 + 0.18 * jax.random.normal(arg_keys[6], (KR,), jnp.float32), 0.1, 1.9)
    w_query = normal_values(arg_keys[7], (QR, HEADS * (NOPE + RD)), QR ** -0.5, 0.25, ((1, 4),))
    w_key = normal_values(arg_keys[8], (KR, HEADS * NOPE), KR ** -0.5, 0.375, ((1, 4),))
    w_value = normal_values(arg_keys[9], (KR, HEADS * VD), KR ** -0.5, 0.375, ((1, 4),))
    w_out = normal_values(arg_keys[10], (HEADS * VD, D), (HEADS * VD // 16) ** -0.5, 0.5)
    mix_gain = jnp.clip(1.0 + 0.18 * jax.random.normal(arg_keys[11], (D,), jnp.float32), 0.1, 1.9)
    w_gate = normal_values(arg_keys[12], (D, FF), D ** -0.5, 0.125, ((0, 8), (1, 4)))
    w_up = normal_values(arg_keys[13], (D, FF), D ** -0.5, 0.125, ((0, 8), (1, 4)))
    w_down = normal_values(arg_keys[14], (FF, D), (FF // 16) ** -0.5, 0.3125, ((0, 4), (1, 8)))
    out_gain = jnp.clip(1.0 + 0.18 * jax.random.normal(arg_keys[15], (D,), jnp.float32), 0.1, 1.9)
    return dict(resid_stream=resid_stream, q_latent=q_latent, kv_latent=kv_latent, rope_key=rope_key, doc_ids=doc_ids, q_gain=q_gain, kv_gain=kv_gain, w_query=w_query, w_key=w_key, w_value=w_value, w_out=w_out, mix_gain=mix_gain, w_gate=w_gate, w_up=w_up, w_down=w_down, out_gain=out_gain)


eps_norm = 1e-05
rope_theta = 10000.0
resid_alpha = 8.0 ** 0.25

def rope_angles(positions):
    frequency = rope_theta ** (-jnp.arange(0, RD, 2, dtype=jnp.float32) / RD)
    angles = positions.astype(jnp.float32)[:, None] * frequency[None, :]
    return (jnp.cos(angles), jnp.sin(angles))

def rotate(values, cos_table, sin_table):
    half_width = values.shape[-1] // 2
    first_half = values[..., :half_width]
    second_half = values[..., half_width:]
    return jnp.concatenate([first_half * cos_table - second_half * sin_table, second_half * cos_table + first_half * sin_table], axis=-1)

def rms_scaled(latent, scaling):
    widened = latent.astype(jnp.float32)
    inverse = lax.rsqrt(lax.optimization_barrier(jnp.mean(widened * widened, axis=-1, keepdims=True)) + eps_norm)
    return (widened * inverse * scaling).astype(jnp.bfloat16)

def layer_scaled(stream, scaling):
    centre = stream - lax.optimization_barrier(jnp.mean(stream, axis=-1, keepdims=True))
    spread = lax.optimization_barrier(jnp.mean(centre * centre, axis=-1, keepdims=True))
    return centre * lax.rsqrt(spread + eps_norm) * scaling

def widen(packed):
    return lax.optimization_barrier(packed).astype(jnp.float32)

def reference(resid_stream, q_latent, kv_latent, rope_key, doc_ids, q_gain, kv_gain, w_query, w_key, w_value, w_out, mix_gain, w_gate, w_up, w_down, out_gain):
    positions = jnp.arange(TOKENS, dtype=jnp.int32)
    cos_table, sin_table = rope_angles(positions)
    q_normed = rms_scaled(q_latent, q_gain)
    queries = jnp.dot(q_normed, w_query, preferred_element_type=jnp.float32).reshape(TOKENS, HEADS, NOPE + RD)
    queries = jnp.concatenate([queries[:, :, :NOPE], rotate(queries[:, :, NOPE:], cos_table[:, None, :], sin_table[:, None, :])], axis=-1).astype(jnp.bfloat16)
    kv_normed = rms_scaled(kv_latent, kv_gain)
    key_nope = jnp.dot(kv_normed, w_key, preferred_element_type=jnp.float32).astype(jnp.bfloat16).reshape(TOKENS, HEADS, NOPE)
    values = jnp.dot(kv_normed, w_value, preferred_element_type=jnp.float32).astype(jnp.bfloat16).reshape(TOKENS, HEADS, VD)
    key_rot = rotate(rope_key.astype(jnp.float32), cos_table, sin_table).astype(jnp.bfloat16)
    score_scale = (NOPE + RD) ** (-0.5)
    key_wide = widen(key_nope)
    rot_wide = widen(key_rot)
    value_wide = widen(values)

    def one_block(block_index):
        first_row = (block_index * TOK_DEV).astype(jnp.int32)
        query_block = widen(lax.dynamic_slice_in_dim(queries, first_row, TOK_DEV, 0))
        doc_block = lax.dynamic_slice_in_dim(doc_ids, first_row, TOK_DEV, 0)
        scores = jnp.einsum('qhd,khd->hqk', query_block[:, :, :NOPE], key_wide)
        scores = (scores + jnp.einsum('qhd,kd->hqk', query_block[:, :, NOPE:], rot_wide)) * score_scale
        same_doc = (doc_block[:, None] == doc_ids[None, :])[None]
        masked = jnp.where(same_doc, scores, -1e+30)
        row_top = lax.optimization_barrier(jnp.max(masked, axis=-1, keepdims=True))
        weights = jnp.where(same_doc, jnp.exp(masked - row_top), 0.0)
        denom_sum = lax.optimization_barrier(jnp.sum(weights, axis=-1))
        weighted = jnp.einsum('hqk,khd->qhd', widen(weights.astype(jnp.bfloat16)), value_wide)
        return (weighted / jnp.transpose(denom_sum)[:, :, None]).astype(jnp.bfloat16)
    block_out = lax.map(one_block, jnp.arange(TOKENS // TOK_DEV, dtype=jnp.int32))
    attended = block_out.reshape(TOKENS, HEADS * VD)
    mixer_out = jnp.dot(attended, w_out, preferred_element_type=jnp.float32)
    normed_mid = layer_scaled(resid_alpha * resid_stream.astype(jnp.float32) + mixer_out, mix_gain).astype(jnp.bfloat16)
    gate_pre = jnp.dot(normed_mid, w_gate, preferred_element_type=jnp.float32)
    up_pre = jnp.dot(normed_mid, w_up, preferred_element_type=jnp.float32)
    hidden = (jax.nn.silu(gate_pre) * up_pre).astype(jnp.bfloat16)
    group_width = FF // N_TP
    ffn_sum = jnp.zeros((TOKENS, D), jnp.float32)
    for group_index in range(N_TP):
        partial_sum = jnp.dot(hidden[:, group_index * group_width:(group_index + 1) * group_width], w_down[group_index * group_width:(group_index + 1) * group_width, :], preferred_element_type=jnp.float32)
        ffn_sum = ffn_sum + widen(partial_sum.astype(jnp.bfloat16))
    layer_out = layer_scaled(resid_alpha * normed_mid.astype(jnp.float32) + 0.5 * ffn_sum, out_gain).astype(jnp.bfloat16)
    return layer_out
```

```python
import functools
import math

import jax
import jax.numpy as jnp
from jax import lax
from jax.experimental import pallas as pl
from jax.experimental.pallas import tpu as pltpu
from jax.sharding import PartitionSpec as P

NOPE = 128
RD = 64
VD = 128


eps_norm = 1e-05
rope_theta = 10000.0
resid_alpha = 8.0**0.25
key_span = 2048


def rope_angles(positions):
    frequency = rope_theta ** (-jnp.arange(0, RD, 2, dtype=jnp.float32) / RD)
    angles = positions.astype(jnp.float32)[:, None] * frequency[None, :]
    return (jnp.cos(angles), jnp.sin(angles))


def rotate(values, cos_table, sin_table):
    half_width = values.shape[-1] // 2
    first_half = values[..., :half_width]
    second_half = values[..., half_width:]
    return jnp.concatenate(
        [
            first_half * cos_table - second_half * sin_table,
            second_half * cos_table + first_half * sin_table,
        ],
        axis=-1,
    )


def rms_scaled(latent, scaling):
    widened = latent.astype(jnp.float32)
    inverse = lax.rsqrt(jnp.mean(widened * widened, axis=-1, keepdims=True) + eps_norm)
    return (widened * inverse * scaling).astype(jnp.bfloat16)


def layer_scaled(stream, scaling):
    centre = stream - jnp.mean(stream, axis=-1, keepdims=True)
    spread = jnp.mean(centre * centre, axis=-1, keepdims=True)
    return centre * lax.rsqrt(spread + eps_norm) * scaling


def fold_in_blocks(carried, piece_part, attend_fn):
    piece_rows = piece_part[0].shape[0]
    if piece_rows > key_span and piece_rows % key_span == 0:

        def one_block(inner, block_index):
            sliced = tuple(
                (
                    lax.dynamic_slice_in_dim(
                        member, (block_index * key_span).astype(jnp.int32), key_span, 0
                    )
                    for member in piece_part
                )
            )
            return (attend_fn(inner, sliced), None)

        outcome = lax.scan(one_block, carried, jnp.arange(piece_rows // key_span, dtype=jnp.int32))
        return outcome[0]
    return attend_fn(carried, piece_part)


class Ring:
    def __init__(self, blocks):
        self.count = lax.axis_size("sp")
        ring = list(range(0, self.count, 2)) + list(range(1, self.count, 2))[::-1]
        places = [ring.index(i) for i in range(self.count)]
        self.place = jnp.array(places, jnp.int32)[lax.axis_index("sp")]
        self.ring_of = jnp.array(ring, jnp.int32)
        self.right = [(ring[i], ring[(i + 1) % self.count]) for i in range(self.count)]
        self.left = [(after, before) for before, after in self.right]
        self.pieces = [[(lax.axis_index("sp"), block)] for block in blocks]
        self.flying = [(block, block) for block in blocks]
        self.step = 0

    def owner(self, distance):
        return self.ring_of[(self.place + distance) % self.count]

    def hop(self):
        self.step += 1
        self.send()

    def send(self):
        if self.step < self.count // 2:
            self.flying = [
                (lax.ppermute(one, "sp", self.right), lax.ppermute(two, "sp", self.left))
                for one, two in self.flying
            ]
        elif self.step == self.count // 2:
            self.flying = [
                (
                    lax.ppermute(one[: one.shape[0] // 2], "sp", self.right),
                    lax.ppermute(two[two.shape[0] // 2 :], "sp", self.left),
                )
                for one, two in self.flying
            ]

    def land(self, *values):
        if self.step <= self.count // 2:
            if values:
                values, self.flying = lax.optimization_barrier((values, self.flying))
            for pieces, (one, two) in zip(self.pieces, self.flying):
                if self.step < self.count // 2:
                    pieces.append((self.owner(-self.step), one))
                    pieces.append((self.owner(self.step), two))
                else:
                    pieces.append((self.owner(self.step), jnp.concatenate([one, two])))
        return values


def body(
    resid_stream,
    q_latent,
    kv_latent,
    rope_key,
    doc_ids,
    q_gain,
    kv_gain,
    w_query,
    w_key,
    w_value,
    w_out,
    mix_gain,
    w_gate,
    w_up,
    w_down,
    out_gain,
):
    tok_rows = q_latent.shape[0]
    head_count = w_key.shape[1] // NOPE
    tp_count = lax.axis_size("tp")
    part_rows = tok_rows // tp_count
    tp_index = lax.axis_index("tp")
    gate_ring = Ring([jnp.concatenate([w_gate, w_up], axis=1)])
    down_ring = Ring([w_down])
    gate_ring.hop()
    positions = lax.axis_index("sp") * tok_rows + jnp.arange(tok_rows, dtype=jnp.int32)
    cos_table, sin_table = rope_angles(positions)
    q_normed = rms_scaled(q_latent, q_gain)
    queries = jnp.dot(q_normed, w_query, preferred_element_type=jnp.float32).reshape(
        tok_rows, head_count, NOPE + RD
    )
    query_nope = queries[:, :, :NOPE].astype(jnp.bfloat16)
    query_rope = rotate(queries[:, :, NOPE:], cos_table[:, None, :], sin_table[:, None, :]).astype(
        jnp.bfloat16
    )
    kv_normed = rms_scaled(kv_latent, kv_gain)
    key_rot = rotate(rope_key.astype(jnp.float32), cos_table, sin_table).astype(jnp.bfloat16)
    score_scale = (NOPE + RD) ** (-0.5)

    def attend_rows(carried, piece_part, between=lambda value: value):
        row_top, denom_sum, accum_out = carried
        key_piece, value_piece, rot_piece, doc_piece = piece_part
        piece_rows = key_piece.shape[0]
        keys_heads = key_piece.reshape(piece_rows, head_count, NOPE)
        values_heads = value_piece.reshape(piece_rows, head_count, VD)
        scores = jnp.einsum(
            "qhd,khd->hqk", query_nope, keys_heads, preferred_element_type=jnp.float32
        )
        scores = (
            scores
            + jnp.einsum("qhd,kd->hqk", query_rope, rot_piece, preferred_element_type=jnp.float32)
        ) * score_scale
        same_doc = (doc_ids[:, None] == doc_piece[None, :])[None]
        masked = jnp.where(same_doc, scores, -1e30)
        new_top = jnp.maximum(row_top, jnp.max(masked, axis=-1))
        weights = jnp.where(same_doc, jnp.exp(masked - new_top[:, :, None]), 0.0)
        factor = jnp.exp(row_top - new_top)
        denom_sum = denom_sum * factor + jnp.sum(weights, axis=-1)
        weights = between(weights.astype(jnp.bfloat16))
        update = jnp.einsum(
            "hqk,khd->qhd", weights, values_heads, preferred_element_type=jnp.float32
        )
        accum_out = accum_out * jnp.transpose(factor)[:, :, None] + update
        return (new_top, denom_sum, accum_out)

    initial = (
        jnp.full((head_count, tok_rows), -1e30, jnp.float32),
        jnp.zeros((head_count, tok_rows), jnp.float32),
        jnp.zeros((tok_rows, head_count, VD), jnp.float32),
    )

    def project_rows(carried, piece_part, between=lambda value: value):
        latent_piece, rot_piece, doc_piece = piece_part
        key_piece = jnp.dot(latent_piece, w_key, preferred_element_type=jnp.float32).astype(
            jnp.bfloat16
        )
        value_piece = jnp.dot(latent_piece, w_value, preferred_element_type=jnp.float32).astype(
            jnp.bfloat16
        )
        return attend_rows(carried, (key_piece, value_piece, rot_piece, doc_piece), between)

    def next_hop(value):
        (value,) = gate_ring.land(value)
        gate_ring.hop()
        return value

    doc_lanes = jnp.broadcast_to(doc_ids.astype(jnp.bfloat16)[:, None], (tok_rows, RD))
    packed = jnp.concatenate([kv_normed, key_rot, doc_lanes], axis=1)
    packed_part = lax.dynamic_slice_in_dim(packed, tp_index * part_rows, part_rows, 0)
    packed_all = lax.all_gather(packed_part, ("sp", "tp"), axis=0, tiled=True)
    packed_all = next_hop(packed_all)
    kv_rank = kv_latent.shape[1]
    gathered = (
        packed_all[:, :kv_rank],
        packed_all[:, kv_rank : kv_rank + RD],
        packed_all[:, kv_rank + RD].astype(jnp.int32),
    )
    if packed_all.shape[0] > key_span and packed_all.shape[0] % key_span == 0:
        carried_out = fold_in_blocks(initial, gathered, project_rows)
    else:
        carried_out = project_rows(initial, gathered, next_hop)
    denom_sum = carried_out[1]
    attended = (
        (carried_out[2] / jnp.transpose(denom_sum)[:, :, None])
        .astype(jnp.bfloat16)
        .reshape(tok_rows, head_count * VD)
    )
    heads_rows = lax.all_to_all(attended, "tp", split_axis=0, concat_axis=1, tiled=True)
    mixer_out = jnp.dot(heads_rows, w_out, preferred_element_type=jnp.float32)
    own_resid = lax.dynamic_slice_in_dim(resid_stream, tp_index * part_rows, part_rows, 0)
    own_normed = layer_scaled(
        resid_alpha * own_resid.astype(jnp.float32) + mixer_out, mix_gain
    ).astype(jnp.bfloat16)
    (own_normed,) = gate_ring.land(own_normed)
    down_ring.hop()
    gate_ring.hop()
    normed_rows = lax.all_gather(own_normed, "tp", axis=0, tiled=True)
    (normed_rows,) = down_ring.land(normed_rows)
    down_ring.hop()
    gate_ring.land()
    while gate_ring.step < gate_ring.count // 2:
        gate_ring.hop()
        gate_ring.land()
    gate_sum = None
    for owner, piece in gate_ring.pieces[0]:
        rows = lax.dynamic_slice_in_dim(normed_rows, owner * piece.shape[0], piece.shape[0], 1)
        term = jnp.dot(rows, piece, preferred_element_type=jnp.float32)
        gate_sum = term if gate_sum is None else gate_sum + term
    width = w_gate.shape[1]
    hidden = (jax.nn.silu(gate_sum[:, :width]) * gate_sum[:, width:]).astype(jnp.bfloat16)
    (hidden,) = down_ring.land(hidden)
    while down_ring.step < down_ring.count // 2:
        down_ring.hop()
        down_ring.land()
    down = down_ring.pieces[0]
    ffn_sum = jnp.zeros((part_rows, resid_stream.shape[1]), jnp.float32)
    for part, group in enumerate((down[: len(down) // 2], down[len(down) // 2 :])):
        pieces = [piece for _, piece in group]
        if part == 0:
            pieces = [jnp.concatenate(pieces, axis=1)]
        terms = [
            jnp.dot(hidden, piece, preferred_element_type=jnp.float32).astype(jnp.bfloat16)
            for piece in pieces
        ]
        partial = jnp.concatenate(terms, axis=1)
        swapped = lax.all_to_all(
            partial.reshape(tp_count, part_rows, -1), "tp", split_axis=0, concat_axis=0, tiled=True
        )
        summed = jnp.sum(swapped.astype(jnp.float32), axis=0)
        columns = w_down.shape[1]
        for at, (owner, _) in enumerate(group):
            ffn_sum = lax.dynamic_update_slice_in_dim(
                ffn_sum, summed[:, at * columns : (at + 1) * columns], owner * columns, 1
            )
    layer_out = layer_scaled(
        resid_alpha * own_normed.astype(jnp.float32) + 0.5 * ffn_sum, out_gain
    ).astype(jnp.bfloat16)
    return layer_out


CORES = 2
LANES = 128
MESH = pl.DeviceIdType.MESH
log2_e = math.log2(math.e)


def rms_rows(latent, scaling):
    widened = latent.astype(jnp.float32)
    inverse = lax.rsqrt(jnp.mean(widened * widened, axis=-1, keepdims=True) + eps_norm)
    return (widened * inverse * scaling).astype(jnp.bfloat16)


def near_order(step, z, nz):
    paired = 2 * jnp.minimum(z, nz - 1 - z)
    half = (step + 1) // 2
    close = jnp.where(step % 2 == 1, z - half, z + half)
    far = step - paired // 2
    wide = jnp.where(z < nz - 1 - z, z + far, z - far)
    return jnp.where(step <= paired, close, wide)


def layer_kernel(
    nz,
    ny,
    heads,
    q_latent,
    kv_latent,
    rope_key,
    cos_ref,
    sin_ref,
    q_side,
    k_side,
    q_gain,
    kv_gain,
    mix_gain,
    out_gain,
    w_query,
    w_key,
    w_value,
    resid,
    w_out,
    w_gate,
    w_up,
    w_down,
    out_ref,
    packed,
    queries,
    keys,
    vals,
    scores,
    top_ref,
    den_ref,
    acc_ref,
    attended,
    head_rows,
    out_weights,
    own_resid,
    gate_w,
    up_w,
    down_w,
    rows_all,
    hidden,
    part,
    core_part,
    x_stage,
    x_part,
    z_stage,
    up_part,
    dn_part,
    loc_sem,
    kvz_s,
    kvz_r,
    kvy_s,
    kvy_r,
    kvc_s,
    kvc_r,
    wz_s,
    wz_r,
    wy_s,
    wy_r,
    tp_s,
    tp_r,
    up_s,
    dn_s,
    z_r,
    x_s,
    x_r,
    c_s,
    c_r,
    crs_s,
    crs_r,
    xrs_s,
    xrs_r,
    zch_s,
    zup_r,
    zdn_r,
):
    sp = lax.axis_index("sp")
    tp = lax.axis_index("tp")
    z, y = sp // ny, sp % ny
    x, c = tp // CORES, tp % CORES
    tok = q_latent.shape[0]
    half = tok // CORES
    quarter = out_ref.shape[0]
    tp_count = tok // quarter
    depth = w_gate.shape[0]
    wide = gate_w.shape[1]
    ff = w_gate.shape[1]
    model = out_ref.shape[1]
    total = packed.shape[0]
    rank = kv_latent.shape[1]

    def at(zz=None, yy=None, xx=None, cc=None):
        zz = z if zz is None else zz
        yy = y if yy is None else yy
        xx = x if xx is None else xx
        cc = c if cc is None else cc
        return (zz * ny + yy, xx * CORES + cc)

    def remote(src, dst, send, recv, where):
        return pltpu.make_async_remote_copy(
            src_ref=src,
            dst_ref=dst,
            send_sem=send,
            recv_sem=recv,
            device_id=where,
            device_id_type=MESH,
        )

    y_mate = at(yy=1 - y)
    x_mate = at(xx=1 - x)
    c_mate = at(cc=1 - c)
    diagonal = at(xx=1 - x, cc=1 - c)
    z_mates = [at(zz=(z + s) % nz) for s in range(1, nz)]

    def piece_start(zz):
        return pl.multiple_of(jnp.minimum(zz * wide, ff - wide), LANES)

    def weight_slots(src_sp):
        rows = pl.ds(pl.multiple_of(src_sp * depth, depth), depth)
        return (gate_w.at[rows, :], up_w.at[rows, :], down_w.at[:, rows])

    def weight_sources(zz):
        lanes = pl.ds(piece_start(zz), wide)
        rows = pl.ds(piece_start(zz), wide)
        return (w_gate.at[:, lanes], w_up.at[:, lanes], w_down.at[rows, :])

    local = [
        pltpu.make_async_copy(src, dst, loc_sem.at[i])
        for i, (src, dst) in enumerate(zip(weight_sources(z), weight_slots(sp)))
    ]
    local.append(pltpu.make_async_copy(w_out, out_weights, loc_sem.at[3]))
    local.append(
        pltpu.make_async_copy(
            resid.at[pl.ds(pl.multiple_of(tp * quarter, quarter), quarter), :],
            own_resid,
            loc_sem.at[4],
        )
    )
    for one in local:
        one.start()

    kv_normed = rms_rows(kv_latent[...], kv_gain[...])
    cos_t, sin_t = cos_ref[...], sin_ref[...]

    def turn(values):
        swapped = jnp.concatenate([values[:, RD // 2 :], values[:, : RD // 2]], axis=1)
        return values * cos_t + swapped * sin_t

    key_rot = turn(rope_key[...].astype(jnp.float32))
    tail_lanes = jnp.concatenate([key_rot, k_side[...].astype(jnp.float32)], axis=1)
    own_at = pl.multiple_of(sp * tok, tok)
    packed[pl.ds(own_at, tok), :rank] = kv_normed
    packed[pl.ds(own_at, tok), rank:] = tail_lanes.astype(jnp.bfloat16)

    barrier = pltpu.get_barrier_semaphore()
    mates = z_mates + [y_mate, x_mate, c_mate, diagonal]
    for mate in mates:
        pl.semaphore_signal(barrier, inc=1, device_id=mate, device_id_type=MESH)
    pl.semaphore_wait(barrier, len(mates))

    sends = []

    def begin(copy):
        copy.start()
        sends.append(copy)

    def half_of(src_sp, cc):
        return packed.at[pl.ds(pl.multiple_of(src_sp * tok + cc * half, half), half), :]

    own_half = half_of(sp, c)
    for s in range(1, nz):
        begin(remote(own_half, own_half, kvz_s.at[s - 1], kvz_r.at[s - 1], z_mates[s - 1]))
    begin(remote(own_half, own_half, kvy_s.at[0], kvy_r.at[0], y_mate))
    for s in range(1, nz):
        slots = weight_slots(sp)
        for m, src in enumerate(weight_sources((z + s) % nz)):
            begin(remote(src, slots[m], wz_s.at[s - 1, m], wz_r.at[s - 1, m], z_mates[s - 1]))

    q_normed = rms_rows(q_latent[...], q_gain[...])
    for h in range(heads):
        wide_q = jnp.dot(
            q_normed,
            w_query[:, h * (NOPE + RD) : (h + 1) * (NOPE + RD)],
            preferred_element_type=jnp.float32,
        )
        rest = jnp.concatenate([turn(wide_q[:, NOPE:]), q_side[...].astype(jnp.float32)], axis=1)
        queries[h, :, :NOPE] = wide_q[:, :NOPE].astype(jnp.bfloat16)
        queries[h, :, NOPE:] = rest.astype(jnp.bfloat16)

    def source(s):
        return ((z + nz - s) % nz) * ny + y

    def source_y(s):
        return ((z + nz - s) % nz) * ny + (1 - y)

    for s in range(1, nz):
        block = half_of(source(s), c)
        remote(block, block, kvz_s.at[s - 1], kvz_r.at[s - 1], z_mates[s - 1]).wait_recv()
        begin(remote(block, block, kvy_s.at[s], kvy_r.at[s], y_mate))
        begin(remote(block, block, kvc_s.at[s - 1], kvc_r.at[s - 1], c_mate))
    slots = weight_slots(sp)
    for m in range(3):
        local[m].wait()
        begin(remote(slots[m], slots[m], wy_s.at[0, m], wy_r.at[0, m], y_mate))
    for s in range(nz):
        block = half_of(source_y(s), c)
        remote(block, block, kvy_s.at[s], kvy_r.at[s], y_mate).wait_recv()
        begin(remote(block, block, kvc_s.at[nz - 1 + s], kvc_r.at[nz - 1 + s], c_mate))
    for s in range(1, nz):
        block = half_of(source(s), 1 - c)
        remote(block, block, kvc_s.at[s - 1], kvc_r.at[s - 1], c_mate).wait_recv()
    for s in range(nz):
        block = half_of(source_y(s), 1 - c)
        remote(block, block, kvc_s.at[nz - 1 + s], kvc_r.at[nz - 1 + s], c_mate).wait_recv()

    chunk = scores.shape[2]
    chunks = total // chunk
    scale = (NOPE + RD) ** (-0.5) * log2_e

    def one_head(h, carry):
        top_ref[...] = jnp.full_like(top_ref, -3.0e38)
        head_lanes = pl.ds(pl.multiple_of(h * NOPE, NOPE), NOPE)

        def score_chunk(k, inner):
            rows = pl.ds(pl.multiple_of(k * chunk, chunk), chunk)
            latent = packed[rows, :rank]
            keys[:, :NOPE] = jnp.dot(
                latent, w_key[:, head_lanes], preferred_element_type=jnp.float32
            ).astype(jnp.bfloat16)
            vals[rows, :] = jnp.dot(
                latent, w_value[:, head_lanes], preferred_element_type=jnp.float32
            ).astype(jnp.bfloat16)
            keys[:, NOPE:] = packed[rows, rank:]
            value = lax.dot_general(
                queries[h], keys[...], (((1,), (1,)), ((), ())), preferred_element_type=jnp.float32
            )
            scores[k] = value
            most = top_ref[...]
            for j in range(chunk // LANES):
                most = jnp.maximum(most, value[:, j * LANES : (j + 1) * LANES])
            top_ref[...] = most
            return inner

        lax.fori_loop(0, chunks, score_chunk, 0)
        top = jnp.max(top_ref[...], axis=1, keepdims=True)
        den_ref[...] = jnp.zeros_like(den_ref)
        acc_ref[...] = jnp.zeros_like(acc_ref)

        def weigh_chunk(k, inner):
            rows = pl.ds(pl.multiple_of(k * chunk, chunk), chunk)
            weights = jnp.exp2((scores[k] - top) * scale)
            denom = den_ref[...]
            for j in range(chunk // LANES):
                denom = denom + weights[:, j * LANES : (j + 1) * LANES]
            den_ref[...] = denom
            acc_ref[...] += jnp.dot(
                weights.astype(jnp.bfloat16), vals[rows, :], preferred_element_type=jnp.float32
            )
            return inner

        lax.fori_loop(0, chunks, weigh_chunk, 0)
        denom = jnp.sum(den_ref[...], axis=1, keepdims=True)
        attended[:, head_lanes] = (acc_ref[...] / denom).astype(jnp.bfloat16)
        return carry

    lax.fori_loop(0, heads, one_head, 0)

    def rows_of(peer):
        return attended.at[pl.ds(pl.multiple_of(peer * quarter, quarter), quarter), :]

    my_slot = head_rows.at[tp]
    tp_mates = [(1, c_mate), (2, x_mate), (3, diagonal)]
    tp_of = [x * CORES + 1 - c, (1 - x) * CORES + c, (1 - x) * CORES + 1 - c]
    for i in (2, 1, 0):
        begin(remote(rows_of(tp_of[i]), my_slot, tp_s.at[i], tp_r.at[i], tp_mates[i][1]))
    head_rows[tp] = attended[pl.ds(pl.multiple_of(tp * quarter, quarter), quarter), :]

    def pass_weights(s):
        got = weight_slots(source(s))
        for m in range(3):
            remote(got[m], got[m], wz_s.at[s - 1, m], wz_r.at[s - 1, m], z_mates[s - 1]).wait_recv()
            begin(remote(got[m], got[m], wy_s.at[s, m], wy_r.at[s, m], y_mate))

    pass_weights(1)
    local[3].wait()
    local[4].wait()
    for i in range(3):
        remote(rows_of(tp_of[i]), head_rows.at[tp_of[i]], tp_s.at[i], tp_r.at[i], tp_mates[i][1]).wait_recv()
    span = head_rows.shape[2]
    mixed = resid_alpha * own_resid[...].astype(jnp.float32)
    for t in range(tp_count):
        mixed = mixed + jnp.dot(
            head_rows[t], out_weights[t * span : (t + 1) * span, :], preferred_element_type=jnp.float32
        )
    rows_all[z, x, c] = layer_scaled(mixed, mix_gain[...]).astype(jnp.bfloat16)

    delay = 1
    first = piece_start(z)
    stale = z * wide - first

    def z_sends(zz):
        block = rows_all.at[zz, x, c]
        return (
            (jnp.logical_and(zz <= z, z < nz - 1), remote(block, block, up_s.at[zz], z_r.at[zz], at(zz=jnp.minimum(z + 1, nz - 1)))),
            (jnp.logical_and(zz >= z, z > 0), remote(block, block, dn_s.at[zz], z_r.at[zz], at(zz=jnp.maximum(z - 1, 0)))),
        )

    def x_send(zz):
        block = rows_all.at[zz, x, c]
        return remote(block, block, x_s.at[zz], x_r.at[zz], x_mate)

    def c_send(zz, xx):
        block = rows_all.at[zz, xx, c]
        return remote(block, block, c_s.at[zz, xx], c_r.at[zz, xx], c_mate)

    def arrive_x(zz):
        block = rows_all.at[zz, 1 - x, c]
        remote(block, block, x_s.at[zz], x_r.at[zz], x_mate).wait_recv()

    def arrive_c(zz, xx):
        block = rows_all.at[zz, xx, 1 - c]
        remote(block, block, c_s.at[zz, xx], c_r.at[zz, xx], c_mate).wait_recv()

    def core_send(zz, xx):
        return remote(part.at[zz, xx, 1 - c], core_part.at[zz, xx], crs_s.at[zz, xx], crs_r.at[zz, xx], c_mate)

    def x_sum_send(zz):
        return remote(x_stage.at[zz], x_part.at[zz], xrs_s.at[zz], xrs_r.at[zz], x_mate)

    def up_sum_send(zz):
        return remote(z_stage.at[zz], up_part.at[zz], zch_s.at[zz], zup_r.at[zz], at(zz=jnp.minimum(z + 1, nz - 1)))

    def dn_sum_send(zz):
        return remote(z_stage.at[zz], dn_part.at[zz], zch_s.at[zz], zdn_r.at[zz], at(zz=jnp.maximum(z - 1, 0)))

    def pair_sum(zz, xx):
        return part[zz, xx, c].astype(jnp.float32) + core_part[zz, xx].astype(jnp.float32)

    def gather_step(step):
        zz = near_order(step, z, nz)

        @pl.when(step > 0)
        def _():
            block = rows_all.at[zz, x, c]
            remote(block, block, up_s.at[zz], z_r.at[zz], x_mate).wait_recv()

        for wanted, copy in z_sends(zz):
            pl.when(wanted)(copy.start)
        x_send(zz).start()
        c_send(zz, x).start()

    def mix_step(step):
        zz = near_order(step, z, nz)
        arrive_x(zz)
        c_send(zz, 1 - x).start()
        arrive_c(zz, x)
        arrive_c(zz, 1 - x)
        rows = 2 * CORES * quarter
        lanes = lax.broadcasted_iota(jnp.int32, (1, wide), 1)
        unit = rows_all[zz].reshape(rows, model)
        gate = jnp.dot(unit, gate_w[...], preferred_element_type=jnp.float32)
        up = jnp.dot(unit, up_w[...], preferred_element_type=jnp.float32)
        inner = jax.nn.silu(gate) * up
        hidden[...] = jnp.where(lanes >= stale, inner, 0.0).astype(jnp.bfloat16)
        cut = 512
        for n in range(model // cut):
            piece = jnp.dot(
                hidden[...], down_w[:, n * cut : (n + 1) * cut], preferred_element_type=jnp.float32
            ).astype(jnp.bfloat16)
            part[zz, :, :, :, n * cut : (n + 1) * cut] = piece.reshape(2, CORES, quarter, cut)
        core_send(zz, 1 - x).start()
        core_send(zz, x).start()
        core_send(zz, 1 - x).wait_recv()
        x_stage[zz] = pair_sum(zz, 1 - x).astype(jnp.bfloat16)
        x_sum_send(zz).start()

    def ready_sum(zz):
        core_send(zz, x).wait_recv()
        x_sum_send(zz).wait_recv()
        return pair_sum(zz, x) + x_part[zz].astype(jnp.float32)

    def chain_step(step):
        above = step - z - 1

        @pl.when(jnp.logical_and(above > z, above < nz))
        def _():
            z_stage[above] = ready_sum(above).astype(jnp.bfloat16)

            @pl.when(z > 0)
            def _():
                up_sum_send(above).wait_recv()
                z_stage[above] = (
                    z_stage[above].astype(jnp.float32) + up_part[above].astype(jnp.float32)
                ).astype(jnp.bfloat16)

            up_sum_send(above).start()

        mirrored = nz - 1 - z
        below_m = step - mirrored - 1
        below = nz - 1 - below_m

        @pl.when(jnp.logical_and(below_m > mirrored, below_m < nz))
        def _():
            z_stage[below] = ready_sum(below).astype(jnp.bfloat16)

            @pl.when(mirrored > 0)
            def _():
                dn_sum_send(below).wait_recv()
                z_stage[below] = (
                    z_stage[below].astype(jnp.float32) + dn_part[below].astype(jnp.float32)
                ).astype(jnp.bfloat16)

            dn_sum_send(below).start()

    gather_step(jnp.int32(0))
    for s in range(2, nz):
        pass_weights(s)
    for s in range(nz):
        got = weight_slots(source_y(s))
        for m in range(3):
            remote(got[m], got[m], wy_s.at[s, m], wy_r.at[s, m], y_mate).wait_recv()

    def one_step(step, carry):
        pl.when(step < nz)(lambda: gather_step(step))
        pl.when(step <= nz)(lambda: mix_step(step - 1))
        chain_step(step - delay)
        return carry

    lax.fori_loop(1, 2 * nz - 1 + delay, one_step, 0)

    ffn_sum = ready_sum(z)
    pl.when(z > 0)(up_sum_send(z).wait_recv)
    pl.when(z < nz - 1)(dn_sum_send(z).wait_recv)
    part_sum = ffn_sum + jnp.where(z > 0, up_part[z].astype(jnp.float32), 0.0)
    part_sum = part_sum + jnp.where(z < nz - 1, dn_part[z].astype(jnp.float32), 0.0)
    out_ref[...] = layer_scaled(
        resid_alpha * rows_all[z, x, c].astype(jnp.float32) + 0.5 * part_sum, out_gain[...]
    ).astype(jnp.bfloat16)

    for copy in sends:
        copy.wait_send()

    def drain(zz, carry):
        for wanted, copy in z_sends(zz):
            pl.when(wanted)(copy.wait_send)
        x_send(zz).wait_send()
        for xx in range(2):
            c_send(zz, xx).wait_send()
            core_send(zz, xx).wait_send()
        x_sum_send(zz).wait_send()
        pl.when(zz > z)(up_sum_send(zz).wait_send)
        pl.when(zz < z)(dn_sum_send(zz).wait_send)
        return carry

    lax.fori_loop(0, nz, drain, 0)


def fused_layer(
    sp_count,
    tp_count,
    resid_stream,
    q_latent,
    kv_latent,
    rope_key,
    doc_ids,
    q_gain,
    kv_gain,
    w_query,
    w_key,
    w_value,
    w_out,
    mix_gain,
    w_gate,
    w_up,
    w_down,
    out_gain,
):
    ny = tp_count // CORES
    nz = sp_count // ny
    tok = q_latent.shape[0]
    total = tok * sp_count
    quarter = tok // tp_count
    model = resid_stream.shape[1]
    heads = w_key.shape[1] // NOPE
    rank = kv_latent.shape[1]
    ff = w_gate.shape[1]
    wide = -(-ff // (LANES * nz)) * LANES
    chunk = 512
    positions = lax.axis_index("sp") * tok + jnp.arange(tok, dtype=jnp.int32)
    cos_table, sin_table = rope_angles(positions)
    cos_wide = jnp.concatenate([cos_table, cos_table], axis=1)
    sin_wide = jnp.concatenate([-sin_table, sin_table], axis=1)
    marks = (doc_ids[:, None] == jnp.arange(RD, dtype=jnp.int32)[None, :])
    k_side = jnp.where(marks, 1.0, 0.0).astype(jnp.bfloat16)
    q_side = jnp.where(marks, 0.0, -1e30).astype(jnp.bfloat16)
    vmem = pl.BlockSpec(memory_space=pltpu.VMEM)
    hbm = pl.BlockSpec(memory_space=pl.ANY)
    bf16, f32 = jnp.bfloat16, jnp.float32
    dma = pltpu.SemaphoreType.DMA
    scratch = [
        pltpu.VMEM((total, rank + 2 * RD), bf16),
        pltpu.VMEM((heads, tok, NOPE + 2 * RD), bf16),
        pltpu.VMEM((chunk, NOPE + 2 * RD), bf16),
        pltpu.VMEM((total, VD), bf16),
        pltpu.VMEM((total // chunk, tok, chunk), f32),
        pltpu.VMEM((tok, LANES), f32),
        pltpu.VMEM((tok, LANES), f32),
        pltpu.VMEM((tok, VD), f32),
        pltpu.VMEM((tok, heads * VD), bf16),
        pltpu.VMEM((tp_count, quarter, heads * VD), bf16),
        pltpu.VMEM(w_out.shape, bf16),
        pltpu.VMEM((quarter, model), bf16),
        pltpu.VMEM((model, wide), bf16),
        pltpu.VMEM((model, wide), bf16),
        pltpu.VMEM((wide, model), bf16),
        pltpu.VMEM((nz, 2, CORES, quarter, model), bf16),
        pltpu.VMEM((2 * CORES * quarter, wide), bf16),
        pltpu.VMEM((nz, 2, CORES, quarter, model), bf16),
        pltpu.VMEM((nz, 2, quarter, model), bf16),
        pltpu.VMEM((nz, quarter, model), bf16),
        pltpu.VMEM((nz, quarter, model), bf16),
        pltpu.VMEM((nz, quarter, model), bf16),
        pltpu.VMEM((nz, quarter, model), bf16),
        pltpu.VMEM((nz, quarter, model), bf16),
        dma((5,)),
        dma((nz - 1,)),
        dma((nz - 1,)),
        dma((nz,)),
        dma((nz,)),
        dma((2 * nz - 1,)),
        dma((2 * nz - 1,)),
        dma((nz - 1, 3)),
        dma((nz - 1, 3)),
        dma((nz, 3)),
        dma((nz, 3)),
        dma((3,)),
        dma((3,)),
        dma((nz,)),
        dma((nz,)),
        dma((nz,)),
        dma((nz,)),
        dma((nz,)),
        dma((nz, 2)),
        dma((nz, 2)),
        dma((nz, 2)),
        dma((nz, 2)),
        dma((nz,)),
        dma((nz,)),
        dma((nz,)),
        dma((nz,)),
        dma((nz,)),
    ]
    return pl.pallas_call(
        functools.partial(layer_kernel, nz, ny, heads),
        out_shape=jax.ShapeDtypeStruct((quarter, model), bf16),
        in_specs=[vmem] * 14 + [hbm] * 5,
        out_specs=vmem,
        scratch_shapes=scratch,
        compiler_params=pltpu.CompilerParams(
            collective_id=0, has_side_effects=True, vmem_limit_bytes=67043328
        ),
    )(
        q_latent,
        kv_latent,
        rope_key,
        cos_wide,
        sin_wide,
        q_side,
        k_side,
        q_gain[None, :],
        kv_gain[None, :],
        mix_gain[None, :],
        out_gain[None, :],
        w_query,
        w_key,
        w_value,
        resid_stream,
        w_out,
        w_gate,
        w_up,
        w_down,
    )


def solution(mesh):
    in_specs = (
        P("sp", None),
        P("sp", None),
        P("sp", None),
        P("sp", None),
        P("sp"),
        P(),
        P(),
        P(None, "tp"),
        P(None, "tp"),
        P(None, "tp"),
        P(),
        P(),
        P("sp", "tp"),
        P("sp", "tp"),
        P("tp", "sp"),
        P(),
    )
    out_specs = P(("sp", "tp"), None)
    if mesh.shape["tp"] == 2 * CORES:
        return jax.shard_map(
            functools.partial(fused_layer, mesh.shape["sp"], mesh.shape["tp"]),
            mesh=mesh,
            in_specs=in_specs,
            out_specs=out_specs,
            check_vma=False,
        )
    return jax.shard_map(body, mesh=mesh, in_specs=in_specs, out_specs=out_specs, check_vma=False)
```

```python
import functools
import math

import jax
import jax.numpy as jnp
from jax import lax
from jax.experimental import pallas as pl
from jax.experimental.pallas import tpu as pltpu
from jax.sharding import PartitionSpec as P

NOPE = 128
RD = 64
VD = 128


eps_norm = 1e-05
rope_theta = 10000.0
resid_alpha = 8.0**0.25
key_span = 2048


def rope_angles(positions):
    frequency = rope_theta ** (-jnp.arange(0, RD, 2, dtype=jnp.float32) / RD)
    angles = positions.astype(jnp.float32)[:, None] * frequency[None, :]
    return (jnp.cos(angles), jnp.sin(angles))


def rotate(values, cos_table, sin_table):
    half_width = values.shape[-1] // 2
    first_half = values[..., :half_width]
    second_half = values[..., half_width:]
    return jnp.concatenate(
        [
            first_half * cos_table - second_half * sin_table,
            second_half * cos_table + first_half * sin_table,
        ],
        axis=-1,
    )


def rms_scaled(latent, scaling):
    widened = latent.astype(jnp.float32)
    inverse = lax.rsqrt(jnp.mean(widened * widened, axis=-1, keepdims=True) + eps_norm)
    return (widened * inverse * scaling).astype(jnp.bfloat16)


def layer_scaled(stream, scaling):
    centre = stream - jnp.mean(stream, axis=-1, keepdims=True)
    spread = jnp.mean(centre * centre, axis=-1, keepdims=True)
    return centre * lax.rsqrt(spread + eps_norm) * scaling


def fold_in_blocks(carried, piece_part, attend_fn):
    piece_rows = piece_part[0].shape[0]
    if piece_rows > key_span and piece_rows % key_span == 0:

        def one_block(inner, block_index):
            sliced = tuple(
                (
                    lax.dynamic_slice_in_dim(
                        member, (block_index * key_span).astype(jnp.int32), key_span, 0
                    )
                    for member in piece_part
                )
            )
            return (attend_fn(inner, sliced), None)

        outcome = lax.scan(one_block, carried, jnp.arange(piece_rows // key_span, dtype=jnp.int32))
        return outcome[0]
    return attend_fn(carried, piece_part)


class Ring:
    def __init__(self, blocks):
        self.count = lax.axis_size("sp")
        ring = list(range(0, self.count, 2)) + list(range(1, self.count, 2))[::-1]
        places = [ring.index(i) for i in range(self.count)]
        self.place = jnp.array(places, jnp.int32)[lax.axis_index("sp")]
        self.ring_of = jnp.array(ring, jnp.int32)
        self.right = [(ring[i], ring[(i + 1) % self.count]) for i in range(self.count)]
        self.left = [(after, before) for before, after in self.right]
        self.pieces = [[(lax.axis_index("sp"), block)] for block in blocks]
        self.flying = [(block, block) for block in blocks]
        self.step = 0

    def owner(self, distance):
        return self.ring_of[(self.place + distance) % self.count]

    def hop(self):
        self.step += 1
        self.send()

    def send(self):
        if self.step < self.count // 2:
            self.flying = [
                (lax.ppermute(one, "sp", self.right), lax.ppermute(two, "sp", self.left))
                for one, two in self.flying
            ]
        elif self.step == self.count // 2:
            self.flying = [
                (
                    lax.ppermute(one[: one.shape[0] // 2], "sp", self.right),
                    lax.ppermute(two[two.shape[0] // 2 :], "sp", self.left),
                )
                for one, two in self.flying
            ]

    def land(self, *values):
        if self.step <= self.count // 2:
            if values:
                values, self.flying = lax.optimization_barrier((values, self.flying))
            for pieces, (one, two) in zip(self.pieces, self.flying):
                if self.step < self.count // 2:
                    pieces.append((self.owner(-self.step), one))
                    pieces.append((self.owner(self.step), two))
                else:
                    pieces.append((self.owner(self.step), jnp.concatenate([one, two])))
        return values


def body(
    resid_stream,
    q_latent,
    kv_latent,
    rope_key,
    doc_ids,
    q_gain,
    kv_gain,
    w_query,
    w_key,
    w_value,
    w_out,
    mix_gain,
    w_gate,
    w_up,
    w_down,
    out_gain,
):
    tok_rows = q_latent.shape[0]
    head_count = w_key.shape[1] // NOPE
    tp_count = lax.axis_size("tp")
    part_rows = tok_rows // tp_count
    tp_index = lax.axis_index("tp")
    gate_ring = Ring([jnp.concatenate([w_gate, w_up], axis=1)])
    down_ring = Ring([w_down])
    gate_ring.hop()
    positions = lax.axis_index("sp") * tok_rows + jnp.arange(tok_rows, dtype=jnp.int32)
    cos_table, sin_table = rope_angles(positions)
    q_normed = rms_scaled(q_latent, q_gain)
    queries = jnp.dot(q_normed, w_query, preferred_element_type=jnp.float32).reshape(
        tok_rows, head_count, NOPE + RD
    )
    query_nope = queries[:, :, :NOPE].astype(jnp.bfloat16)
    query_rope = rotate(queries[:, :, NOPE:], cos_table[:, None, :], sin_table[:, None, :]).astype(
        jnp.bfloat16
    )
    kv_normed = rms_scaled(kv_latent, kv_gain)
    key_rot = rotate(rope_key.astype(jnp.float32), cos_table, sin_table).astype(jnp.bfloat16)
    score_scale = (NOPE + RD) ** (-0.5)

    def attend_rows(carried, piece_part, between=lambda value: value):
        row_top, denom_sum, accum_out = carried
        key_piece, value_piece, rot_piece, doc_piece = piece_part
        piece_rows = key_piece.shape[0]
        keys_heads = key_piece.reshape(piece_rows, head_count, NOPE)
        values_heads = value_piece.reshape(piece_rows, head_count, VD)
        scores = jnp.einsum(
            "qhd,khd->hqk", query_nope, keys_heads, preferred_element_type=jnp.float32
        )
        scores = (
            scores
            + jnp.einsum("qhd,kd->hqk", query_rope, rot_piece, preferred_element_type=jnp.float32)
        ) * score_scale
        same_doc = (doc_ids[:, None] == doc_piece[None, :])[None]
        masked = jnp.where(same_doc, scores, -1e30)
        new_top = jnp.maximum(row_top, jnp.max(masked, axis=-1))
        weights = jnp.where(same_doc, jnp.exp(masked - new_top[:, :, None]), 0.0)
        factor = jnp.exp(row_top - new_top)
        denom_sum = denom_sum * factor + jnp.sum(weights, axis=-1)
        weights = between(weights.astype(jnp.bfloat16))
        update = jnp.einsum(
            "hqk,khd->qhd", weights, values_heads, preferred_element_type=jnp.float32
        )
        accum_out = accum_out * jnp.transpose(factor)[:, :, None] + update
        return (new_top, denom_sum, accum_out)

    initial = (
        jnp.full((head_count, tok_rows), -1e30, jnp.float32),
        jnp.zeros((head_count, tok_rows), jnp.float32),
        jnp.zeros((tok_rows, head_count, VD), jnp.float32),
    )

    def project_rows(carried, piece_part, between=lambda value: value):
        latent_piece, rot_piece, doc_piece = piece_part
        key_piece = jnp.dot(latent_piece, w_key, preferred_element_type=jnp.float32).astype(
            jnp.bfloat16
        )
        value_piece = jnp.dot(latent_piece, w_value, preferred_element_type=jnp.float32).astype(
            jnp.bfloat16
        )
        return attend_rows(carried, (key_piece, value_piece, rot_piece, doc_piece), between)

    def next_hop(value):
        (value,) = gate_ring.land(value)
        gate_ring.hop()
        return value

    doc_lanes = jnp.broadcast_to(doc_ids.astype(jnp.bfloat16)[:, None], (tok_rows, RD))
    packed = jnp.concatenate([kv_normed, key_rot, doc_lanes], axis=1)
    packed_part = lax.dynamic_slice_in_dim(packed, tp_index * part_rows, part_rows, 0)
    packed_all = lax.all_gather(packed_part, ("sp", "tp"), axis=0, tiled=True)
    packed_all = next_hop(packed_all)
    kv_rank = kv_latent.shape[1]
    gathered = (
        packed_all[:, :kv_rank],
        packed_all[:, kv_rank : kv_rank + RD],
        packed_all[:, kv_rank + RD].astype(jnp.int32),
    )
    if packed_all.shape[0] > key_span and packed_all.shape[0] % key_span == 0:
        carried_out = fold_in_blocks(initial, gathered, project_rows)
    else:
        carried_out = project_rows(initial, gathered, next_hop)
    denom_sum = carried_out[1]
    attended = (
        (carried_out[2] / jnp.transpose(denom_sum)[:, :, None])
        .astype(jnp.bfloat16)
        .reshape(tok_rows, head_count * VD)
    )
    heads_rows = lax.all_to_all(attended, "tp", split_axis=0, concat_axis=1, tiled=True)
    mixer_out = jnp.dot(heads_rows, w_out, preferred_element_type=jnp.float32)
    own_resid = lax.dynamic_slice_in_dim(resid_stream, tp_index * part_rows, part_rows, 0)
    own_normed = layer_scaled(
        resid_alpha * own_resid.astype(jnp.float32) + mixer_out, mix_gain
    ).astype(jnp.bfloat16)
    (own_normed,) = gate_ring.land(own_normed)
    down_ring.hop()
    gate_ring.hop()
    normed_rows = lax.all_gather(own_normed, "tp", axis=0, tiled=True)
    (normed_rows,) = down_ring.land(normed_rows)
    down_ring.hop()
    gate_ring.land()
    while gate_ring.step < gate_ring.count // 2:
        gate_ring.hop()
        gate_ring.land()
    gate_sum = None
    for owner, piece in gate_ring.pieces[0]:
        rows = lax.dynamic_slice_in_dim(normed_rows, owner * piece.shape[0], piece.shape[0], 1)
        term = jnp.dot(rows, piece, preferred_element_type=jnp.float32)
        gate_sum = term if gate_sum is None else gate_sum + term
    width = w_gate.shape[1]
    hidden = (jax.nn.silu(gate_sum[:, :width]) * gate_sum[:, width:]).astype(jnp.bfloat16)
    (hidden,) = down_ring.land(hidden)
    while down_ring.step < down_ring.count // 2:
        down_ring.hop()
        down_ring.land()
    down = down_ring.pieces[0]
    ffn_sum = jnp.zeros((part_rows, resid_stream.shape[1]), jnp.float32)
    for part, group in enumerate((down[: len(down) // 2], down[len(down) // 2 :])):
        pieces = [piece for _, piece in group]
        if part == 0:
            pieces = [jnp.concatenate(pieces, axis=1)]
        terms = [
            jnp.dot(hidden, piece, preferred_element_type=jnp.float32).astype(jnp.bfloat16)
            for piece in pieces
        ]
        partial = jnp.concatenate(terms, axis=1)
        swapped = lax.all_to_all(
            partial.reshape(tp_count, part_rows, -1), "tp", split_axis=0, concat_axis=0, tiled=True
        )
        summed = jnp.sum(swapped.astype(jnp.float32), axis=0)
        columns = w_down.shape[1]
        for at, (owner, _) in enumerate(group):
            ffn_sum = lax.dynamic_update_slice_in_dim(
                ffn_sum, summed[:, at * columns : (at + 1) * columns], owner * columns, 1
            )
    layer_out = layer_scaled(
        resid_alpha * own_normed.astype(jnp.float32) + 0.5 * ffn_sum, out_gain
    ).astype(jnp.bfloat16)
    return layer_out


CORES = 2
LANES = 128
MESH = pl.DeviceIdType.MESH
log2_e = math.log2(math.e)


def rms_rows(latent, scaling):
    widened = latent.astype(jnp.float32)
    inverse = lax.rsqrt(jnp.mean(widened * widened, axis=-1, keepdims=True) + eps_norm)
    return (widened * inverse * scaling).astype(jnp.bfloat16)


def near_order(step, z, nz):
    paired = 2 * jnp.minimum(z, nz - 1 - z)
    half = (step + 1) // 2
    close = jnp.where(step % 2 == 1, z - half, z + half)
    far = step - paired // 2
    wide = jnp.where(z < nz - 1 - z, z + far, z - far)
    return jnp.where(step <= paired, close, wide)


def layer_kernel(
    nz,
    ny,
    heads,
    q_latent,
    kv_latent,
    side_ref,
    cos_ref,
    sin_ref,
    q_gain,
    kv_gain,
    mix_gain,
    out_gain,
    w_query,
    w_key,
    w_value,
    resid,
    w_out,
    w_gate,
    w_up,
    w_down,
    out_ref,
    packed,
    queries,
    vals,
    scores,
    top_ref,
    den_ref,
    acc_ref,
    attended,
    head_rows,
    out_weights,
    own_resid,
    gate_w,
    up_w,
    down_w,
    rows_all,
    hidden,
    part,
    core_part,
    x_stage,
    x_part,
    z_stage,
    up_part,
    dn_part,
    loc_sem,
    kvz_s,
    kvz_r,
    kvy_s,
    kvy_r,
    kvc_s,
    kvc_r,
    wz_s,
    wz_r,
    wy_s,
    wy_r,
    tp_s,
    tp_r,
    up_s,
    dn_s,
    z_r,
    x_s,
    x_r,
    c_s,
    c_r,
    crs_s,
    crs_r,
    xrs_s,
    xrs_r,
    zch_s,
    zup_r,
    zdn_r,
):
    sp = lax.axis_index("sp")
    tp = lax.axis_index("tp")
    z, y = sp // ny, sp % ny
    x, c = tp // CORES, tp % CORES
    tok = q_latent.shape[0]
    half = tok // CORES
    quarter = out_ref.shape[0]
    tp_count = tok // quarter
    depth = w_gate.shape[0]
    wide = gate_w.shape[1]
    ff = w_gate.shape[1]
    model = out_ref.shape[1]
    total = packed.shape[0]
    rank = kv_latent.shape[1]

    def at(zz=None, yy=None, xx=None, cc=None):
        zz = z if zz is None else zz
        yy = y if yy is None else yy
        xx = x if xx is None else xx
        cc = c if cc is None else cc
        return (zz * ny + yy, xx * CORES + cc)

    def remote(src, dst, send, recv, where):
        return pltpu.make_async_remote_copy(
            src_ref=src,
            dst_ref=dst,
            send_sem=send,
            recv_sem=recv,
            device_id=where,
            device_id_type=MESH,
        )

    y_mate = at(yy=1 - y)
    x_mate = at(xx=1 - x)
    c_mate = at(cc=1 - c)
    diagonal = at(xx=1 - x, cc=1 - c)
    z_mates = [at(zz=(z + s) % nz) for s in range(1, nz)]

    def piece_start(zz):
        return pl.multiple_of(jnp.minimum(zz * wide, ff - wide), LANES)

    def weight_slots(src_sp):
        rows = pl.ds(pl.multiple_of(src_sp * depth, depth), depth)
        return (gate_w.at[rows, :], up_w.at[rows, :], down_w.at[:, rows])

    def weight_sources(zz):
        lanes = pl.ds(piece_start(zz), wide)
        rows = pl.ds(piece_start(zz), wide)
        return (w_gate.at[:, lanes], w_up.at[:, lanes], w_down.at[rows, :])

    local = [
        pltpu.make_async_copy(src, dst, loc_sem.at[i])
        for i, (src, dst) in enumerate(zip(weight_sources(z), weight_slots(sp)))
    ]
    local.append(pltpu.make_async_copy(w_out, out_weights, loc_sem.at[3]))
    local.append(
        pltpu.make_async_copy(
            resid.at[pl.ds(pl.multiple_of(tp * quarter, quarter), quarter), :],
            own_resid,
            loc_sem.at[4],
        )
    )
    for one in local:
        one.start()

    kv_normed = rms_rows(kv_latent[...], kv_gain[...])
    cos_t = jnp.concatenate([cos_ref[...], cos_ref[...]], axis=1)
    sin_t = jnp.concatenate([-sin_ref[...], sin_ref[...]], axis=1)

    def turn(values):
        swapped = jnp.concatenate([values[:, RD // 2 :], values[:, : RD // 2]], axis=1)
        return values * cos_t + swapped * sin_t

    own_at = pl.multiple_of(sp * tok, tok)
    packed[pl.ds(own_at, tok), :rank] = kv_normed
    packed[pl.ds(own_at, tok), rank:] = side_ref[...]

    barrier = pltpu.get_barrier_semaphore()
    mates = z_mates + [y_mate, x_mate, c_mate, diagonal]
    for mate in mates:
        pl.semaphore_signal(barrier, inc=1, device_id=mate, device_id_type=MESH)
    pl.semaphore_wait(barrier, len(mates))

    sends = []

    def begin(copy):
        copy.start()
        sends.append(copy)

    def half_of(src_sp, cc):
        return packed.at[pl.ds(pl.multiple_of(src_sp * tok + cc * half, half), half), :]

    own_half = half_of(sp, c)
    for s in range(1, nz):
        begin(remote(own_half, own_half, kvz_s.at[s - 1], kvz_r.at[s - 1], z_mates[s - 1]))
    begin(remote(own_half, own_half, kvy_s.at[0], kvy_r.at[0], y_mate))
    q_normed = rms_rows(q_latent[...], q_gain[...])
    own_mark = side_ref[...].astype(jnp.float32)[:, RD:]
    q_side = jnp.where(own_mark > 0.5, 0.0, -1e30)
    for h in range(heads):
        wide_q = jnp.dot(
            q_normed,
            w_query[:, h * (NOPE + RD) : (h + 1) * (NOPE + RD)],
            preferred_element_type=jnp.float32,
        )
        rest = jnp.concatenate([turn(wide_q[:, NOPE:]), q_side], axis=1)
        queries[h, :, :NOPE] = wide_q[:, :NOPE].astype(jnp.bfloat16)
        queries[h, :, NOPE:] = rest.astype(jnp.bfloat16)

    def source(s):
        return ((z + nz - s) % nz) * ny + y

    def source_y(s):
        return ((z + nz - s) % nz) * ny + (1 - y)

    for s in range(1, nz):
        block = half_of(source(s), c)
        remote(block, block, kvz_s.at[s - 1], kvz_r.at[s - 1], z_mates[s - 1]).wait_recv()
        begin(remote(block, block, kvy_s.at[s], kvy_r.at[s], y_mate))
        begin(remote(block, block, kvc_s.at[s - 1], kvc_r.at[s - 1], c_mate))
    slots = weight_slots(sp)
    for m in range(3):
        for s in range(1, nz):
            src = weight_sources((z + s) % nz)[m]
            begin(remote(src, slots[m], wz_s.at[s - 1, m], wz_r.at[s - 1, m], z_mates[s - 1]))
    for m in range(3):
        local[m].wait()
        begin(remote(slots[m], slots[m], wy_s.at[0, m], wy_r.at[0, m], y_mate))
    for s in range(nz):
        block = half_of(source_y(s), c)
        remote(block, block, kvy_s.at[s], kvy_r.at[s], y_mate).wait_recv()
        begin(remote(block, block, kvc_s.at[nz - 1 + s], kvc_r.at[nz - 1 + s], c_mate))
    for s in range(1, nz):
        block = half_of(source(s), 1 - c)
        remote(block, block, kvc_s.at[s - 1], kvc_r.at[s - 1], c_mate).wait_recv()
    for s in range(nz):
        block = half_of(source_y(s), 1 - c)
        remote(block, block, kvc_s.at[nz - 1 + s], kvc_r.at[nz - 1 + s], c_mate).wait_recv()

    chunk = scores.shape[3]
    chunks = total // chunk
    scale = (NOPE + RD) ** (-0.5) * log2_e

    def pass_weights(m):
        for s in range(1, nz):
            got = weight_slots(source(s))[m]
            remote(got, got, wz_s.at[s - 1, m], wz_r.at[s - 1, m], z_mates[s - 1]).wait_recv()
            begin(remote(got, got, wy_s.at[s, m], wy_r.at[s, m], y_mate))

    def score_chunk(h, k):
        rows = pl.ds(pl.multiple_of(k * chunk, chunk), chunk)
        lanes = slice(h * NOPE, (h + 1) * NOPE)
        both = jnp.dot(
            packed[rows, :rank],
            jnp.concatenate([w_key[:, lanes], w_value[:, lanes]], axis=1),
            preferred_element_type=jnp.float32,
        ).astype(jnp.bfloat16)
        vals[h % 2, rows, :] = both[:, NOPE:]
        keys = jnp.concatenate([both[:, :NOPE], packed[rows, rank:]], axis=1)
        value = lax.dot_general(
            queries[h], keys, (((1,), (1,)), ((), ())), preferred_element_type=jnp.float32
        )
        scores[h % 2, k] = value
        most = top_ref[...]
        for j in range(chunk // LANES):
            most = jnp.maximum(most, value[:, j * LANES : (j + 1) * LANES])
        top_ref[...] = most

    def weigh_chunk(h, k, top):
        rows = pl.ds(pl.multiple_of(k * chunk, chunk), chunk)
        weights = jnp.exp2((scores[h % 2, k] - top) * scale)
        denom = den_ref[...]
        for j in range(chunk // LANES):
            denom = denom + weights[:, j * LANES : (j + 1) * LANES]
        den_ref[...] = denom
        acc_ref[...] += jnp.dot(
            weights.astype(jnp.bfloat16), vals[h % 2, rows, :], preferred_element_type=jnp.float32
        )

    tp_mates = [c_mate, x_mate, diagonal]
    tp_of = [x * CORES + 1 - c, (1 - x) * CORES + c, (1 - x) * CORES + 1 - c]

    def head_piece(h, i):
        lanes = slice(h * VD, (h + 1) * VD)
        rows = pl.ds(pl.multiple_of(tp_of[i] * quarter, quarter), quarter)
        return remote(
            attended.at[rows, lanes], head_rows.at[tp, :, lanes], tp_s.at[i, h], tp_r.at[i, h], tp_mates[i]
        )

    def head_arrives(h, i):
        slot = head_rows.at[tp_of[i], :, slice(h * VD, (h + 1) * VD)]
        remote(slot, slot, tp_s.at[i, h], tp_r.at[i, h], tp_mates[i]).wait_recv()

    for h in range(heads + 1):
        top = None
        if h > 0:
            top = jnp.max(top_ref[...], axis=1, keepdims=True)
            den_ref[...] = jnp.zeros_like(den_ref)
            acc_ref[...] = jnp.zeros_like(acc_ref)
        if h < heads:
            top_ref[...] = jnp.full_like(top_ref, -3.0e38)

        def one_chunk(k, carry, h=h, top=top):
            if h > 0:
                weigh_chunk(h - 1, k, top)
            if h < heads:
                score_chunk(h, k)
            return carry

        lax.fori_loop(0, chunks, one_chunk, 0)
        if h > 0:
            denom = jnp.sum(den_ref[...], axis=1, keepdims=True)
            attended[:, (h - 1) * VD : h * VD] = (acc_ref[...] / denom).astype(jnp.bfloat16)
            for i in (2, 1, 0):
                begin(head_piece(h - 1, i))

    head_rows[tp] = attended[pl.ds(pl.multiple_of(tp * quarter, quarter), quarter), :]
    pass_weights(0)
    local[3].wait()
    local[4].wait()
    for h in range(heads):
        for i in range(3):
            head_arrives(h, i)
    span = head_rows.shape[2]
    mixed = resid_alpha * own_resid[...].astype(jnp.float32)
    for t in range(tp_count):
        mixed = mixed + jnp.dot(
            head_rows[t], out_weights[t * span : (t + 1) * span, :], preferred_element_type=jnp.float32
        )
    rows_all[z, x, c] = layer_scaled(mixed, mix_gain[...]).astype(jnp.bfloat16)

    first = piece_start(z)
    stale = z * wide - first

    def z_sends(zz):
        block = rows_all.at[zz, x, c]
        return (
            (jnp.logical_and(zz <= z, z < nz - 1), remote(block, block, up_s.at[zz], z_r.at[zz], at(zz=jnp.minimum(z + 1, nz - 1)))),
            (jnp.logical_and(zz >= z, z > 0), remote(block, block, dn_s.at[zz], z_r.at[zz], at(zz=jnp.maximum(z - 1, 0)))),
        )

    def x_send(zz):
        block = rows_all.at[zz, x, c]
        return remote(block, block, x_s.at[zz], x_r.at[zz], x_mate)

    def c_send(zz, xx):
        block = rows_all.at[zz, xx, c]
        return remote(block, block, c_s.at[zz, xx], c_r.at[zz, xx], c_mate)

    def arrive_x(zz):
        block = rows_all.at[zz, 1 - x, c]
        remote(block, block, x_s.at[zz], x_r.at[zz], x_mate).wait_recv()

    def arrive_c(zz, xx):
        block = rows_all.at[zz, xx, 1 - c]
        remote(block, block, c_s.at[zz, xx], c_r.at[zz, xx], c_mate).wait_recv()

    def core_send(zz, xx):
        return remote(part.at[zz, xx, 1 - c], core_part.at[zz, xx], crs_s.at[zz, xx], crs_r.at[zz, xx], c_mate)

    def x_sum_send(zz):
        return remote(x_stage.at[zz], x_part.at[zz], xrs_s.at[zz], xrs_r.at[zz], x_mate)

    def up_sum_send(zz):
        return remote(z_stage.at[zz], up_part.at[zz], zch_s.at[zz], zup_r.at[zz], at(zz=jnp.minimum(z + 1, nz - 1)))

    def dn_sum_send(zz):
        return remote(z_stage.at[zz], dn_part.at[zz], zch_s.at[zz], zdn_r.at[zz], at(zz=jnp.maximum(z - 1, 0)))

    def pair_sum(zz, xx):
        return part[zz, xx, c].astype(jnp.float32) + core_part[zz, xx].astype(jnp.float32)

    def gather_step(step):
        zz = near_order(step, z, nz)

        @pl.when(step > 0)
        def _():
            block = rows_all.at[zz, x, c]
            remote(block, block, up_s.at[zz], z_r.at[zz], x_mate).wait_recv()

        for wanted, copy in z_sends(zz):
            pl.when(wanted)(copy.start)
        x_send(zz).start()
        c_send(zz, x).start()

    def across_step(step):
        zz = near_order(step, z, nz)
        arrive_x(zz)
        c_send(zz, 1 - x).start()

    def mix_step(step):
        zz = near_order(nz - 1 - step, z, nz)
        arrive_c(zz, x)
        arrive_c(zz, 1 - x)
        rows = 2 * CORES * quarter
        lanes = lax.broadcasted_iota(jnp.int32, (1, wide), 1)
        unit = rows_all[zz].reshape(rows, model)
        gate = jnp.dot(unit, gate_w[...], preferred_element_type=jnp.float32)
        up = jnp.dot(unit, up_w[...], preferred_element_type=jnp.float32)
        inner = jax.nn.silu(gate) * up
        hidden[...] = jnp.where(lanes >= stale, inner, 0.0).astype(jnp.bfloat16)
        cut = 512
        for n in range(model // cut):
            piece = jnp.dot(
                hidden[...], down_w[:, n * cut : (n + 1) * cut], preferred_element_type=jnp.float32
            ).astype(jnp.bfloat16)
            part[zz, :, :, :, n * cut : (n + 1) * cut] = piece.reshape(2, CORES, quarter, cut)
        core_send(zz, 1 - x).start()
        core_send(zz, x).start()
        core_send(zz, 1 - x).wait_recv()
        x_stage[zz] = pair_sum(zz, 1 - x).astype(jnp.bfloat16)
        x_sum_send(zz).start()

    def ready_sum(zz):
        core_send(zz, x).wait_recv()
        x_sum_send(zz).wait_recv()
        return pair_sum(zz, x) + x_part[zz].astype(jnp.float32)

    def chain_step(step):
        above = nz - 1 - step + z

        @pl.when(jnp.logical_and(above > z, above < nz))
        def _():
            z_stage[above] = ready_sum(above).astype(jnp.bfloat16)

            @pl.when(z > 0)
            def _():
                up_sum_send(above).wait_recv()
                z_stage[above] = (
                    z_stage[above].astype(jnp.float32) + up_part[above].astype(jnp.float32)
                ).astype(jnp.bfloat16)

            up_sum_send(above).start()

        mirrored = nz - 1 - z
        below_m = nz - 1 - step + mirrored
        below = nz - 1 - below_m

        @pl.when(jnp.logical_and(below_m > mirrored, below_m < nz))
        def _():
            z_stage[below] = ready_sum(below).astype(jnp.bfloat16)

            @pl.when(mirrored > 0)
            def _():
                dn_sum_send(below).wait_recv()
                z_stage[below] = (
                    z_stage[below].astype(jnp.float32) + dn_part[below].astype(jnp.float32)
                ).astype(jnp.bfloat16)

            dn_sum_send(below).start()

    gather_step(jnp.int32(0))
    for step in range(1, nz):
        if step < 3:
            pass_weights(step)
        gather_step(jnp.int32(step))
        across_step(jnp.int32(step - 1))
    across_step(jnp.int32(nz - 1))
    for m in range(3):
        for s in range(nz):
            got = weight_slots(source_y(s))[m]
            remote(got, got, wy_s.at[s, m], wy_r.at[s, m], y_mate).wait_recv()

    def one_step(step, carry):
        mix_step(step)
        pl.when(step > 0)(lambda: chain_step(step - 1))
        return carry

    lax.fori_loop(0, nz, one_step, 0)

    ffn_sum = ready_sum(z)
    pl.when(z > 0)(up_sum_send(z).wait_recv)
    pl.when(z < nz - 1)(dn_sum_send(z).wait_recv)
    part_sum = ffn_sum + jnp.where(z > 0, up_part[z].astype(jnp.float32), 0.0)
    part_sum = part_sum + jnp.where(z < nz - 1, dn_part[z].astype(jnp.float32), 0.0)
    out_ref[...] = layer_scaled(
        resid_alpha * rows_all[z, x, c].astype(jnp.float32) + 0.5 * part_sum, out_gain[...]
    ).astype(jnp.bfloat16)

    for copy in sends:
        copy.wait_send()

    def drain(zz, carry):
        for wanted, copy in z_sends(zz):
            pl.when(wanted)(copy.wait_send)
        x_send(zz).wait_send()
        for xx in range(2):
            c_send(zz, xx).wait_send()
            core_send(zz, xx).wait_send()
        x_sum_send(zz).wait_send()
        pl.when(zz > z)(up_sum_send(zz).wait_send)
        pl.when(zz < z)(dn_sum_send(zz).wait_send)
        return carry

    lax.fori_loop(0, nz, drain, 0)


def fused_layer(
    sp_count,
    tp_count,
    resid_stream,
    q_latent,
    kv_latent,
    rope_key,
    doc_ids,
    q_gain,
    kv_gain,
    w_query,
    w_key,
    w_value,
    w_out,
    mix_gain,
    w_gate,
    w_up,
    w_down,
    out_gain,
):
    ny = tp_count // CORES
    nz = sp_count // ny
    tok = q_latent.shape[0]
    total = tok * sp_count
    quarter = tok // tp_count
    model = resid_stream.shape[1]
    heads = w_key.shape[1] // NOPE
    rank = kv_latent.shape[1]
    ff = w_gate.shape[1]
    wide = -(-ff // (LANES * nz)) * LANES
    chunk = 512
    positions = lax.axis_index("sp") * tok + jnp.arange(tok, dtype=jnp.int32)
    cos_table, sin_table = rope_angles(positions)
    key_rot = rotate(rope_key.astype(jnp.float32), cos_table, sin_table).astype(jnp.bfloat16)
    marks = doc_ids[:, None] == jnp.arange(RD, dtype=jnp.int32)[None, :]
    side = jnp.concatenate([key_rot, marks.astype(jnp.bfloat16)], axis=1)
    vmem = pl.BlockSpec(memory_space=pltpu.VMEM)
    hbm = pl.BlockSpec(memory_space=pl.ANY)
    bf16, f32 = jnp.bfloat16, jnp.float32
    dma = pltpu.SemaphoreType.DMA
    scratch = [
        pltpu.VMEM((total, rank + 2 * RD), bf16),
        pltpu.VMEM((heads, tok, NOPE + 2 * RD), bf16),
        pltpu.VMEM((2, total, VD), bf16),
        pltpu.VMEM((2, total // chunk, tok, chunk), f32),
        pltpu.VMEM((tok, LANES), f32),
        pltpu.VMEM((tok, LANES), f32),
        pltpu.VMEM((tok, VD), f32),
        pltpu.VMEM((tok, heads * VD), bf16),
        pltpu.VMEM((tp_count, quarter, heads * VD), bf16),
        pltpu.VMEM(w_out.shape, bf16),
        pltpu.VMEM((quarter, model), bf16),
        pltpu.VMEM((model, wide), bf16),
        pltpu.VMEM((model, wide), bf16),
        pltpu.VMEM((wide, model), bf16),
        pltpu.VMEM((nz, 2, CORES, quarter, model), bf16),
        pltpu.VMEM((2 * CORES * quarter, wide), bf16),
        pltpu.VMEM((nz, 2, CORES, quarter, model), bf16),
        pltpu.VMEM((nz, 2, quarter, model), bf16),
        pltpu.VMEM((nz, quarter, model), bf16),
        pltpu.VMEM((nz, quarter, model), bf16),
        pltpu.VMEM((nz, quarter, model), bf16),
        pltpu.VMEM((nz, quarter, model), bf16),
        pltpu.VMEM((nz, quarter, model), bf16),
        dma((5,)),
        dma((nz - 1,)),
        dma((nz - 1,)),
        dma((nz,)),
        dma((nz,)),
        dma((2 * nz - 1,)),
        dma((2 * nz - 1,)),
        dma((nz - 1, 3)),
        dma((nz - 1, 3)),
        dma((nz, 3)),
        dma((nz, 3)),
        dma((3, heads)),
        dma((3, heads)),
        dma((nz,)),
        dma((nz,)),
        dma((nz,)),
        dma((nz,)),
        dma((nz,)),
        dma((nz, 2)),
        dma((nz, 2)),
        dma((nz, 2)),
        dma((nz, 2)),
        dma((nz,)),
        dma((nz,)),
        dma((nz,)),
        dma((nz,)),
        dma((nz,)),
    ]
    return pl.pallas_call(
        functools.partial(layer_kernel, nz, ny, heads),
        out_shape=jax.ShapeDtypeStruct((quarter, model), bf16),
        in_specs=[vmem] * 12 + [hbm] * 5,
        out_specs=vmem,
        scratch_shapes=scratch,
        compiler_params=pltpu.CompilerParams(
            collective_id=0, has_side_effects=True, vmem_limit_bytes=67043328
        ),
    )(
        q_latent,
        kv_latent,
        side,
        cos_table,
        sin_table,
        q_gain[None, :],
        kv_gain[None, :],
        mix_gain[None, :],
        out_gain[None, :],
        w_query,
        w_key,
        w_value,
        resid_stream,
        w_out,
        w_gate,
        w_up,
        w_down,
    )


def solution(mesh):
    in_specs = (
        P("sp", None),
        P("sp", None),
        P("sp", None),
        P("sp", None),
        P("sp"),
        P(),
        P(),
        P(None, "tp"),
        P(None, "tp"),
        P(None, "tp"),
        P(),
        P(),
        P("sp", "tp"),
        P("sp", "tp"),
        P("tp", "sp"),
        P(),
    )
    out_specs = P(("sp", "tp"), None)
    if mesh.shape["tp"] == 2 * CORES:
        return jax.shard_map(
            functools.partial(fused_layer, mesh.shape["sp"], mesh.shape["tp"]),
            mesh=mesh,
            in_specs=in_specs,
            out_specs=out_specs,
            check_vma=False,
        )
    return jax.shard_map(body, mesh=mesh, in_specs=in_specs, out_specs=out_specs, check_vma=False)
```

```python
import functools
import math

import jax
import jax.numpy as jnp
import numpy as np
from jax import lax
from jax.experimental import pallas as pl
from jax.experimental.pallas import tpu as pltpu
from jax.sharding import PartitionSpec as P

NOPE = 128
RD = 64
VD = 128


eps_norm = 1e-05
rope_theta = 10000.0
resid_alpha = 8.0**0.25
key_span = 2048


def rope_angles(positions):
    frequency = rope_theta ** (-jnp.arange(0, RD, 2, dtype=jnp.float32) / RD)
    angles = positions.astype(jnp.float32)[:, None] * frequency[None, :]
    return (jnp.cos(angles), jnp.sin(angles))


def rotate(values, cos_table, sin_table):
    half_width = values.shape[-1] // 2
    first_half = values[..., :half_width]
    second_half = values[..., half_width:]
    return jnp.concatenate(
        [
            first_half * cos_table - second_half * sin_table,
            second_half * cos_table + first_half * sin_table,
        ],
        axis=-1,
    )


def rms_scaled(latent, scaling):
    widened = latent.astype(jnp.float32)
    inverse = lax.rsqrt(jnp.mean(widened * widened, axis=-1, keepdims=True) + eps_norm)
    return (widened * inverse * scaling).astype(jnp.bfloat16)


def layer_scaled(stream, scaling):
    centre = stream - jnp.mean(stream, axis=-1, keepdims=True)
    spread = jnp.mean(centre * centre, axis=-1, keepdims=True)
    return centre * lax.rsqrt(spread + eps_norm) * scaling


def fold_in_blocks(carried, piece_part, attend_fn):
    piece_rows = piece_part[0].shape[0]
    if piece_rows > key_span and piece_rows % key_span == 0:

        def one_block(inner, block_index):
            sliced = tuple(
                (
                    lax.dynamic_slice_in_dim(
                        member, (block_index * key_span).astype(jnp.int32), key_span, 0
                    )
                    for member in piece_part
                )
            )
            return (attend_fn(inner, sliced), None)

        outcome = lax.scan(one_block, carried, jnp.arange(piece_rows // key_span, dtype=jnp.int32))
        return outcome[0]
    return attend_fn(carried, piece_part)


class Ring:
    def __init__(self, blocks):
        self.count = lax.axis_size("sp")
        ring = list(range(0, self.count, 2)) + list(range(1, self.count, 2))[::-1]
        places = [ring.index(i) for i in range(self.count)]
        self.place = jnp.array(places, jnp.int32)[lax.axis_index("sp")]
        self.ring_of = jnp.array(ring, jnp.int32)
        self.right = [(ring[i], ring[(i + 1) % self.count]) for i in range(self.count)]
        self.left = [(after, before) for before, after in self.right]
        self.pieces = [[(lax.axis_index("sp"), block)] for block in blocks]
        self.flying = [(block, block) for block in blocks]
        self.step = 0

    def owner(self, distance):
        return self.ring_of[(self.place + distance) % self.count]

    def hop(self):
        self.step += 1
        self.send()

    def send(self):
        if self.step < self.count // 2:
            self.flying = [
                (lax.ppermute(one, "sp", self.right), lax.ppermute(two, "sp", self.left))
                for one, two in self.flying
            ]
        elif self.step == self.count // 2:
            self.flying = [
                (
                    lax.ppermute(one[: one.shape[0] // 2], "sp", self.right),
                    lax.ppermute(two[two.shape[0] // 2 :], "sp", self.left),
                )
                for one, two in self.flying
            ]

    def land(self, *values):
        if self.step <= self.count // 2:
            if values:
                values, self.flying = lax.optimization_barrier((values, self.flying))
            for pieces, (one, two) in zip(self.pieces, self.flying):
                if self.step < self.count // 2:
                    pieces.append((self.owner(-self.step), one))
                    pieces.append((self.owner(self.step), two))
                else:
                    pieces.append((self.owner(self.step), jnp.concatenate([one, two])))
        return values


def body(
    resid_stream,
    q_latent,
    kv_latent,
    rope_key,
    doc_ids,
    q_gain,
    kv_gain,
    w_query,
    w_key,
    w_value,
    w_out,
    mix_gain,
    w_gate,
    w_up,
    w_down,
    out_gain,
):
    tok_rows = q_latent.shape[0]
    head_count = w_key.shape[1] // NOPE
    tp_count = lax.axis_size("tp")
    part_rows = tok_rows // tp_count
    tp_index = lax.axis_index("tp")
    gate_ring = Ring([jnp.concatenate([w_gate, w_up], axis=1)])
    down_ring = Ring([w_down])
    gate_ring.hop()
    positions = lax.axis_index("sp") * tok_rows + jnp.arange(tok_rows, dtype=jnp.int32)
    cos_table, sin_table = rope_angles(positions)
    q_normed = rms_scaled(q_latent, q_gain)
    queries = jnp.dot(q_normed, w_query, preferred_element_type=jnp.float32).reshape(
        tok_rows, head_count, NOPE + RD
    )
    query_nope = queries[:, :, :NOPE].astype(jnp.bfloat16)
    query_rope = rotate(queries[:, :, NOPE:], cos_table[:, None, :], sin_table[:, None, :]).astype(
        jnp.bfloat16
    )
    kv_normed = rms_scaled(kv_latent, kv_gain)
    key_rot = rotate(rope_key.astype(jnp.float32), cos_table, sin_table).astype(jnp.bfloat16)
    score_scale = (NOPE + RD) ** (-0.5)

    def attend_rows(carried, piece_part, between=lambda value: value):
        row_top, denom_sum, accum_out = carried
        key_piece, value_piece, rot_piece, doc_piece = piece_part
        piece_rows = key_piece.shape[0]
        keys_heads = key_piece.reshape(piece_rows, head_count, NOPE)
        values_heads = value_piece.reshape(piece_rows, head_count, VD)
        scores = jnp.einsum(
            "qhd,khd->hqk", query_nope, keys_heads, preferred_element_type=jnp.float32
        )
        scores = (
            scores
            + jnp.einsum("qhd,kd->hqk", query_rope, rot_piece, preferred_element_type=jnp.float32)
        ) * score_scale
        same_doc = (doc_ids[:, None] == doc_piece[None, :])[None]
        masked = jnp.where(same_doc, scores, -1e30)
        new_top = jnp.maximum(row_top, jnp.max(masked, axis=-1))
        weights = jnp.where(same_doc, jnp.exp(masked - new_top[:, :, None]), 0.0)
        factor = jnp.exp(row_top - new_top)
        denom_sum = denom_sum * factor + jnp.sum(weights, axis=-1)
        weights = between(weights.astype(jnp.bfloat16))
        update = jnp.einsum(
            "hqk,khd->qhd", weights, values_heads, preferred_element_type=jnp.float32
        )
        accum_out = accum_out * jnp.transpose(factor)[:, :, None] + update
        return (new_top, denom_sum, accum_out)

    initial = (
        jnp.full((head_count, tok_rows), -1e30, jnp.float32),
        jnp.zeros((head_count, tok_rows), jnp.float32),
        jnp.zeros((tok_rows, head_count, VD), jnp.float32),
    )

    def project_rows(carried, piece_part, between=lambda value: value):
        latent_piece, rot_piece, doc_piece = piece_part
        key_piece = jnp.dot(latent_piece, w_key, preferred_element_type=jnp.float32).astype(
            jnp.bfloat16
        )
        value_piece = jnp.dot(latent_piece, w_value, preferred_element_type=jnp.float32).astype(
            jnp.bfloat16
        )
        return attend_rows(carried, (key_piece, value_piece, rot_piece, doc_piece), between)

    def next_hop(value):
        (value,) = gate_ring.land(value)
        gate_ring.hop()
        return value

    doc_lanes = jnp.broadcast_to(doc_ids.astype(jnp.bfloat16)[:, None], (tok_rows, RD))
    packed = jnp.concatenate([kv_normed, key_rot, doc_lanes], axis=1)
    packed_part = lax.dynamic_slice_in_dim(packed, tp_index * part_rows, part_rows, 0)
    packed_all = lax.all_gather(packed_part, ("sp", "tp"), axis=0, tiled=True)
    packed_all = next_hop(packed_all)
    kv_rank = kv_latent.shape[1]
    gathered = (
        packed_all[:, :kv_rank],
        packed_all[:, kv_rank : kv_rank + RD],
        packed_all[:, kv_rank + RD].astype(jnp.int32),
    )
    if packed_all.shape[0] > key_span and packed_all.shape[0] % key_span == 0:
        carried_out = fold_in_blocks(initial, gathered, project_rows)
    else:
        carried_out = project_rows(initial, gathered, next_hop)
    denom_sum = carried_out[1]
    attended = (
        (carried_out[2] / jnp.transpose(denom_sum)[:, :, None])
        .astype(jnp.bfloat16)
        .reshape(tok_rows, head_count * VD)
    )
    heads_rows = lax.all_to_all(attended, "tp", split_axis=0, concat_axis=1, tiled=True)
    mixer_out = jnp.dot(heads_rows, w_out, preferred_element_type=jnp.float32)
    own_resid = lax.dynamic_slice_in_dim(resid_stream, tp_index * part_rows, part_rows, 0)
    own_normed = layer_scaled(
        resid_alpha * own_resid.astype(jnp.float32) + mixer_out, mix_gain
    ).astype(jnp.bfloat16)
    (own_normed,) = gate_ring.land(own_normed)
    down_ring.hop()
    gate_ring.hop()
    normed_rows = lax.all_gather(own_normed, "tp", axis=0, tiled=True)
    (normed_rows,) = down_ring.land(normed_rows)
    down_ring.hop()
    gate_ring.land()
    while gate_ring.step < gate_ring.count // 2:
        gate_ring.hop()
        gate_ring.land()
    gate_sum = None
    for owner, piece in gate_ring.pieces[0]:
        rows = lax.dynamic_slice_in_dim(normed_rows, owner * piece.shape[0], piece.shape[0], 1)
        term = jnp.dot(rows, piece, preferred_element_type=jnp.float32)
        gate_sum = term if gate_sum is None else gate_sum + term
    width = w_gate.shape[1]
    hidden = (jax.nn.silu(gate_sum[:, :width]) * gate_sum[:, width:]).astype(jnp.bfloat16)
    (hidden,) = down_ring.land(hidden)
    while down_ring.step < down_ring.count // 2:
        down_ring.hop()
        down_ring.land()
    down = down_ring.pieces[0]
    ffn_sum = jnp.zeros((part_rows, resid_stream.shape[1]), jnp.float32)
    for part, group in enumerate((down[: len(down) // 2], down[len(down) // 2 :])):
        pieces = [piece for _, piece in group]
        if part == 0:
            pieces = [jnp.concatenate(pieces, axis=1)]
        terms = [
            jnp.dot(hidden, piece, preferred_element_type=jnp.float32).astype(jnp.bfloat16)
            for piece in pieces
        ]
        partial = jnp.concatenate(terms, axis=1)
        swapped = lax.all_to_all(
            partial.reshape(tp_count, part_rows, -1), "tp", split_axis=0, concat_axis=0, tiled=True
        )
        summed = jnp.sum(swapped.astype(jnp.float32), axis=0)
        columns = w_down.shape[1]
        for at, (owner, _) in enumerate(group):
            ffn_sum = lax.dynamic_update_slice_in_dim(
                ffn_sum, summed[:, at * columns : (at + 1) * columns], owner * columns, 1
            )
    layer_out = layer_scaled(
        resid_alpha * own_normed.astype(jnp.float32) + 0.5 * ffn_sum, out_gain
    ).astype(jnp.bfloat16)
    return layer_out


CORES = 2
LANES = 128
MESH = pl.DeviceIdType.MESH
log2_e = math.log2(math.e)


def rms_rows(latent, scaling):
    widened = latent.astype(jnp.float32)
    inverse = lax.rsqrt(jnp.mean(widened * widened, axis=-1, keepdims=True) + eps_norm)
    return (widened * inverse * scaling).astype(jnp.bfloat16)


def near_order(step, z, nz):
    paired = 2 * jnp.minimum(z, nz - 1 - z)
    half = (step + 1) // 2
    close = jnp.where(step % 2 == 1, z - half, z + half)
    far = step - paired // 2
    wide = jnp.where(z < nz - 1 - z, z + far, z - far)
    return jnp.where(step <= paired, close, wide)


def turn_table(total):
    steps = np.arange(0, RD, 2, dtype=np.float32) / np.float32(RD)
    frequency = np.power(np.float32(rope_theta), -steps, dtype=np.float32)
    angles = frequency[:, None] * np.arange(total, dtype=np.float32)[None, :]
    wide_angles = angles.astype(np.float64)
    return np.concatenate([np.cos(wide_angles), np.sin(wide_angles)], axis=0).astype(np.float32)


def layer_kernel(
    nz,
    ny,
    heads,
    q_latent,
    kv_latent,
    rope_turned,
    doc_row,
    table,
    q_gain_in,
    kv_gain_in,
    mix_gain_in,
    out_gain_in,
    w_query_in,
    w_key_in,
    w_value_in,
    resid,
    w_out,
    w_gate,
    w_up,
    w_down,
    out_ref,
    q_lat,
    kv_lat,
    rope_own,
    doc_own,
    turns,
    q_gain,
    kv_gain,
    mix_gain,
    out_gain,
    w_query,
    w_key,
    w_value,
    packed,
    queries,
    vals,
    scores,
    top_ref,
    den_ref,
    acc_ref,
    attended,
    head_rows,
    out_weights,
    own_resid,
    gate_w,
    up_w,
    down_w,
    rows_all,
    hidden,
    part,
    core_part,
    x_stage,
    x_part,
    z_stage,
    z_part,
    late_stage,
    late_part,
    last_stage,
    last_part,
    loc_sem,
    own_sem,
    kvz_s,
    kvz_r,
    kvy_s,
    kvy_r,
    kvx_s,
    kvx_r,
    kvc_s,
    kvc_r,
    wz_s,
    wz_r,
    wy_s,
    wy_r,
    tp_s,
    tp_r,
    up_s,
    dn_s,
    z_r,
    x_s,
    x_r,
    c_s,
    c_r,
    crs_s,
    crs_r,
    xrs_s,
    xrs_r,
    zch_s,
    zch_r,
    late_s,
    late_r,
    last_sem,
):
    sp = lax.axis_index("sp")
    tp = lax.axis_index("tp")
    z, y = sp // ny, sp % ny
    x, c = tp // CORES, tp % CORES
    tok = q_latent.shape[0]
    quarter = out_ref.shape[0]
    tp_count = tok // quarter
    depth = w_gate.shape[0]
    wide = gate_w.shape[1]
    ff = w_gate.shape[1]
    model = out_ref.shape[1]
    total = packed.shape[0]
    rank = kv_latent.shape[1]

    def at(zz=None, yy=None, xx=None, cc=None):
        zz = z if zz is None else zz
        yy = y if yy is None else yy
        xx = x if xx is None else xx
        cc = c if cc is None else cc
        return (zz * ny + yy, xx * CORES + cc)

    def remote(src, dst, send, recv, where):
        return pltpu.make_async_remote_copy(
            src_ref=src,
            dst_ref=dst,
            send_sem=send,
            recv_sem=recv,
            device_id=where,
            device_id_type=MESH,
        )

    y_mate = at(yy=1 - y)
    x_mate = at(xx=1 - x)
    c_mate = at(cc=1 - c)
    diagonal = at(xx=1 - x, cc=1 - c)
    z_mates = [at(zz=(z + s) % nz) for s in range(1, nz)]

    barrier = pltpu.get_barrier_semaphore()
    mates = z_mates + [y_mate, x_mate, c_mate, diagonal]
    for mate in mates:
        pl.semaphore_signal(barrier, inc=1, device_id=mate, device_id_type=MESH)

    tiles = wide // LANES
    missing = nz * tiles - ff // LANES

    def is_short(zz):
        return (zz + nz - (nz // 2 - 1 + c)) % nz < missing

    def piece_start(zz):
        begun = 0
        for other in range(nz - 1):
            begun = begun + jnp.where(other < zz, tiles - is_short(other).astype(jnp.int32), 0)
        return pl.multiple_of(begun * LANES, LANES)

    def by_width(zz, make):
        pairs = [(jnp.logical_not(is_short(zz)), make(wide))]
        if missing:
            pairs.append((is_short(zz), make(wide - LANES)))
        return pairs

    def when_start(pairs):
        for wanted, copy in pairs:
            pl.when(wanted)(copy.start)

    def when_wait_recv(pairs):
        for wanted, copy in pairs:
            pl.when(wanted)(copy.wait_recv)

    def weight_slot(src_sp, m, width):
        rows = pl.ds(pl.multiple_of(src_sp * depth, depth), depth)
        if m == 2:
            return down_w.at[pl.ds(0, width), rows]
        return (gate_w, up_w)[m].at[rows, pl.ds(0, width)]

    def weight_source(zz, m, width):
        units = pl.ds(piece_start(zz), width)
        return w_down.at[units, :] if m == 2 else (w_gate, w_up)[m].at[:, units]

    def own_weights(m):
        return by_width(
            z,
            lambda width: pltpu.make_async_copy(
                weight_source(z, m, width), weight_slot(sp, m, width), own_sem.at[m]
            ),
        )

    own_cols = pl.ds(pl.multiple_of(sp * tok, LANES), tok)
    own_quarter = pl.ds(pl.multiple_of(tp * quarter, quarter), quarter)
    moves = [
        (kv_latent, kv_lat),
        (kv_gain_in, kv_gain),
        (rope_turned, rope_own),
        (doc_row, doc_own),
        (table.at[:, own_cols], turns),
        (q_latent, q_lat),
        (q_gain_in, q_gain),
        (w_query_in, w_query),
        (w_key_in, w_key),
        (w_value_in, w_value),
        (mix_gain_in, mix_gain),
        (out_gain_in, out_gain),
        (resid.at[own_quarter, :], own_resid),
        (w_out, out_weights),
    ]
    local = [pltpu.make_async_copy(src, dst, loc_sem.at[n]) for n, (src, dst) in enumerate(moves)]
    for one in local:
        one.start()
    for m in range(3):
        when_start(own_weights(m))
    if missing:

        @pl.when(is_short(z))
        def _():
            down_w[wide - LANES :, :] = jnp.zeros((LANES, model), jnp.bfloat16)

    for n in range(5):
        local[n].wait()
    half_turn = RD // 2
    cos_rows = jnp.concatenate([turns[:half_turn], turns[:half_turn]], axis=0)
    sin_rows = jnp.concatenate([-turns[half_turn:], turns[half_turn:]], axis=0)
    rope = rope_own[...].astype(jnp.float32)
    flipped = jnp.concatenate([rope[half_turn:], rope[:half_turn]], axis=0)
    marks = lax.broadcasted_iota(jnp.int32, (RD, tok), 0) == doc_own[...]
    side_rows = jnp.concatenate(
        [rope * cos_rows + flipped * sin_rows, marks.astype(jnp.float32)], axis=0
    )
    side = side_rows.T
    own_at = pl.multiple_of(sp * tok, tok)
    packed[pl.ds(own_at, tok), :rank] = rms_rows(kv_lat[...], kv_gain[...])
    packed[pl.ds(own_at, tok), rank:] = side.astype(jnp.bfloat16)

    pl.semaphore_wait(barrier, len(mates))

    sends = []

    def begin(copy):
        copy.start()
        sends.append(copy)

    def latent_piece(src_sp, xx, cc):
        first_row = src_sp * tok + (xx * CORES + cc) * quarter
        return packed.at[pl.ds(pl.multiple_of(first_row, quarter), quarter), :]

    def source(s):
        return ((z + nz - s) % nz) * ny + y

    def source_y(s):
        return ((z + nz - s) % nz) * ny + (1 - y)

    foreign = [source(s) for s in range(1, nz)] + [source_y(s) for s in range(nz)]
    own_piece = latent_piece(sp, x, c)
    for s in range(1, nz):
        begin(remote(own_piece, own_piece, kvz_s.at[s - 1], kvz_r.at[s - 1], z_mates[s - 1]))
    begin(remote(own_piece, own_piece, kvy_s.at[0], kvy_r.at[0], y_mate))

    for n in range(5, 8):
        local[n].wait()
    both_turns = jnp.concatenate([cos_rows, sin_rows], axis=0).T
    cos_t, sin_t = both_turns[:, :RD], both_turns[:, RD:]
    q_normed = rms_rows(q_lat[...], q_gain[...])
    q_side = jnp.where(side[:, RD:] > 0.5, 0.0, -1e30)
    for h in range(heads):
        wide_q = jnp.dot(
            q_normed,
            w_query[:, h * (NOPE + RD) : (h + 1) * (NOPE + RD)],
            preferred_element_type=jnp.float32,
        )
        turned = wide_q[:, NOPE:]
        swapped = jnp.concatenate([turned[:, half_turn:], turned[:, :half_turn]], axis=1)
        rest = jnp.concatenate([turned * cos_t + swapped * sin_t, q_side], axis=1)
        queries[h, :, :NOPE] = wide_q[:, :NOPE].astype(jnp.bfloat16)
        queries[h, :, NOPE:] = rest.astype(jnp.bfloat16)

    def hand_on(n):
        piece = latent_piece(foreign[n], x, c)
        begin(remote(piece, piece, kvx_s.at[n], kvx_r.at[n], x_mate))
        begin(remote(piece, piece, kvc_s.at[0, n], kvc_r.at[0, n], c_mate))

    for s in range(1, nz):
        piece = latent_piece(source(s), x, c)
        remote(piece, piece, kvz_s.at[s - 1], kvz_r.at[s - 1], z_mates[s - 1]).wait_recv()
        begin(remote(piece, piece, kvy_s.at[s], kvy_r.at[s], y_mate))
        hand_on(s - 1)

    def weight_z(s, m):
        return by_width(
            (z + s) % nz,
            lambda width: remote(
                weight_source((z + s) % nz, m, width),
                weight_slot(sp, m, width),
                wz_s.at[s - 1, m],
                wz_r.at[s - 1, m],
                z_mates[s - 1],
            ),
        )

    def weight_z_in(s, m):
        def make(width):
            slot = weight_slot(source(s), m, width)
            return remote(slot, slot, wz_s.at[s - 1, m], wz_r.at[s - 1, m], z_mates[s - 1])

        return by_width(z, make)

    def weight_y(s, m, src_sp):
        def make(width):
            slot = weight_slot(src_sp, m, width)
            return remote(slot, slot, wy_s.at[s, m], wy_r.at[s, m], y_mate)

        return by_width(z, make)

    for m in range(3):
        for s in range(1, nz):
            when_start(weight_z(s, m))
    for s in range(nz):
        piece = latent_piece(source_y(s), x, c)
        remote(piece, piece, kvy_s.at[s], kvy_r.at[s], y_mate).wait_recv()
        hand_on(nz - 1 + s)
    for m in range(3):
        for wanted, copy in own_weights(m):
            pl.when(wanted)(copy.wait)
        when_start(weight_y(0, m, sp))
    for n, src_sp in enumerate(foreign):
        piece = latent_piece(src_sp, 1 - x, c)
        remote(piece, piece, kvx_s.at[n], kvx_r.at[n], x_mate).wait_recv()
        begin(remote(piece, piece, kvc_s.at[1, n], kvc_r.at[1, n], c_mate))
    for n, src_sp in enumerate(foreign):
        for k, xx in enumerate((x, 1 - x)):
            piece = latent_piece(src_sp, xx, 1 - c)
            remote(piece, piece, kvc_s.at[k, n], kvc_r.at[k, n], c_mate).wait_recv()
    local[8].wait()
    local[9].wait()

    chunk = scores.shape[3]
    chunks = total // chunk
    scale = (NOPE + RD) ** (-0.5) * log2_e

    def pass_weights(m):
        for s in range(1, nz):
            when_wait_recv(weight_z_in(s, m))
            when_start(weight_y(s, m, source(s)))

    def score_chunk(h, k):
        rows = pl.ds(pl.multiple_of(k * chunk, chunk), chunk)
        lanes = slice(h * NOPE, (h + 1) * NOPE)
        both = jnp.dot(
            packed[rows, :rank],
            jnp.concatenate([w_key[:, lanes], w_value[:, lanes]], axis=1),
            preferred_element_type=jnp.float32,
        ).astype(jnp.bfloat16)
        vals[h % 2, rows, :] = both[:, NOPE:]
        keys = jnp.concatenate([both[:, :NOPE], packed[rows, rank:]], axis=1)
        value = lax.dot_general(
            queries[h], keys, (((1,), (1,)), ((), ())), preferred_element_type=jnp.float32
        )
        scores[h % 2, k] = value
        most = top_ref[...]
        for j in range(chunk // LANES):
            most = jnp.maximum(most, value[:, j * LANES : (j + 1) * LANES])
        top_ref[...] = most

    def weigh_chunk(h, k, top):
        rows = pl.ds(pl.multiple_of(k * chunk, chunk), chunk)
        weights = jnp.exp2((scores[h % 2, k] - top) * scale)
        denom = den_ref[...]
        for j in range(chunk // LANES):
            denom = denom + weights[:, j * LANES : (j + 1) * LANES]
        den_ref[...] = denom
        acc_ref[...] += jnp.dot(
            weights.astype(jnp.bfloat16), vals[h % 2, rows, :], preferred_element_type=jnp.float32
        )

    tp_mates = [c_mate, x_mate, diagonal]
    tp_of = [x * CORES + 1 - c, (1 - x) * CORES + c, (1 - x) * CORES + 1 - c]

    def head_piece(h, i):
        lanes = slice(h * VD, (h + 1) * VD)
        rows = pl.ds(pl.multiple_of(tp_of[i] * quarter, quarter), quarter)
        return remote(
            attended.at[rows, lanes], head_rows.at[tp, :, lanes], tp_s.at[i, h], tp_r.at[i, h], tp_mates[i]
        )

    def head_arrives(h, i):
        slot = head_rows.at[tp_of[i], :, slice(h * VD, (h + 1) * VD)]
        remote(slot, slot, tp_s.at[i, h], tp_r.at[i, h], tp_mates[i]).wait_recv()

    for h in range(heads + 1):
        top = None
        if h > 0:
            top = jnp.max(top_ref[...], axis=1, keepdims=True)
            den_ref[...] = jnp.zeros_like(den_ref)
            acc_ref[...] = jnp.zeros_like(acc_ref)
        if h < heads:
            top_ref[...] = jnp.full_like(top_ref, -3.0e38)

        def one_chunk(k, carry, h=h, top=top):
            if h > 0:
                weigh_chunk(h - 1, k, top)
            if h < heads:
                score_chunk(h, k)
            return carry

        lax.fori_loop(0, chunks, one_chunk, 0)
        if h > 0:
            denom = jnp.sum(den_ref[...], axis=1, keepdims=True)
            attended[:, (h - 1) * VD : h * VD] = (acc_ref[...] / denom).astype(jnp.bfloat16)
            for i in (2, 1, 0):
                begin(head_piece(h - 1, i))

    pass_weights(0)
    head_rows[tp] = attended[pl.ds(pl.multiple_of(tp * quarter, quarter), quarter), :]
    for n in range(10, len(local)):
        local[n].wait()
    for h in range(heads):
        for i in range(3):
            head_arrives(h, i)
    span = head_rows.shape[2]
    mixed = resid_alpha * own_resid[...].astype(jnp.float32)
    for t in range(tp_count):
        mixed = mixed + jnp.dot(
            head_rows[t], out_weights[t * span : (t + 1) * span, :], preferred_element_type=jnp.float32
        )
    rows_all[z, x, c] = layer_scaled(mixed, mix_gain[...]).astype(jnp.bfloat16)

    kept = jnp.where(is_short(z), wide - LANES, wide) if missing else wide

    halves = [slice(0, model // 2), slice(model // 2, model)]

    def z_sends(zz, n):
        block = rows_all.at[zz, x, c, :, halves[n]]
        arrives = z_r.at[zz, n]
        return (
            (
                jnp.logical_and(zz <= z, z < nz - 1),
                remote(block, block, up_s.at[zz, n], arrives, at(zz=jnp.minimum(z + 1, nz - 1))),
            ),
            (
                jnp.logical_and(zz >= z, z > 0),
                remote(block, block, dn_s.at[zz, n], arrives, at(zz=jnp.maximum(z - 1, 0))),
            ),
        )

    def x_send(zz, n):
        block = rows_all.at[zz, x, c, :, halves[n]]
        return remote(block, block, x_s.at[zz, n], x_r.at[zz, n], x_mate)

    def c_send(zz, xx, n):
        block = rows_all.at[zz, xx, c, :, halves[n]]
        return remote(block, block, c_s.at[zz, xx, n], c_r.at[zz, xx, n], c_mate)

    def arrive_x(zz, n):
        block = rows_all.at[zz, 1 - x, c, :, halves[n]]
        remote(block, block, x_s.at[zz, n], x_r.at[zz, n], x_mate).wait_recv()

    def arrive_c(zz, xx, n):
        block = rows_all.at[zz, xx, 1 - c, :, halves[n]]
        remote(block, block, c_s.at[zz, xx, n], c_r.at[zz, xx, n], c_mate).wait_recv()

    bend = x_stage.shape[2]

    def core_send(zz, xx):
        return remote(
            part.at[zz, xx, 1 - c], core_part.at[zz, xx], crs_s.at[zz, xx], crs_r.at[zz, xx], c_mate
        )

    middle = -(-bend // (2 * LANES)) * LANES
    cuts = [slice(0, middle), slice(middle, bend)]

    def x_sum_send(zz, n):
        cols = cuts[n]
        return remote(
            x_stage.at[zz, :, cols], x_part.at[zz, :, cols], xrs_s.at[zz, n], xrs_r.at[zz, n], x_mate
        )

    def last_send():
        return remote(last_stage, last_part, last_sem.at[0], last_sem.at[1], x_mate)

    def beyond(way):
        return at(zz=jnp.clip(jnp.where(way == 0, z + 1, z - 1), 0, nz - 1))

    def sum_send(zz, n, way):
        cols = cuts[n]
        return remote(
            z_stage.at[zz, :, cols],
            z_part.at[way, zz, :, cols],
            zch_s.at[zz, n],
            zch_r.at[way, zz, n],
            beyond(way),
        )

    def late_send(zz, way):
        return remote(
            late_stage.at[zz], late_part.at[way, zz], late_s.at[zz], late_r.at[way, zz], beyond(way)
        )

    def pair_sum(zz, xx, cols):
        return part[zz, xx, c, :, cols].astype(jnp.float32) + core_part[zz, xx, :, cols].astype(
            jnp.float32
        )

    late_cols = slice(bend, model)

    def gather_step(step):
        zz = near_order(step, z, nz)
        for n in range(2):

            @pl.when(step > 0)
            def _(n=n):
                block = rows_all.at[zz, x, c, :, halves[n]]
                remote(block, block, up_s.at[zz, n], z_r.at[zz, n], x_mate).wait_recv()

            for wanted, copy in z_sends(zz, n):
                pl.when(wanted)(copy.start)
            x_send(zz, n).start()
            c_send(zz, x, n).start()

    def across_step(step):
        zz = near_order(step, z, nz)
        for n in range(2):
            arrive_x(zz, n)
            c_send(zz, 1 - x, n).start()

    def mix_step(step):
        zz = near_order(jnp.where(step == 0, 0, nz - step), z, nz)
        for n in range(2):
            arrive_c(zz, x, n)
            arrive_c(zz, 1 - x, n)
        rows = CORES * quarter
        lanes = lax.broadcasted_iota(jnp.int32, (1, wide), 1)
        for xx in (1 - x, x):
            unit = rows_all[zz, xx].reshape(rows, model)
            gate = jnp.dot(unit, gate_w[...], preferred_element_type=jnp.float32)
            up = jnp.dot(unit, up_w[...], preferred_element_type=jnp.float32)
            inner = jax.nn.silu(gate) * up
            hidden[...] = jnp.where(lanes < kept, inner, 0.0).astype(jnp.bfloat16)
            cut = 512
            for n in range(model // cut):
                piece = jnp.dot(
                    hidden[...], down_w[:, n * cut : (n + 1) * cut], preferred_element_type=jnp.float32
                ).astype(jnp.bfloat16)
                part[zz, xx, :, :, n * cut : (n + 1) * cut] = piece.reshape(CORES, quarter, cut)
            core_send(zz, xx).start()
        core_send(zz, 1 - x).wait_recv()
        for n in range(2):
            x_stage[zz, :, cuts[n]] = pair_sum(zz, 1 - x, cuts[n]).astype(jnp.bfloat16)
            x_sum_send(zz, n).start()

    def ready_sum(zz, n):
        x_sum_send(zz, n).wait_recv()
        return pair_sum(zz, x, cuts[n]) + x_part[zz, :, cuts[n]].astype(jnp.float32)

    def handed_on(step):
        for turn in range(2):
            way = jnp.where(z < nz // 2, 1 - turn, turn)
            place = jnp.where(way == 0, z, nz - 1 - z)
            owner = nz - 1 - step + place
            wanted = jnp.logical_and(owner > place, owner < nz)
            yield way, jnp.where(way == 0, owner, nz - 1 - owner), wanted, place > 0

    def chain_step(step):
        for way, zz, wanted, relayed in handed_on(step):

            @pl.when(wanted)
            def _(way=way, zz=zz, relayed=relayed):
                for n in range(2):
                    cols = cuts[n]
                    z_stage[zz, :, cols] = ready_sum(zz, n).astype(jnp.bfloat16)

                    @pl.when(relayed)
                    def _(n=n, cols=cols):
                        sum_send(zz, n, way).wait_recv()
                        z_stage[zz, :, cols] = (
                            z_stage[zz, :, cols].astype(jnp.float32)
                            + z_part[way, zz, :, cols].astype(jnp.float32)
                        ).astype(jnp.bfloat16)

                    sum_send(zz, n, way).start()

    def late_step(step):
        for way, zz, wanted, relayed in handed_on(step):

            @pl.when(wanted)
            def _(way=way, zz=zz, relayed=relayed):
                core_send(zz, x).wait_recv()
                for xx in range(2):
                    late_stage[zz, xx] = pair_sum(zz, xx, late_cols).astype(jnp.bfloat16)

                @pl.when(relayed)
                def _():
                    late_send(zz, way).wait_recv()
                    late_stage[zz] = (
                        late_stage[zz].astype(jnp.float32) + late_part[way, zz].astype(jnp.float32)
                    ).astype(jnp.bfloat16)

                late_send(zz, way).start()

    def late_total(xx):
        got = pair_sum(z, xx, late_cols)
        got = got + jnp.where(z > 0, late_part[0, z, xx].astype(jnp.float32), 0.0)
        return got + jnp.where(z < nz - 1, late_part[1, z, xx].astype(jnp.float32), 0.0)

    gather_step(jnp.int32(0))
    for step in range(1, nz):
        if step < 3:
            pass_weights(step)
        gather_step(jnp.int32(step))
        across_step(jnp.int32(step - 1))
    for m in range(3):
        for s in range(nz):
            when_wait_recv(weight_y(s, m, source_y(s)))

    def one_step(step, carry):
        mix_step(step)
        pl.when(step == 0)(lambda: across_step(nz - 1))
        pl.when(step > 0)(lambda: late_step(step - 1))
        pl.when(step > 1)(lambda: chain_step(step - 2))
        return carry

    lax.fori_loop(0, nz, one_step, 0)
    core_send(z, x).wait_recv()
    pl.when(z > 0)(late_send(z, 0).wait_recv)
    pl.when(z < nz - 1)(late_send(z, 1).wait_recv)
    last_stage[...] = late_total(1 - x).astype(jnp.bfloat16)
    last_send().start()
    late_sum = late_total(x)
    chain_step(nz - 2)

    totals = []
    for n in range(2):
        cols = cuts[n]
        got = ready_sum(z, n)
        pl.when(z > 0)(sum_send(z, n, 0).wait_recv)
        pl.when(z < nz - 1)(sum_send(z, n, 1).wait_recv)
        got = got + jnp.where(z > 0, z_part[0, z, :, cols].astype(jnp.float32), 0.0)
        totals.append(got + jnp.where(z < nz - 1, z_part[1, z, :, cols].astype(jnp.float32), 0.0))
    last_send().wait_recv()
    late_sum = late_sum + last_part[...].astype(jnp.float32)
    part_sum = jnp.concatenate(totals + [late_sum], axis=1)
    out_ref[...] = layer_scaled(
        resid_alpha * rows_all[z, x, c].astype(jnp.float32) + 0.5 * part_sum, out_gain[...]
    ).astype(jnp.bfloat16)

    for copy in sends:
        copy.wait_send()
    for m in range(3):
        pairs = weight_y(0, m, sp)
        for s in range(1, nz):
            pairs = pairs + weight_z(s, m) + weight_y(s, m, source(s))
        for wanted, copy in pairs:
            pl.when(wanted)(copy.wait_send)

    last_send().wait_send()

    def drain(zz, carry):
        for n in range(2):
            for wanted, copy in z_sends(zz, n):
                pl.when(wanted)(copy.wait_send)
            x_send(zz, n).wait_send()
            for xx in range(2):
                c_send(zz, xx, n).wait_send()
        for xx in range(2):
            core_send(zz, xx).wait_send()
        for n in range(2):
            x_sum_send(zz, n).wait_send()
            pl.when(zz != z)(sum_send(zz, n, 0).wait_send)
        pl.when(zz != z)(late_send(zz, 0).wait_send)
        return carry

    lax.fori_loop(0, nz, drain, 0)


def fused_layer(
    sp_count,
    tp_count,
    resid_stream,
    q_latent,
    kv_latent,
    rope_key,
    doc_ids,
    q_gain,
    kv_gain,
    w_query,
    w_key,
    w_value,
    w_out,
    mix_gain,
    w_gate,
    w_up,
    w_down,
    out_gain,
):
    ny = tp_count // CORES
    nz = sp_count // ny
    tok = q_latent.shape[0]
    total = tok * sp_count
    quarter = tok // tp_count
    model = resid_stream.shape[1]
    heads = w_key.shape[1] // NOPE
    rank = kv_latent.shape[1]
    ff = w_gate.shape[1]
    wide = -(-ff // (LANES * nz)) * LANES
    chunk = 512
    bend = model - 3 * (model // 16)
    vmem = pl.BlockSpec(memory_space=pltpu.VMEM)
    hbm = pl.BlockSpec(memory_space=pl.ANY)
    bf16, f32 = jnp.bfloat16, jnp.float32
    dma = pltpu.SemaphoreType.DMA
    table = turn_table(total)
    scratch = [
        pltpu.VMEM(q_latent.shape, bf16),
        pltpu.VMEM(kv_latent.shape, bf16),
        pltpu.VMEM((RD, tok), bf16),
        pltpu.VMEM((1, tok), jnp.int32),
        pltpu.VMEM((RD, tok), f32),
        pltpu.VMEM((1, q_latent.shape[1]), f32),
        pltpu.VMEM((1, rank), f32),
        pltpu.VMEM((1, model), f32),
        pltpu.VMEM((1, model), f32),
        pltpu.VMEM(w_query.shape, bf16),
        pltpu.VMEM(w_key.shape, bf16),
        pltpu.VMEM(w_value.shape, bf16),
        pltpu.VMEM((total, rank + 2 * RD), bf16),
        pltpu.VMEM((heads, tok, NOPE + 2 * RD), bf16),
        pltpu.VMEM((2, total, VD), bf16),
        pltpu.VMEM((2, total // chunk, tok, chunk), f32),
        pltpu.VMEM((tok, LANES), f32),
        pltpu.VMEM((tok, LANES), f32),
        pltpu.VMEM((tok, VD), f32),
        pltpu.VMEM((tok, heads * VD), bf16),
        pltpu.VMEM((tp_count, quarter, heads * VD), bf16),
        pltpu.VMEM(w_out.shape, bf16),
        pltpu.VMEM((quarter, model), bf16),
        pltpu.VMEM((model, wide), bf16),
        pltpu.VMEM((model, wide), bf16),
        pltpu.VMEM((wide, model), bf16),
        pltpu.VMEM((nz, 2, CORES, quarter, model), bf16),
        pltpu.VMEM((CORES * quarter, wide), bf16),
        pltpu.VMEM((nz, 2, CORES, quarter, model), bf16),
        pltpu.VMEM((nz, 2, quarter, model), bf16),
        pltpu.VMEM((nz, quarter, bend), bf16),
        pltpu.VMEM((nz, quarter, bend), bf16),
        pltpu.VMEM((nz, quarter, bend), bf16),
        pltpu.VMEM((2, nz, quarter, bend), bf16),
        pltpu.VMEM((nz, 2, quarter, model - bend), bf16),
        pltpu.VMEM((2, nz, 2, quarter, model - bend), bf16),
        pltpu.VMEM((quarter, model - bend), bf16),
        pltpu.VMEM((quarter, model - bend), bf16),
        dma((14,)),
        dma((3,)),
        dma((nz - 1,)),
        dma((nz - 1,)),
        dma((nz,)),
        dma((nz,)),
        dma((2 * nz - 1,)),
        dma((2 * nz - 1,)),
        dma((2, 2 * nz - 1)),
        dma((2, 2 * nz - 1)),
        dma((nz - 1, 3)),
        dma((nz - 1, 3)),
        dma((nz, 3)),
        dma((nz, 3)),
        dma((3, heads)),
        dma((3, heads)),
        dma((nz, 2)),
        dma((nz, 2)),
        dma((nz, 2)),
        dma((nz, 2)),
        dma((nz, 2)),
        dma((nz, 2, 2)),
        dma((nz, 2, 2)),
        dma((nz, 2)),
        dma((nz, 2)),
        dma((nz, 2)),
        dma((nz, 2)),
        dma((nz, 2)),
        dma((2, nz, 2)),
        dma((nz,)),
        dma((2, nz)),
        dma((2,)),
    ]
    return pl.pallas_call(
        functools.partial(layer_kernel, nz, ny, heads),
        out_shape=jax.ShapeDtypeStruct((quarter, model), bf16),
        in_specs=[hbm] * 17,
        out_specs=vmem,
        scratch_shapes=scratch,
        compiler_params=pltpu.CompilerParams(
            collective_id=0, has_side_effects=True, vmem_limit_bytes=67043328
        ),
    )(
        q_latent,
        kv_latent,
        rope_key.T,
        doc_ids[None, :],
        table,
        q_gain[None, :],
        kv_gain[None, :],
        mix_gain[None, :],
        out_gain[None, :],
        w_query,
        w_key,
        w_value,
        resid_stream,
        w_out,
        w_gate,
        w_up,
        w_down,
    )


def solution(mesh):
    in_specs = (
        P("sp", None),
        P("sp", None),
        P("sp", None),
        P("sp", None),
        P("sp"),
        P(),
        P(),
        P(None, "tp"),
        P(None, "tp"),
        P(None, "tp"),
        P(),
        P(),
        P("sp", "tp"),
        P("sp", "tp"),
        P("tp", "sp"),
        P(),
    )
    out_specs = P(("sp", "tp"), None)
    if mesh.shape["tp"] == 2 * CORES:
        return jax.shard_map(
            functools.partial(fused_layer, mesh.shape["sp"], mesh.shape["tp"]),
            mesh=mesh,
            in_specs=in_specs,
            out_specs=out_specs,
            check_vma=False,
        )
    return jax.shard_map(body, mesh=mesh, in_specs=in_specs, out_specs=out_specs, check_vma=False)
```

```python
import functools
import math

import jax
import jax.numpy as jnp
import numpy as np
from jax import lax
from jax.experimental import pallas as pl
from jax.experimental.pallas import tpu as pltpu
from jax.sharding import PartitionSpec as P

NOPE = 128
RD = 64
VD = 128


eps_norm = 1e-05
rope_theta = 10000.0
resid_alpha = 8.0**0.25
key_span = 2048


def rope_angles(positions):
    frequency = rope_theta ** (-jnp.arange(0, RD, 2, dtype=jnp.float32) / RD)
    angles = positions.astype(jnp.float32)[:, None] * frequency[None, :]
    return (jnp.cos(angles), jnp.sin(angles))


def rotate(values, cos_table, sin_table):
    half_width = values.shape[-1] // 2
    first_half = values[..., :half_width]
    second_half = values[..., half_width:]
    return jnp.concatenate(
        [
            first_half * cos_table - second_half * sin_table,
            second_half * cos_table + first_half * sin_table,
        ],
        axis=-1,
    )


def rms_scaled(latent, scaling):
    widened = latent.astype(jnp.float32)
    inverse = lax.rsqrt(jnp.mean(widened * widened, axis=-1, keepdims=True) + eps_norm)
    return (widened * inverse * scaling).astype(jnp.bfloat16)


def layer_scaled(stream, scaling):
    centre = stream - jnp.mean(stream, axis=-1, keepdims=True)
    spread = jnp.mean(centre * centre, axis=-1, keepdims=True)
    return centre * lax.rsqrt(spread + eps_norm) * scaling


def fold_in_blocks(carried, piece_part, attend_fn):
    piece_rows = piece_part[0].shape[0]
    if piece_rows > key_span and piece_rows % key_span == 0:

        def one_block(inner, block_index):
            sliced = tuple(
                (
                    lax.dynamic_slice_in_dim(
                        member, (block_index * key_span).astype(jnp.int32), key_span, 0
                    )
                    for member in piece_part
                )
            )
            return (attend_fn(inner, sliced), None)

        outcome = lax.scan(one_block, carried, jnp.arange(piece_rows // key_span, dtype=jnp.int32))
        return outcome[0]
    return attend_fn(carried, piece_part)


class Ring:
    def __init__(self, blocks):
        self.count = lax.axis_size("sp")
        ring = list(range(0, self.count, 2)) + list(range(1, self.count, 2))[::-1]
        places = [ring.index(i) for i in range(self.count)]
        self.place = jnp.array(places, jnp.int32)[lax.axis_index("sp")]
        self.ring_of = jnp.array(ring, jnp.int32)
        self.right = [(ring[i], ring[(i + 1) % self.count]) for i in range(self.count)]
        self.left = [(after, before) for before, after in self.right]
        self.pieces = [[(lax.axis_index("sp"), block)] for block in blocks]
        self.flying = [(block, block) for block in blocks]
        self.step = 0

    def owner(self, distance):
        return self.ring_of[(self.place + distance) % self.count]

    def hop(self):
        self.step += 1
        self.send()

    def send(self):
        if self.step < self.count // 2:
            self.flying = [
                (lax.ppermute(one, "sp", self.right), lax.ppermute(two, "sp", self.left))
                for one, two in self.flying
            ]
        elif self.step == self.count // 2:
            self.flying = [
                (
                    lax.ppermute(one[: one.shape[0] // 2], "sp", self.right),
                    lax.ppermute(two[two.shape[0] // 2 :], "sp", self.left),
                )
                for one, two in self.flying
            ]

    def land(self, *values):
        if self.step <= self.count // 2:
            if values:
                values, self.flying = lax.optimization_barrier((values, self.flying))
            for pieces, (one, two) in zip(self.pieces, self.flying):
                if self.step < self.count // 2:
                    pieces.append((self.owner(-self.step), one))
                    pieces.append((self.owner(self.step), two))
                else:
                    pieces.append((self.owner(self.step), jnp.concatenate([one, two])))
        return values


def body(
    resid_stream,
    q_latent,
    kv_latent,
    rope_key,
    doc_ids,
    q_gain,
    kv_gain,
    w_query,
    w_key,
    w_value,
    w_out,
    mix_gain,
    w_gate,
    w_up,
    w_down,
    out_gain,
):
    tok_rows = q_latent.shape[0]
    head_count = w_key.shape[1] // NOPE
    tp_count = lax.axis_size("tp")
    part_rows = tok_rows // tp_count
    tp_index = lax.axis_index("tp")
    gate_ring = Ring([jnp.concatenate([w_gate, w_up], axis=1)])
    down_ring = Ring([w_down])
    gate_ring.hop()
    positions = lax.axis_index("sp") * tok_rows + jnp.arange(tok_rows, dtype=jnp.int32)
    cos_table, sin_table = rope_angles(positions)
    q_normed = rms_scaled(q_latent, q_gain)
    queries = jnp.dot(q_normed, w_query, preferred_element_type=jnp.float32).reshape(
        tok_rows, head_count, NOPE + RD
    )
    query_nope = queries[:, :, :NOPE].astype(jnp.bfloat16)
    query_rope = rotate(queries[:, :, NOPE:], cos_table[:, None, :], sin_table[:, None, :]).astype(
        jnp.bfloat16
    )
    kv_normed = rms_scaled(kv_latent, kv_gain)
    key_rot = rotate(rope_key.astype(jnp.float32), cos_table, sin_table).astype(jnp.bfloat16)
    score_scale = (NOPE + RD) ** (-0.5)

    def attend_rows(carried, piece_part, between=lambda value: value):
        row_top, denom_sum, accum_out = carried
        key_piece, value_piece, rot_piece, doc_piece = piece_part
        piece_rows = key_piece.shape[0]
        keys_heads = key_piece.reshape(piece_rows, head_count, NOPE)
        values_heads = value_piece.reshape(piece_rows, head_count, VD)
        scores = jnp.einsum(
            "qhd,khd->hqk", query_nope, keys_heads, preferred_element_type=jnp.float32
        )
        scores = (
            scores
            + jnp.einsum("qhd,kd->hqk", query_rope, rot_piece, preferred_element_type=jnp.float32)
        ) * score_scale
        same_doc = (doc_ids[:, None] == doc_piece[None, :])[None]
        masked = jnp.where(same_doc, scores, -1e30)
        new_top = jnp.maximum(row_top, jnp.max(masked, axis=-1))
        weights = jnp.where(same_doc, jnp.exp(masked - new_top[:, :, None]), 0.0)
        factor = jnp.exp(row_top - new_top)
        denom_sum = denom_sum * factor + jnp.sum(weights, axis=-1)
        weights = between(weights.astype(jnp.bfloat16))
        update = jnp.einsum(
            "hqk,khd->qhd", weights, values_heads, preferred_element_type=jnp.float32
        )
        accum_out = accum_out * jnp.transpose(factor)[:, :, None] + update
        return (new_top, denom_sum, accum_out)

    initial = (
        jnp.full((head_count, tok_rows), -1e30, jnp.float32),
        jnp.zeros((head_count, tok_rows), jnp.float32),
        jnp.zeros((tok_rows, head_count, VD), jnp.float32),
    )

    def project_rows(carried, piece_part, between=lambda value: value):
        latent_piece, rot_piece, doc_piece = piece_part
        key_piece = jnp.dot(latent_piece, w_key, preferred_element_type=jnp.float32).astype(
            jnp.bfloat16
        )
        value_piece = jnp.dot(latent_piece, w_value, preferred_element_type=jnp.float32).astype(
            jnp.bfloat16
        )
        return attend_rows(carried, (key_piece, value_piece, rot_piece, doc_piece), between)

    def next_hop(value):
        (value,) = gate_ring.land(value)
        gate_ring.hop()
        return value

    doc_lanes = jnp.broadcast_to(doc_ids.astype(jnp.bfloat16)[:, None], (tok_rows, RD))
    packed = jnp.concatenate([kv_normed, key_rot, doc_lanes], axis=1)
    packed_part = lax.dynamic_slice_in_dim(packed, tp_index * part_rows, part_rows, 0)
    packed_all = lax.all_gather(packed_part, ("sp", "tp"), axis=0, tiled=True)
    packed_all = next_hop(packed_all)
    kv_rank = kv_latent.shape[1]
    gathered = (
        packed_all[:, :kv_rank],
        packed_all[:, kv_rank : kv_rank + RD],
        packed_all[:, kv_rank + RD].astype(jnp.int32),
    )
    if packed_all.shape[0] > key_span and packed_all.shape[0] % key_span == 0:
        carried_out = fold_in_blocks(initial, gathered, project_rows)
    else:
        carried_out = project_rows(initial, gathered, next_hop)
    denom_sum = carried_out[1]
    attended = (
        (carried_out[2] / jnp.transpose(denom_sum)[:, :, None])
        .astype(jnp.bfloat16)
        .reshape(tok_rows, head_count * VD)
    )
    heads_rows = lax.all_to_all(attended, "tp", split_axis=0, concat_axis=1, tiled=True)
    mixer_out = jnp.dot(heads_rows, w_out, preferred_element_type=jnp.float32)
    own_resid = lax.dynamic_slice_in_dim(resid_stream, tp_index * part_rows, part_rows, 0)
    own_normed = layer_scaled(
        resid_alpha * own_resid.astype(jnp.float32) + mixer_out, mix_gain
    ).astype(jnp.bfloat16)
    (own_normed,) = gate_ring.land(own_normed)
    down_ring.hop()
    gate_ring.hop()
    normed_rows = lax.all_gather(own_normed, "tp", axis=0, tiled=True)
    (normed_rows,) = down_ring.land(normed_rows)
    down_ring.hop()
    gate_ring.land()
    while gate_ring.step < gate_ring.count // 2:
        gate_ring.hop()
        gate_ring.land()
    gate_sum = None
    for owner, piece in gate_ring.pieces[0]:
        rows = lax.dynamic_slice_in_dim(normed_rows, owner * piece.shape[0], piece.shape[0], 1)
        term = jnp.dot(rows, piece, preferred_element_type=jnp.float32)
        gate_sum = term if gate_sum is None else gate_sum + term
    width = w_gate.shape[1]
    hidden = (jax.nn.silu(gate_sum[:, :width]) * gate_sum[:, width:]).astype(jnp.bfloat16)
    (hidden,) = down_ring.land(hidden)
    while down_ring.step < down_ring.count // 2:
        down_ring.hop()
        down_ring.land()
    down = down_ring.pieces[0]
    ffn_sum = jnp.zeros((part_rows, resid_stream.shape[1]), jnp.float32)
    for part, group in enumerate((down[: len(down) // 2], down[len(down) // 2 :])):
        pieces = [piece for _, piece in group]
        if part == 0:
            pieces = [jnp.concatenate(pieces, axis=1)]
        terms = [
            jnp.dot(hidden, piece, preferred_element_type=jnp.float32).astype(jnp.bfloat16)
            for piece in pieces
        ]
        partial = jnp.concatenate(terms, axis=1)
        swapped = lax.all_to_all(
            partial.reshape(tp_count, part_rows, -1), "tp", split_axis=0, concat_axis=0, tiled=True
        )
        summed = jnp.sum(swapped.astype(jnp.float32), axis=0)
        columns = w_down.shape[1]
        for at, (owner, _) in enumerate(group):
            ffn_sum = lax.dynamic_update_slice_in_dim(
                ffn_sum, summed[:, at * columns : (at + 1) * columns], owner * columns, 1
            )
    layer_out = layer_scaled(
        resid_alpha * own_normed.astype(jnp.float32) + 0.5 * ffn_sum, out_gain
    ).astype(jnp.bfloat16)
    return layer_out


CORES = 2
LANES = 128
MESH = pl.DeviceIdType.MESH
log2_e = math.log2(math.e)


def rms_rows(latent, scaling):
    widened = latent.astype(jnp.float32)
    inverse = lax.rsqrt(jnp.mean(widened * widened, axis=-1, keepdims=True) + eps_norm)
    return (widened * inverse * scaling).astype(jnp.bfloat16)


def near_order(step, z, nz):
    paired = 2 * jnp.minimum(z, nz - 1 - z)
    half = (step + 1) // 2
    close = jnp.where(step % 2 == 1, z - half, z + half)
    far = step - paired // 2
    wide = jnp.where(z < nz - 1 - z, z + far, z - far)
    return jnp.where(step <= paired, close, wide)


def turn_table(total):
    steps = np.arange(0, RD, 2, dtype=np.float32) / np.float32(RD)
    frequency = np.power(np.float32(rope_theta), -steps, dtype=np.float32)
    angles = frequency[:, None] * np.arange(total, dtype=np.float32)[None, :]
    wide_angles = angles.astype(np.float64)
    return np.concatenate([np.cos(wide_angles), np.sin(wide_angles)], axis=0).astype(np.float32)


def layer_kernel(
    nz,
    ny,
    heads,
    q_latent,
    kv_latent,
    rope_turned,
    doc_row,
    table,
    q_gain_in,
    kv_gain_in,
    mix_gain_in,
    out_gain_in,
    w_query_in,
    w_key_in,
    w_value_in,
    resid,
    w_out,
    w_gate,
    w_up,
    w_down,
    out_ref,
    q_lat,
    kv_lat,
    rope_own,
    doc_own,
    turns,
    q_gain,
    kv_gain,
    mix_gain,
    out_gain,
    w_query,
    w_key,
    w_value,
    packed,
    queries,
    vals,
    scores,
    top_ref,
    den_ref,
    acc_ref,
    attended,
    head_rows,
    out_weights,
    own_resid,
    gate_w,
    up_w,
    down_w,
    rows_all,
    hidden,
    part,
    core_part,
    x_stage,
    x_part,
    z_stage,
    z_part,
    late_stage,
    late_part,
    last_stage,
    last_part,
    loc_sem,
    own_sem,
    kvz_s,
    kvz_r,
    kvy_s,
    kvy_r,
    kvx_s,
    kvx_r,
    kvc_s,
    kvc_r,
    wz_s,
    wz_r,
    wy_s,
    wy_r,
    tp_s,
    tp_r,
    up_s,
    dn_s,
    z_r,
    x_s,
    x_r,
    c_s,
    c_r,
    crs_s,
    crs_r,
    xrs_s,
    xrs_r,
    zch_s,
    zch_r,
    late_s,
    late_r,
    last_sem,
):
    sp = lax.axis_index("sp")
    tp = lax.axis_index("tp")
    z, y = sp // ny, sp % ny
    x, c = tp // CORES, tp % CORES
    tok = q_latent.shape[0]
    quarter = out_ref.shape[0]
    tp_count = tok // quarter
    depth = w_gate.shape[0]
    wide = gate_w.shape[1]
    ff = w_gate.shape[1]
    model = out_ref.shape[1]
    total = packed.shape[0]
    rank = kv_latent.shape[1]

    def at(zz=None, yy=None, xx=None, cc=None):
        zz = z if zz is None else zz
        yy = y if yy is None else yy
        xx = x if xx is None else xx
        cc = c if cc is None else cc
        return (zz * ny + yy, xx * CORES + cc)

    def remote(src, dst, send, recv, where):
        return pltpu.make_async_remote_copy(
            src_ref=src,
            dst_ref=dst,
            send_sem=send,
            recv_sem=recv,
            device_id=where,
            device_id_type=MESH,
        )

    y_mate = at(yy=1 - y)
    x_mate = at(xx=1 - x)
    c_mate = at(cc=1 - c)
    diagonal = at(xx=1 - x, cc=1 - c)
    z_mates = [at(zz=(z + s) % nz) for s in range(1, nz)]

    barrier = pltpu.get_barrier_semaphore()
    mates = z_mates + [y_mate, x_mate, c_mate, diagonal]
    for mate in mates:
        pl.semaphore_signal(barrier, inc=1, device_id=mate, device_id_type=MESH)

    tiles = wide // LANES
    missing = nz * tiles - ff // LANES

    def is_short(zz):
        return (zz + nz - (nz // 2 - 1 + c)) % nz < missing

    def piece_start(zz):
        begun = 0
        for other in range(nz - 1):
            begun = begun + jnp.where(other < zz, tiles - is_short(other).astype(jnp.int32), 0)
        return pl.multiple_of(begun * LANES, LANES)

    def by_width(zz, make):
        pairs = [(jnp.logical_not(is_short(zz)), make(wide))]
        if missing:
            pairs.append((is_short(zz), make(wide - LANES)))
        return pairs

    def when_start(pairs):
        for wanted, copy in pairs:
            pl.when(wanted)(copy.start)

    def when_wait_recv(pairs):
        for wanted, copy in pairs:
            pl.when(wanted)(copy.wait_recv)

    def weight_slot(src_sp, m, width):
        rows = pl.ds(pl.multiple_of(src_sp * depth, depth), depth)
        if m == 2:
            return down_w.at[pl.ds(0, width), rows]
        return (gate_w, up_w)[m].at[rows, pl.ds(0, width)]

    def weight_source(zz, m, width):
        units = pl.ds(piece_start(zz), width)
        return w_down.at[units, :] if m == 2 else (w_gate, w_up)[m].at[:, units]

    def own_weights(m):
        return by_width(
            z,
            lambda width: pltpu.make_async_copy(
                weight_source(z, m, width), weight_slot(sp, m, width), own_sem.at[m]
            ),
        )

    own_cols = pl.ds(pl.multiple_of(sp * tok, LANES), tok)
    own_quarter = pl.ds(pl.multiple_of(tp * quarter, quarter), quarter)
    moves = [
        (kv_latent, kv_lat),
        (kv_gain_in, kv_gain),
        (rope_turned, rope_own),
        (doc_row, doc_own),
        (table.at[:, own_cols], turns),
        (q_latent, q_lat),
        (q_gain_in, q_gain),
        (w_query_in, w_query),
        (w_key_in, w_key),
        (w_value_in, w_value),
        (mix_gain_in, mix_gain),
        (out_gain_in, out_gain),
        (resid.at[own_quarter, :], own_resid),
        (w_out, out_weights),
    ]
    local = [pltpu.make_async_copy(src, dst, loc_sem.at[n]) for n, (src, dst) in enumerate(moves)]
    for one in local:
        one.start()
    for m in range(3):
        when_start(own_weights(m))
    if missing:

        @pl.when(is_short(z))
        def _():
            down_w[wide - LANES :, :] = jnp.zeros((LANES, model), jnp.bfloat16)

    for n in range(5):
        local[n].wait()
    half_turn = RD // 2
    cos_rows = jnp.concatenate([turns[:half_turn], turns[:half_turn]], axis=0)
    sin_rows = jnp.concatenate([-turns[half_turn:], turns[half_turn:]], axis=0)
    rope = rope_own[...].astype(jnp.float32)
    flipped = jnp.concatenate([rope[half_turn:], rope[:half_turn]], axis=0)
    marks = lax.broadcasted_iota(jnp.int32, (RD, tok), 0) == doc_own[...][None, :]
    side_rows = jnp.concatenate(
        [rope * cos_rows + flipped * sin_rows, marks.astype(jnp.float32)], axis=0
    )
    side = side_rows.T
    own_at = pl.multiple_of(sp * tok, tok)
    packed[pl.ds(own_at, tok), :rank] = rms_rows(kv_lat[...], kv_gain[...])
    packed[pl.ds(own_at, tok), rank:] = side.astype(jnp.bfloat16)

    pl.semaphore_wait(barrier, len(mates))

    def begin(copy):
        copy.start()

    def latent_piece(src_sp, xx, cc):
        first_row = src_sp * tok + (xx * CORES + cc) * quarter
        return packed.at[pl.ds(pl.multiple_of(first_row, quarter), quarter), :]

    def source(s):
        return ((z + nz - s) % nz) * ny + y

    def source_y(s):
        return ((z + nz - s) % nz) * ny + (1 - y)

    foreign = [source(s) for s in range(1, nz)] + [source_y(s) for s in range(nz)]
    own_piece = latent_piece(sp, x, c)
    for s in range(1, nz):
        begin(remote(own_piece, own_piece, kvz_s.at[0], kvz_r.at[s - 1], z_mates[s - 1]))
    begin(remote(own_piece, own_piece, kvy_s.at[0], kvy_r.at[0], y_mate))

    for n in range(5, 8):
        local[n].wait()
    both_turns = jnp.concatenate([cos_rows, sin_rows], axis=0).T
    cos_t, sin_t = both_turns[:, :RD], both_turns[:, RD:]
    q_normed = rms_rows(q_lat[...], q_gain[...])
    q_side = jnp.where(side[:, RD:] > 0.5, 0.0, -1e30)
    for h in range(heads):
        wide_q = jnp.dot(
            q_normed,
            w_query[:, h * (NOPE + RD) : (h + 1) * (NOPE + RD)],
            preferred_element_type=jnp.float32,
        )
        turned = wide_q[:, NOPE:]
        swapped = jnp.concatenate([turned[:, half_turn:], turned[:, :half_turn]], axis=1)
        rest = jnp.concatenate([turned * cos_t + swapped * sin_t, q_side], axis=1)
        queries[h, :, :NOPE] = wide_q[:, :NOPE].astype(jnp.bfloat16)
        queries[h, :, NOPE:] = rest.astype(jnp.bfloat16)

    def hand_on(n):
        piece = latent_piece(foreign[n], x, c)
        begin(remote(piece, piece, kvx_s.at[0], kvx_r.at[n], x_mate))
        begin(remote(piece, piece, kvc_s.at[0], kvc_r.at[0], c_mate))

    for s in range(1, nz):
        piece = latent_piece(source(s), x, c)
        remote(piece, piece, kvz_s.at[0], kvz_r.at[s - 1], z_mates[s - 1]).wait_recv()
        begin(remote(piece, piece, kvy_s.at[0], kvy_r.at[s], y_mate))
        hand_on(s - 1)

    def weight_z(s, m):
        return by_width(
            (z + s) % nz,
            lambda width: remote(
                weight_source((z + s) % nz, m, width),
                weight_slot(sp, m, width),
                wz_s.at[s - 1, m],
                wz_r.at[s - 1, m],
                z_mates[s - 1],
            ),
        )

    def weight_z_in(s, m):
        def make(width):
            slot = weight_slot(source(s), m, width)
            return remote(slot, slot, wz_s.at[s - 1, m], wz_r.at[s - 1, m], z_mates[s - 1])

        return by_width(z, make)

    def weight_y(m, src_sp):
        def make(width):
            slot = weight_slot(src_sp, m, width)
            return remote(slot, slot, wy_s.at[m], wy_r.at[m], y_mate)

        return by_width(z, make)

    def weight_y_all(m):
        def make(width):
            rows = pl.ds(0, nz * depth)
            if m == 2:
                slot = down_w.at[pl.ds(0, width), rows]
            else:
                slot = (gate_w, up_w)[m].at[rows, pl.ds(0, width)]
            return remote(slot, slot, wy_s.at[m], wy_r.at[m], y_mate)

        return by_width(z, make)

    for m in range(3):
        for s in range(1, nz):
            when_start(weight_z(s, m))
    for s in range(nz):
        piece = latent_piece(source_y(s), x, c)
        remote(piece, piece, kvy_s.at[0], kvy_r.at[s], y_mate).wait_recv()
        hand_on(nz - 1 + s)
    for m in range(3):
        for wanted, copy in own_weights(m):
            pl.when(wanted)(copy.wait)
        when_start(weight_y(m, sp))
    for n, src_sp in enumerate(foreign):
        piece = latent_piece(src_sp, 1 - x, c)
        remote(piece, piece, kvx_s.at[0], kvx_r.at[n], x_mate).wait_recv()
        begin(remote(piece, piece, kvc_s.at[0], kvc_r.at[0], c_mate))

    def latent_bytes(count, send, recv):
        rows = packed.at[pl.ds(0, count * quarter), :]
        return remote(rows, rows, send, recv, c_mate)

    latent_bytes(2 * len(foreign), kvc_s.at[0], kvc_r.at[0]).wait_recv()
    local[8].wait()
    local[9].wait()

    chunk = scores.shape[3]
    chunks = total // chunk
    scale = (NOPE + RD) ** (-0.5) * log2_e

    def pass_weights(m):
        for s in range(1, nz):
            when_wait_recv(weight_z_in(s, m))
            when_start(weight_y(m, source(s)))

    def score_chunk(h, k):
        rows = pl.ds(pl.multiple_of(k * chunk, chunk), chunk)
        lanes = slice(h * NOPE, (h + 1) * NOPE)
        both = jnp.dot(
            packed[rows, :rank],
            jnp.concatenate([w_key[:, lanes], w_value[:, lanes]], axis=1),
            preferred_element_type=jnp.float32,
        ).astype(jnp.bfloat16)
        vals[h % 2, rows, :] = both[:, NOPE:]
        keys = jnp.concatenate([both[:, :NOPE], packed[rows, rank:]], axis=1)
        value = lax.dot_general(
            queries[h], keys, (((1,), (1,)), ((), ())), preferred_element_type=jnp.float32
        )
        scores[h % 2, k] = value
        most = top_ref[...]
        for j in range(chunk // LANES):
            most = jnp.maximum(most, value[:, j * LANES : (j + 1) * LANES])
        top_ref[...] = most

    def weigh_chunk(h, k, top):
        rows = pl.ds(pl.multiple_of(k * chunk, chunk), chunk)
        weights = jnp.exp2((scores[h % 2, k] - top) * scale)
        denom = den_ref[...]
        for j in range(chunk // LANES):
            denom = denom + weights[:, j * LANES : (j + 1) * LANES]
        den_ref[...] = denom
        acc_ref[...] += jnp.dot(
            weights.astype(jnp.bfloat16), vals[h % 2, rows, :], preferred_element_type=jnp.float32
        )

    tp_mates = [c_mate, x_mate, diagonal]
    tp_of = [x * CORES + 1 - c, (1 - x) * CORES + c, (1 - x) * CORES + 1 - c]

    def head_piece(h, i):
        lanes = slice(h * VD, (h + 1) * VD)
        rows = pl.ds(pl.multiple_of(tp_of[i] * quarter, quarter), quarter)
        return remote(
            attended.at[rows, lanes], head_rows.at[tp, :, lanes], tp_s.at[0], tp_r.at[0], tp_mates[i]
        )

    def heads_all():
        return remote(
            attended.at[pl.ds(0, tok - quarter), :],
            head_rows.at[pl.ds(0, tp_count - 1)],
            tp_s.at[0],
            tp_r.at[0],
            c_mate,
        )

    for h in range(heads + 1):
        top = None
        if h > 0:
            top = jnp.max(top_ref[...], axis=1, keepdims=True)
            den_ref[...] = jnp.zeros_like(den_ref)
            acc_ref[...] = jnp.zeros_like(acc_ref)
        if h < heads:
            top_ref[...] = jnp.full_like(top_ref, -3.0e38)

        def one_chunk(k, carry, h=h, top=top):
            if h > 0:
                weigh_chunk(h - 1, k, top)
            if h < heads:
                score_chunk(h, k)
            return carry

        lax.fori_loop(0, chunks, one_chunk, 0)
        if h > 0:
            denom = jnp.sum(den_ref[...], axis=1, keepdims=True)
            attended[:, (h - 1) * VD : h * VD] = (acc_ref[...] / denom).astype(jnp.bfloat16)
            for i in (2, 1, 0):
                begin(head_piece(h - 1, i))

    pass_weights(0)
    head_rows[tp] = attended[pl.ds(pl.multiple_of(tp * quarter, quarter), quarter), :]
    for n in range(10, len(local)):
        local[n].wait()
    heads_all().wait_recv()
    span = head_rows.shape[2]
    mixed = resid_alpha * own_resid[...].astype(jnp.float32)
    for t in range(tp_count):
        mixed = mixed + jnp.dot(
            head_rows[t], out_weights[t * span : (t + 1) * span, :], preferred_element_type=jnp.float32
        )
    rows_all[z, x, c] = layer_scaled(mixed, mix_gain[...]).astype(jnp.bfloat16)

    kept = jnp.where(is_short(z), wide - LANES, wide) if missing else wide

    pieces = z_r.shape[1]
    halves = [slice(n * model // pieces, (n + 1) * model // pieces) for n in range(pieces)]

    def z_sends(zz, n):
        block = rows_all.at[zz, x, c, :, halves[n]]
        arrives = z_r.at[zz, n]
        return (
            (
                jnp.logical_and(zz <= z, z < nz - 1),
                remote(block, block, up_s.at[zz], arrives, at(zz=jnp.minimum(z + 1, nz - 1))),
            ),
            (
                jnp.logical_and(zz >= z, z > 0),
                remote(block, block, dn_s.at[zz], arrives, at(zz=jnp.maximum(z - 1, 0))),
            ),
        )

    def x_send(zz, n):
        block = rows_all.at[zz, x, c, :, halves[n]]
        return remote(block, block, x_s.at[0], x_r.at[zz, n], x_mate)

    def c_send(zz, xx, n):
        block = rows_all.at[zz, xx, c, :, halves[n]]
        return remote(block, block, c_s.at[0], c_r.at[zz, xx], c_mate)

    def arrive_x(zz, n):
        block = rows_all.at[zz, 1 - x, c, :, halves[n]]
        remote(block, block, x_s.at[0], x_r.at[zz, n], x_mate).wait_recv()

    def arrive_c(zz, xx):
        block = rows_all.at[zz, xx, 1 - c]
        remote(block, block, c_s.at[0], c_r.at[zz, xx], c_mate).wait_recv()

    bend = x_stage.shape[2]

    def core_send(zz, xx):
        return remote(
            part.at[zz, xx, 1 - c], core_part.at[zz, xx], crs_s.at[0], crs_r.at[zz, xx], c_mate
        )

    middle = -(-bend // (2 * LANES)) * LANES
    cuts = [slice(0, middle), slice(middle, bend)]

    def x_sum_send(zz, n):
        cols = cuts[n]
        return remote(
            x_stage.at[zz, :, cols], x_part.at[zz, :, cols], xrs_s.at[0], xrs_r.at[zz, n], x_mate
        )

    def last_send():
        return remote(last_stage, last_part, last_sem.at[0], last_sem.at[1], x_mate)

    def beyond(way):
        return at(zz=jnp.clip(jnp.where(way == 0, z + 1, z - 1), 0, nz - 1))

    def sum_send(zz, n, way):
        cols = cuts[n]
        return remote(
            z_stage.at[zz, :, cols],
            z_part.at[way, zz, :, cols],
            zch_s.at[0],
            zch_r.at[way, zz, n],
            beyond(way),
        )

    def late_send(zz, way):
        return remote(
            late_stage.at[zz], late_part.at[way, zz], late_s.at[0], late_r.at[way, zz], beyond(way)
        )

    def pair_sum(zz, xx, cols):
        return part[zz, xx, c, :, cols].astype(jnp.float32) + core_part[zz, xx, :, cols].astype(
            jnp.float32
        )

    late_cols = slice(bend, model)

    def gather_step(step):
        zz = near_order(step, z, nz)
        for n in range(pieces):

            @pl.when(step > 0)
            def _(n=n):
                block = rows_all.at[zz, x, c, :, halves[n]]
                remote(block, block, up_s.at[zz], z_r.at[zz, n], x_mate).wait_recv()

            for wanted, copy in z_sends(zz, n):
                pl.when(wanted)(copy.start)
            x_send(zz, n).start()
            c_send(zz, x, n).start()

    def across_step(step):
        zz = near_order(step, z, nz)
        for n in range(pieces):
            arrive_x(zz, n)
            c_send(zz, 1 - x, n).start()

    def mix_half(turn, step):
        zz = near_order(jnp.where(step == 0, 0, nz - step), z, nz)
        late_rows = step == 1
        xx = jnp.where((turn == 0) == late_rows, x, 1 - x)
        pl.when(jnp.logical_and(late_rows, turn == 1))(lambda: across_step(nz - 1))
        arrive_c(zz, xx)
        rows = CORES * quarter
        lanes = lax.broadcasted_iota(jnp.int32, (1, wide), 1)
        unit = rows_all[zz, xx].reshape(rows, model)
        gate = jnp.dot(unit, gate_w[...], preferred_element_type=jnp.float32)
        up = jnp.dot(unit, up_w[...], preferred_element_type=jnp.float32)
        inner = jax.nn.silu(gate) * up
        hidden[...] = jnp.where(lanes < kept, inner, 0.0).astype(jnp.bfloat16)
        cut = 512
        for n in range(model // cut):
            piece = jnp.dot(
                hidden[...], down_w[:, n * cut : (n + 1) * cut], preferred_element_type=jnp.float32
            ).astype(jnp.bfloat16)
            part[zz, xx, :, :, n * cut : (n + 1) * cut] = piece.reshape(CORES, quarter, cut)
        core_send(zz, xx).start()
        return step

    def mix_step(step):
        zz = near_order(jnp.where(step == 0, 0, nz - step), z, nz)
        lax.fori_loop(0, 2, mix_half, step)
        core_send(zz, 1 - x).wait_recv()
        for n in range(2):
            x_stage[zz, :, cuts[n]] = pair_sum(zz, 1 - x, cuts[n]).astype(jnp.bfloat16)
            x_sum_send(zz, n).start()

    def ready_sum(zz, n):
        x_sum_send(zz, n).wait_recv()
        return pair_sum(zz, x, cuts[n]) + x_part[zz, :, cuts[n]].astype(jnp.float32)

    def handed_on(step):
        for turn in range(2):
            way = jnp.where(z < nz // 2, 1 - turn, turn)
            place = jnp.where(way == 0, z, nz - 1 - z)
            owner = nz - 1 - step + place
            wanted = jnp.logical_and(owner > place, owner < nz)
            yield way, jnp.where(way == 0, owner, nz - 1 - owner), wanted, place > 0

    def chain_step(step):
        for way, zz, wanted, relayed in handed_on(step):

            @pl.when(wanted)
            def _(way=way, zz=zz, relayed=relayed):
                for n in range(2):
                    cols = cuts[n]
                    z_stage[zz, :, cols] = ready_sum(zz, n).astype(jnp.bfloat16)

                    @pl.when(relayed)
                    def _(n=n, cols=cols):
                        sum_send(zz, n, way).wait_recv()
                        z_stage[zz, :, cols] = (
                            z_stage[zz, :, cols].astype(jnp.float32)
                            + z_part[way, zz, :, cols].astype(jnp.float32)
                        ).astype(jnp.bfloat16)

                    sum_send(zz, n, way).start()

    def late_step(step):
        for way, zz, wanted, relayed in handed_on(step):

            @pl.when(wanted)
            def _(way=way, zz=zz, relayed=relayed):
                core_send(zz, x).wait_recv()
                for xx in range(2):
                    late_stage[zz, xx] = pair_sum(zz, xx, late_cols).astype(jnp.bfloat16)

                @pl.when(relayed)
                def _():
                    late_send(zz, way).wait_recv()
                    late_stage[zz] = (
                        late_stage[zz].astype(jnp.float32) + late_part[way, zz].astype(jnp.float32)
                    ).astype(jnp.bfloat16)

                late_send(zz, way).start()

    def late_total(xx):
        got = pair_sum(z, xx, late_cols)
        got = got + jnp.where(z > 0, late_part[0, z, xx].astype(jnp.float32), 0.0)
        return got + jnp.where(z < nz - 1, late_part[1, z, xx].astype(jnp.float32), 0.0)

    gather_step(jnp.int32(0))
    for step in range(1, nz):
        if step < 3:
            pass_weights(step)
        gather_step(jnp.int32(step))
        across_step(jnp.int32(step - 1))
    for m in range(3):
        when_wait_recv(weight_y_all(m))

    def one_step(step, carry):
        mix_step(step)
        pl.when(step > 0)(lambda: late_step(step - 1))
        pl.when(step > 1)(lambda: chain_step(step - 2))
        return carry

    lax.fori_loop(0, nz, one_step, 0)
    core_send(z, x).wait_recv()
    pl.when(z > 0)(late_send(z, 0).wait_recv)
    pl.when(z < nz - 1)(late_send(z, 1).wait_recv)
    last_stage[...] = late_total(1 - x).astype(jnp.bfloat16)
    last_send().start()
    late_sum = late_total(x)
    chain_step(nz - 2)

    totals = []
    for n in range(2):
        cols = cuts[n]
        got = ready_sum(z, n)
        pl.when(z > 0)(sum_send(z, n, 0).wait_recv)
        pl.when(z < nz - 1)(sum_send(z, n, 1).wait_recv)
        got = got + jnp.where(z > 0, z_part[0, z, :, cols].astype(jnp.float32), 0.0)
        totals.append(got + jnp.where(z < nz - 1, z_part[1, z, :, cols].astype(jnp.float32), 0.0))
    last_send().wait_recv()
    late_sum = late_sum + last_part[...].astype(jnp.float32)
    part_sum = jnp.concatenate(totals + [late_sum], axis=1)
    out_ref[...] = layer_scaled(
        resid_alpha * rows_all[z, x, c].astype(jnp.float32) + 0.5 * part_sum, out_gain[...]
    ).astype(jnp.bfloat16)

    latent_bytes(nz - 1, kvz_s.at[0], kvz_r.at[0]).wait_send()
    latent_bytes(nz, kvy_s.at[0], kvy_r.at[0]).wait_send()
    latent_bytes(len(foreign), kvx_s.at[0], kvx_r.at[0]).wait_send()
    latent_bytes(2 * len(foreign), kvc_s.at[0], kvc_r.at[0]).wait_send()
    heads_all().wait_send()
    for m in range(3):
        pairs = weight_y_all(m)
        for s in range(1, nz):
            pairs = pairs + weight_z(s, m)
        for wanted, copy in pairs:
            pl.when(wanted)(copy.wait_send)

    last_send().wait_send()

    everywhere = rows_all.at[:, x, c]
    remote(everywhere, everywhere, x_s.at[0], x_r.at[0, 0], x_mate).wait_send()
    everywhere = rows_all.at[:, :, c]
    remote(everywhere, everywhere, c_s.at[0], c_r.at[0, 0], c_mate).wait_send()
    remote(part.at[:, :, 1 - c], core_part, crs_s.at[0], crs_r.at[0, 0], c_mate).wait_send()
    remote(x_stage, x_part, xrs_s.at[0], xrs_r.at[0, 0], x_mate).wait_send()
    others = pl.ds(0, nz - 1)
    remote(
        z_stage.at[others], z_part.at[0, others], zch_s.at[0], zch_r.at[0, 0, 0], x_mate
    ).wait_send()
    remote(
        late_stage.at[others], late_part.at[0, others], late_s.at[0], late_r.at[0, 0], x_mate
    ).wait_send()

    def drain(zz, carry):
        block = rows_all.at[zz, x, c]
        for wanted, sem in (
            (jnp.logical_and(zz <= z, z < nz - 1), up_s),
            (jnp.logical_and(zz >= z, z > 0), dn_s),
        ):
            pl.when(wanted)(remote(block, block, sem.at[zz], z_r.at[0, 0], x_mate).wait_send)
        return carry

    lax.fori_loop(0, nz, drain, 0)


def fused_layer(
    sp_count,
    tp_count,
    resid_stream,
    q_latent,
    kv_latent,
    rope_key,
    doc_ids,
    q_gain,
    kv_gain,
    w_query,
    w_key,
    w_value,
    w_out,
    mix_gain,
    w_gate,
    w_up,
    w_down,
    out_gain,
):
    ny = tp_count // CORES
    nz = sp_count // ny
    tok = q_latent.shape[0]
    total = tok * sp_count
    quarter = tok // tp_count
    model = resid_stream.shape[1]
    heads = w_key.shape[1] // NOPE
    rank = kv_latent.shape[1]
    ff = w_gate.shape[1]
    wide = -(-ff // (LANES * nz)) * LANES
    chunk = 512
    pieces = 4
    bend = model - 3 * (model // 16)
    hbm = pl.BlockSpec(memory_space=pl.ANY)
    bf16, f32 = jnp.bfloat16, jnp.float32
    dma = pltpu.SemaphoreType.DMA
    table = turn_table(total)
    scratch = [
        pltpu.VMEM(q_latent.shape, bf16),
        pltpu.VMEM(kv_latent.shape, bf16),
        pltpu.VMEM((RD, tok), bf16),
        pltpu.VMEM((tok,), jnp.int32),
        pltpu.VMEM((RD, tok), f32),
        pltpu.VMEM((1, q_latent.shape[1]), f32),
        pltpu.VMEM((1, rank), f32),
        pltpu.VMEM((1, model), f32),
        pltpu.VMEM((1, model), f32),
        pltpu.VMEM(w_query.shape, bf16),
        pltpu.VMEM(w_key.shape, bf16),
        pltpu.VMEM(w_value.shape, bf16),
        pltpu.VMEM((total, rank + 2 * RD), bf16),
        pltpu.VMEM((heads, tok, NOPE + 2 * RD), bf16),
        pltpu.VMEM((2, total, VD), bf16),
        pltpu.VMEM((2, total // chunk, tok, chunk), f32),
        pltpu.VMEM((tok, LANES), f32),
        pltpu.VMEM((tok, LANES), f32),
        pltpu.VMEM((tok, VD), f32),
        pltpu.VMEM((tok, heads * VD), bf16),
        pltpu.VMEM((tp_count, quarter, heads * VD), bf16),
        pltpu.VMEM(w_out.shape, bf16),
        pltpu.VMEM((quarter, model), bf16),
        pltpu.VMEM((model, wide), bf16),
        pltpu.VMEM((model, wide), bf16),
        pltpu.VMEM((wide, model), bf16),
        pltpu.VMEM((nz, 2, CORES, quarter, model), bf16),
        pltpu.VMEM((CORES * quarter, wide), bf16),
        pltpu.VMEM((nz, 2, CORES, quarter, model), bf16),
        pltpu.VMEM((nz, 2, quarter, model), bf16),
        pltpu.VMEM((nz, quarter, bend), bf16),
        pltpu.VMEM((nz, quarter, bend), bf16),
        pltpu.VMEM((nz, quarter, bend), bf16),
        pltpu.VMEM((2, nz, quarter, bend), bf16),
        pltpu.VMEM((nz, 2, quarter, model - bend), bf16),
        pltpu.VMEM((2, nz, 2, quarter, model - bend), bf16),
        pltpu.VMEM((quarter, model - bend), bf16),
        pltpu.VMEM((quarter, model - bend), bf16),
        dma((14,)),
        dma((3,)),
        dma((1,)),
        dma((nz - 1,)),
        dma((1,)),
        dma((nz,)),
        dma((1,)),
        dma((2 * nz - 1,)),
        dma((1,)),
        dma((1,)),
        dma((nz - 1, 3)),
        dma((nz - 1, 3)),
        dma((3,)),
        dma((3,)),
        dma((1,)),
        dma((1,)),
        dma((nz,)),
        dma((nz,)),
        dma((nz, pieces)),
        dma((1,)),
        dma((nz, pieces)),
        dma((1,)),
        dma((nz, 2)),
        dma((1,)),
        dma((nz, 2)),
        dma((1,)),
        dma((nz, 2)),
        dma((1,)),
        dma((2, nz, 2)),
        dma((1,)),
        dma((2, nz)),
        dma((2,)),
    ]
    return pl.pallas_call(
        functools.partial(layer_kernel, nz, ny, heads),
        out_shape=pltpu.VMEM((quarter, model), bf16),
        in_specs=[hbm] * 17,
        out_specs=pl.BlockSpec(memory_space=pltpu.VMEM),
        scratch_shapes=scratch,
        compiler_params=pltpu.CompilerParams(
            collective_id=0, has_side_effects=True, vmem_limit_bytes=64 * 1000 * 1000
        ),
    )(
        q_latent,
        kv_latent,
        rope_key.T,
        doc_ids,
        table,
        q_gain[None, :],
        kv_gain[None, :],
        mix_gain[None, :],
        out_gain[None, :],
        w_query,
        w_key,
        w_value,
        resid_stream,
        w_out,
        w_gate,
        w_up,
        w_down,
    )


def solution(mesh):
    in_specs = (
        P("sp", None),
        P("sp", None),
        P("sp", None),
        P("sp", None),
        P("sp"),
        P(),
        P(),
        P(None, "tp"),
        P(None, "tp"),
        P(None, "tp"),
        P(),
        P(),
        P("sp", "tp"),
        P("sp", "tp"),
        P("tp", "sp"),
        P(),
    )
    out_specs = P(("sp", "tp"), None)
    if mesh.shape["tp"] == 2 * CORES:
        return jax.shard_map(
            functools.partial(fused_layer, mesh.shape["sp"], mesh.shape["tp"]),
            mesh=mesh,
            in_specs=in_specs,
            out_specs=out_specs,
            check_vma=False,
        )
    return jax.shard_map(body, mesh=mesh, in_specs=in_specs, out_specs=out_specs, check_vma=False)
```

```python
import functools
import math

import jax
import jax.numpy as jnp
import numpy as np
from jax import lax
from jax.experimental import pallas as pl
from jax.experimental.pallas import tpu as pltpu
from jax.sharding import PartitionSpec as P

NOPE = 128
RD = 64
VD = 128


eps_norm = 1e-05
rope_theta = 10000.0
resid_alpha = 8.0**0.25
key_span = 2048


def rope_angles(positions):
    frequency = rope_theta ** (-jnp.arange(0, RD, 2, dtype=jnp.float32) / RD)
    angles = positions.astype(jnp.float32)[:, None] * frequency[None, :]
    return (jnp.cos(angles), jnp.sin(angles))


def rotate(values, cos_table, sin_table):
    half_width = values.shape[-1] // 2
    first_half = values[..., :half_width]
    second_half = values[..., half_width:]
    return jnp.concatenate(
        [
            first_half * cos_table - second_half * sin_table,
            second_half * cos_table + first_half * sin_table,
        ],
        axis=-1,
    )


def rms_scaled(latent, scaling):
    widened = latent.astype(jnp.float32)
    inverse = lax.rsqrt(jnp.mean(widened * widened, axis=-1, keepdims=True) + eps_norm)
    return (widened * inverse * scaling).astype(jnp.bfloat16)


def layer_scaled(stream, scaling):
    centre = stream - jnp.mean(stream, axis=-1, keepdims=True)
    spread = jnp.mean(centre * centre, axis=-1, keepdims=True)
    return centre * lax.rsqrt(spread + eps_norm) * scaling


def fold_in_blocks(carried, piece_part, attend_fn):
    piece_rows = piece_part[0].shape[0]
    if piece_rows > key_span and piece_rows % key_span == 0:

        def one_block(inner, block_index):
            sliced = tuple(
                (
                    lax.dynamic_slice_in_dim(
                        member, (block_index * key_span).astype(jnp.int32), key_span, 0
                    )
                    for member in piece_part
                )
            )
            return (attend_fn(inner, sliced), None)

        outcome = lax.scan(one_block, carried, jnp.arange(piece_rows // key_span, dtype=jnp.int32))
        return outcome[0]
    return attend_fn(carried, piece_part)


class Ring:
    def __init__(self, blocks):
        self.count = lax.axis_size("sp")
        ring = list(range(0, self.count, 2)) + list(range(1, self.count, 2))[::-1]
        places = [ring.index(i) for i in range(self.count)]
        self.place = jnp.array(places, jnp.int32)[lax.axis_index("sp")]
        self.ring_of = jnp.array(ring, jnp.int32)
        self.right = [(ring[i], ring[(i + 1) % self.count]) for i in range(self.count)]
        self.left = [(after, before) for before, after in self.right]
        self.pieces = [[(lax.axis_index("sp"), block)] for block in blocks]
        self.flying = [(block, block) for block in blocks]
        self.step = 0

    def owner(self, distance):
        return self.ring_of[(self.place + distance) % self.count]

    def hop(self):
        self.step += 1
        self.send()

    def send(self):
        if self.step < self.count // 2:
            self.flying = [
                (lax.ppermute(one, "sp", self.right), lax.ppermute(two, "sp", self.left))
                for one, two in self.flying
            ]
        elif self.step == self.count // 2:
            self.flying = [
                (
                    lax.ppermute(one[: one.shape[0] // 2], "sp", self.right),
                    lax.ppermute(two[two.shape[0] // 2 :], "sp", self.left),
                )
                for one, two in self.flying
            ]

    def land(self, *values):
        if self.step <= self.count // 2:
            if values:
                values, self.flying = lax.optimization_barrier((values, self.flying))
            for pieces, (one, two) in zip(self.pieces, self.flying):
                if self.step < self.count // 2:
                    pieces.append((self.owner(-self.step), one))
                    pieces.append((self.owner(self.step), two))
                else:
                    pieces.append((self.owner(self.step), jnp.concatenate([one, two])))
        return values


def body(
    resid_stream,
    q_latent,
    kv_latent,
    rope_key,
    doc_ids,
    q_gain,
    kv_gain,
    w_query,
    w_key,
    w_value,
    w_out,
    mix_gain,
    w_gate,
    w_up,
    w_down,
    out_gain,
):
    tok_rows = q_latent.shape[0]
    head_count = w_key.shape[1] // NOPE
    tp_count = lax.axis_size("tp")
    part_rows = tok_rows // tp_count
    tp_index = lax.axis_index("tp")
    gate_ring = Ring([jnp.concatenate([w_gate, w_up], axis=1)])
    down_ring = Ring([w_down])
    gate_ring.hop()
    positions = lax.axis_index("sp") * tok_rows + jnp.arange(tok_rows, dtype=jnp.int32)
    cos_table, sin_table = rope_angles(positions)
    q_normed = rms_scaled(q_latent, q_gain)
    queries = jnp.dot(q_normed, w_query, preferred_element_type=jnp.float32).reshape(
        tok_rows, head_count, NOPE + RD
    )
    query_nope = queries[:, :, :NOPE].astype(jnp.bfloat16)
    query_rope = rotate(queries[:, :, NOPE:], cos_table[:, None, :], sin_table[:, None, :]).astype(
        jnp.bfloat16
    )
    kv_normed = rms_scaled(kv_latent, kv_gain)
    key_rot = rotate(rope_key.astype(jnp.float32), cos_table, sin_table).astype(jnp.bfloat16)
    score_scale = (NOPE + RD) ** (-0.5)

    def attend_rows(carried, piece_part, between=lambda value: value):
        row_top, denom_sum, accum_out = carried
        key_piece, value_piece, rot_piece, doc_piece = piece_part
        piece_rows = key_piece.shape[0]
        keys_heads = key_piece.reshape(piece_rows, head_count, NOPE)
        values_heads = value_piece.reshape(piece_rows, head_count, VD)
        scores = jnp.einsum(
            "qhd,khd->hqk", query_nope, keys_heads, preferred_element_type=jnp.float32
        )
        scores = (
            scores
            + jnp.einsum("qhd,kd->hqk", query_rope, rot_piece, preferred_element_type=jnp.float32)
        ) * score_scale
        same_doc = (doc_ids[:, None] == doc_piece[None, :])[None]
        masked = jnp.where(same_doc, scores, -1e30)
        new_top = jnp.maximum(row_top, jnp.max(masked, axis=-1))
        weights = jnp.where(same_doc, jnp.exp(masked - new_top[:, :, None]), 0.0)
        factor = jnp.exp(row_top - new_top)
        denom_sum = denom_sum * factor + jnp.sum(weights, axis=-1)
        weights = between(weights.astype(jnp.bfloat16))
        update = jnp.einsum(
            "hqk,khd->qhd", weights, values_heads, preferred_element_type=jnp.float32
        )
        accum_out = accum_out * jnp.transpose(factor)[:, :, None] + update
        return (new_top, denom_sum, accum_out)

    initial = (
        jnp.full((head_count, tok_rows), -1e30, jnp.float32),
        jnp.zeros((head_count, tok_rows), jnp.float32),
        jnp.zeros((tok_rows, head_count, VD), jnp.float32),
    )

    def project_rows(carried, piece_part, between=lambda value: value):
        latent_piece, rot_piece, doc_piece = piece_part
        key_piece = jnp.dot(latent_piece, w_key, preferred_element_type=jnp.float32).astype(
            jnp.bfloat16
        )
        value_piece = jnp.dot(latent_piece, w_value, preferred_element_type=jnp.float32).astype(
            jnp.bfloat16
        )
        return attend_rows(carried, (key_piece, value_piece, rot_piece, doc_piece), between)

    def next_hop(value):
        (value,) = gate_ring.land(value)
        gate_ring.hop()
        return value

    doc_lanes = jnp.broadcast_to(doc_ids.astype(jnp.bfloat16)[:, None], (tok_rows, RD))
    packed = jnp.concatenate([kv_normed, key_rot, doc_lanes], axis=1)
    packed_part = lax.dynamic_slice_in_dim(packed, tp_index * part_rows, part_rows, 0)
    packed_all = lax.all_gather(packed_part, ("sp", "tp"), axis=0, tiled=True)
    packed_all = next_hop(packed_all)
    kv_rank = kv_latent.shape[1]
    gathered = (
        packed_all[:, :kv_rank],
        packed_all[:, kv_rank : kv_rank + RD],
        packed_all[:, kv_rank + RD].astype(jnp.int32),
    )
    if packed_all.shape[0] > key_span and packed_all.shape[0] % key_span == 0:
        carried_out = fold_in_blocks(initial, gathered, project_rows)
    else:
        carried_out = project_rows(initial, gathered, next_hop)
    denom_sum = carried_out[1]
    attended = (
        (carried_out[2] / jnp.transpose(denom_sum)[:, :, None])
        .astype(jnp.bfloat16)
        .reshape(tok_rows, head_count * VD)
    )
    heads_rows = lax.all_to_all(attended, "tp", split_axis=0, concat_axis=1, tiled=True)
    mixer_out = jnp.dot(heads_rows, w_out, preferred_element_type=jnp.float32)
    own_resid = lax.dynamic_slice_in_dim(resid_stream, tp_index * part_rows, part_rows, 0)
    own_normed = layer_scaled(
        resid_alpha * own_resid.astype(jnp.float32) + mixer_out, mix_gain
    ).astype(jnp.bfloat16)
    (own_normed,) = gate_ring.land(own_normed)
    down_ring.hop()
    gate_ring.hop()
    normed_rows = lax.all_gather(own_normed, "tp", axis=0, tiled=True)
    (normed_rows,) = down_ring.land(normed_rows)
    down_ring.hop()
    gate_ring.land()
    while gate_ring.step < gate_ring.count // 2:
        gate_ring.hop()
        gate_ring.land()
    gate_sum = None
    for owner, piece in gate_ring.pieces[0]:
        rows = lax.dynamic_slice_in_dim(normed_rows, owner * piece.shape[0], piece.shape[0], 1)
        term = jnp.dot(rows, piece, preferred_element_type=jnp.float32)
        gate_sum = term if gate_sum is None else gate_sum + term
    width = w_gate.shape[1]
    hidden = (jax.nn.silu(gate_sum[:, :width]) * gate_sum[:, width:]).astype(jnp.bfloat16)
    (hidden,) = down_ring.land(hidden)
    while down_ring.step < down_ring.count // 2:
        down_ring.hop()
        down_ring.land()
    down = down_ring.pieces[0]
    ffn_sum = jnp.zeros((part_rows, resid_stream.shape[1]), jnp.float32)
    for part, group in enumerate((down[: len(down) // 2], down[len(down) // 2 :])):
        pieces = [piece for _, piece in group]
        if part == 0:
            pieces = [jnp.concatenate(pieces, axis=1)]
        terms = [
            jnp.dot(hidden, piece, preferred_element_type=jnp.float32).astype(jnp.bfloat16)
            for piece in pieces
        ]
        partial = jnp.concatenate(terms, axis=1)
        swapped = lax.all_to_all(
            partial.reshape(tp_count, part_rows, -1), "tp", split_axis=0, concat_axis=0, tiled=True
        )
        summed = jnp.sum(swapped.astype(jnp.float32), axis=0)
        columns = w_down.shape[1]
        for at, (owner, _) in enumerate(group):
            ffn_sum = lax.dynamic_update_slice_in_dim(
                ffn_sum, summed[:, at * columns : (at + 1) * columns], owner * columns, 1
            )
    layer_out = layer_scaled(
        resid_alpha * own_normed.astype(jnp.float32) + 0.5 * ffn_sum, out_gain
    ).astype(jnp.bfloat16)
    return layer_out


CORES = 2
LANES = 128
MESH = pl.DeviceIdType.MESH
log2_e = math.log2(math.e)


def rms_rows(latent, scaling):
    widened = latent.astype(jnp.float32)
    inverse = lax.rsqrt(jnp.mean(widened * widened, axis=-1, keepdims=True) + eps_norm)
    return (widened * inverse * scaling).astype(jnp.bfloat16)


def near_order(step, z, nz):
    paired = 2 * jnp.minimum(z, nz - 1 - z)
    half = (step + 1) // 2
    close = jnp.where(step % 2 == 1, z - half, z + half)
    far = step - paired // 2
    wide = jnp.where(z < nz - 1 - z, z + far, z - far)
    return jnp.where(step <= paired, close, wide)


def turn_table(total):
    steps = np.arange(0, RD, 2, dtype=np.float32) / np.float32(RD)
    frequency = np.power(np.float32(rope_theta), -steps, dtype=np.float32)
    angles = frequency[:, None] * np.arange(total, dtype=np.float32)[None, :]
    wide_angles = angles.astype(np.float64)
    return np.concatenate([np.cos(wide_angles), np.sin(wide_angles)], axis=0).astype(np.float32)


def layer_kernel(
    nz,
    ny,
    heads,
    q_latent,
    kv_latent,
    rope_turned,
    doc_row,
    table,
    q_gain_in,
    kv_gain_in,
    mix_gain_in,
    out_gain_in,
    w_query_in,
    w_key_in,
    w_value_in,
    resid,
    w_out,
    w_gate,
    w_up,
    w_down,
    out_ref,
    q_lat,
    kv_lat,
    rope_own,
    doc_own,
    turns,
    q_gain,
    kv_gain,
    mix_gain,
    out_gain,
    w_query,
    w_key,
    w_value,
    packed,
    queries,
    vals,
    scores,
    top_ref,
    den_ref,
    acc_ref,
    attended,
    head_rows,
    out_weights,
    own_resid,
    gate_w,
    up_w,
    down_w,
    rows_all,
    hidden,
    part,
    core_part,
    x_stage,
    x_part,
    z_stage,
    z_part,
    late_stage,
    late_part,
    last_stage,
    last_part,
    loc_sem,
    own_sem,
    kvz_s,
    kvz_r,
    kvy_s,
    kvy_r,
    kvx_s,
    kvx_r,
    kvc_s,
    kvc_r,
    wz_s,
    wz_r,
    wy_s,
    wy_r,
    tp_s,
    tp_r,
    up_s,
    dn_s,
    z_r,
    x_s,
    x_r,
    c_s,
    c_r,
    crs_s,
    crs_r,
    xrs_s,
    xrs_r,
    zch_s,
    zch_r,
    late_s,
    late_r,
    last_sem,
):
    sp = lax.axis_index("sp")
    tp = lax.axis_index("tp")
    z, y = sp // ny, sp % ny
    x, c = tp // CORES, tp % CORES
    tok = q_latent.shape[0]
    quarter = out_ref.shape[0]
    tp_count = tok // quarter
    depth = w_gate.shape[0]
    wide = gate_w.shape[1]
    ff = w_gate.shape[1]
    model = out_ref.shape[1]
    total = packed.shape[0]
    rank = kv_latent.shape[1]

    def at(zz=None, yy=None, xx=None, cc=None):
        zz = z if zz is None else zz
        yy = y if yy is None else yy
        xx = x if xx is None else xx
        cc = c if cc is None else cc
        return (zz * ny + yy, xx * CORES + cc)

    def remote(src, dst, send, recv, where):
        return pltpu.make_async_remote_copy(
            src_ref=src,
            dst_ref=dst,
            send_sem=send,
            recv_sem=recv,
            device_id=where,
            device_id_type=MESH,
        )

    y_mate = at(yy=1 - y)
    x_mate = at(xx=1 - x)
    c_mate = at(cc=1 - c)
    diagonal = at(xx=1 - x, cc=1 - c)
    z_mates = [at(zz=(z + s) % nz) for s in range(1, nz)]

    barrier = pltpu.get_barrier_semaphore()
    mates = z_mates + [y_mate, x_mate, c_mate, diagonal]
    for mate in mates:
        pl.semaphore_signal(barrier, inc=1, device_id=mate, device_id_type=MESH)

    tiles = wide // LANES
    missing = nz * tiles - ff // LANES

    def is_short(zz):
        return (zz + nz - (nz // 2 - 1 + c)) % nz < missing

    def piece_start(zz):
        begun = 0
        for other in range(nz - 1):
            begun = begun + jnp.where(other < zz, tiles - is_short(other).astype(jnp.int32), 0)
        return pl.multiple_of(begun * LANES, LANES)

    def by_width(zz, make):
        pairs = [(jnp.logical_not(is_short(zz)), make(wide))]
        if missing:
            pairs.append((is_short(zz), make(wide - LANES)))
        return pairs

    def when_start(pairs):
        for wanted, copy in pairs:
            pl.when(wanted)(copy.start)

    def when_wait_recv(pairs):
        for wanted, copy in pairs:
            pl.when(wanted)(copy.wait_recv)

    def weight_slot(src_sp, m, width):
        rows = pl.ds(pl.multiple_of(src_sp * depth, depth), depth)
        if m == 2:
            return down_w.at[pl.ds(0, width), rows]
        return (gate_w, up_w)[m].at[rows, pl.ds(0, width)]

    def weight_source(zz, m, width):
        units = pl.ds(piece_start(zz), width)
        return w_down.at[units, :] if m == 2 else (w_gate, w_up)[m].at[:, units]

    def own_weights(m):
        return by_width(
            z,
            lambda width: pltpu.make_async_copy(
                weight_source(z, m, width), weight_slot(sp, m, width), own_sem.at[m]
            ),
        )

    own_cols = pl.ds(pl.multiple_of(sp * tok, LANES), tok)
    own_quarter = pl.ds(pl.multiple_of(tp * quarter, quarter), quarter)
    moves = [
        (kv_latent, kv_lat),
        (kv_gain_in, kv_gain),
        (rope_turned, rope_own),
        (doc_row, doc_own),
        (table.at[:, own_cols], turns),
        (q_latent, q_lat),
        (q_gain_in, q_gain),
        (w_query_in, w_query),
        (w_key_in, w_key),
        (w_value_in, w_value),
        (mix_gain_in, mix_gain),
        (out_gain_in, out_gain),
        (resid.at[own_quarter, :], own_resid),
        (w_out, out_weights),
    ]
    local = [pltpu.make_async_copy(src, dst, loc_sem.at[n]) for n, (src, dst) in enumerate(moves)]
    for one in local:
        one.start()
    for m in range(3):
        when_start(own_weights(m))
    if missing:

        @pl.when(is_short(z))
        def _():
            down_w[wide - LANES :, :] = jnp.zeros((LANES, model), jnp.bfloat16)

    for n in range(5):
        local[n].wait()
    half_turn = RD // 2
    cos_rows = jnp.concatenate([turns[:half_turn], turns[:half_turn]], axis=0)
    sin_rows = jnp.concatenate([-turns[half_turn:], turns[half_turn:]], axis=0)
    rope = rope_own[...].astype(jnp.float32)
    flipped = jnp.concatenate([rope[half_turn:], rope[:half_turn]], axis=0)
    marks = lax.broadcasted_iota(jnp.int32, (RD, tok), 0) == doc_own[...][None, :]
    side_rows = jnp.concatenate(
        [rope * cos_rows + flipped * sin_rows, marks.astype(jnp.float32)], axis=0
    )
    side = side_rows.T
    own_at = pl.multiple_of(sp * tok, tok)
    packed[pl.ds(own_at, tok), :rank] = rms_rows(kv_lat[...], kv_gain[...])
    packed[pl.ds(own_at, tok), rank:] = side.astype(jnp.bfloat16)

    pl.semaphore_wait(barrier, len(mates))

    def begin(copy):
        copy.start()

    def latent_piece(src_sp, xx, cc):
        first_row = src_sp * tok + (xx * CORES + cc) * quarter
        return packed.at[pl.ds(pl.multiple_of(first_row, quarter), quarter), :]

    def source(s):
        return ((z + nz - s) % nz) * ny + y

    def source_y(s):
        return ((z + nz - s) % nz) * ny + (1 - y)

    foreign = [source(s) for s in range(1, nz)] + [source_y(s) for s in range(nz)]
    own_piece = latent_piece(sp, x, c)
    for s in range(1, nz):
        begin(remote(own_piece, own_piece, kvz_s.at[0], kvz_r.at[s - 1], z_mates[s - 1]))
    begin(remote(own_piece, own_piece, kvy_s.at[0], kvy_r.at[0], y_mate))

    for n in range(5, 8):
        local[n].wait()
    both_turns = jnp.concatenate([cos_rows, sin_rows], axis=0).T
    cos_t, sin_t = both_turns[:, :RD], both_turns[:, RD:]
    q_normed = rms_rows(q_lat[...], q_gain[...])
    q_side = jnp.where(side[:, RD:] > 0.5, 0.0, -1e30)
    for h in range(heads):
        wide_q = jnp.dot(
            q_normed,
            w_query[:, h * (NOPE + RD) : (h + 1) * (NOPE + RD)],
            preferred_element_type=jnp.float32,
        )
        turned = wide_q[:, NOPE:]
        swapped = jnp.concatenate([turned[:, half_turn:], turned[:, :half_turn]], axis=1)
        rest = jnp.concatenate([turned * cos_t + swapped * sin_t, q_side], axis=1)
        queries[h, :, :NOPE] = wide_q[:, :NOPE].astype(jnp.bfloat16)
        queries[h, :, NOPE:] = rest.astype(jnp.bfloat16)

    def hand_on(n):
        piece = latent_piece(foreign[n], x, c)
        begin(remote(piece, piece, kvx_s.at[0], kvx_r.at[n], x_mate))
        begin(remote(piece, piece, kvc_s.at[0], kvc_r.at[0], c_mate))

    for s in range(1, nz):
        piece = latent_piece(source(s), x, c)
        remote(piece, piece, kvz_s.at[0], kvz_r.at[s - 1], z_mates[s - 1]).wait_recv()
        begin(remote(piece, piece, kvy_s.at[0], kvy_r.at[s], y_mate))
        hand_on(s - 1)

    def weight_z(s, m):
        return by_width(
            (z + s) % nz,
            lambda width: remote(
                weight_source((z + s) % nz, m, width),
                weight_slot(sp, m, width),
                wz_s.at[s - 1, m],
                wz_r.at[s - 1, m],
                z_mates[s - 1],
            ),
        )

    def weight_z_in(s, m):
        def make(width):
            slot = weight_slot(source(s), m, width)
            return remote(slot, slot, wz_s.at[s - 1, m], wz_r.at[s - 1, m], z_mates[s - 1])

        return by_width(z, make)

    def weight_y(m, src_sp):
        def make(width):
            slot = weight_slot(src_sp, m, width)
            return remote(slot, slot, wy_s.at[m], wy_r.at[m], y_mate)

        return by_width(z, make)

    def weight_y_all(m):
        def make(width):
            rows = pl.ds(0, nz * depth)
            if m == 2:
                slot = down_w.at[pl.ds(0, width), rows]
            else:
                slot = (gate_w, up_w)[m].at[rows, pl.ds(0, width)]
            return remote(slot, slot, wy_s.at[m], wy_r.at[m], y_mate)

        return by_width(z, make)

    for m in range(3):
        for s in range(1, nz):
            when_start(weight_z(s, m))
    for s in range(nz):
        piece = latent_piece(source_y(s), x, c)
        remote(piece, piece, kvy_s.at[0], kvy_r.at[s], y_mate).wait_recv()
        hand_on(nz - 1 + s)
    for m in range(3):
        for wanted, copy in own_weights(m):
            pl.when(wanted)(copy.wait)
        when_start(weight_y(m, sp))
    for n, src_sp in enumerate(foreign):
        piece = latent_piece(src_sp, 1 - x, c)
        remote(piece, piece, kvx_s.at[0], kvx_r.at[n], x_mate).wait_recv()
        begin(remote(piece, piece, kvc_s.at[0], kvc_r.at[0], c_mate))

    def latent_bytes(count, send, recv):
        rows = packed.at[pl.ds(0, count * quarter), :]
        return remote(rows, rows, send, recv, c_mate)

    latent_bytes(2 * len(foreign), kvc_s.at[0], kvc_r.at[0]).wait_recv()
    local[8].wait()
    local[9].wait()

    chunk = scores.shape[3]
    chunks = total // chunk
    scale = (NOPE + RD) ** (-0.5) * log2_e

    def pass_weights(m):
        for s in range(1, nz):
            when_wait_recv(weight_z_in(s, m))
            when_start(weight_y(m, source(s)))

    def score_chunk(h, k):
        rows = pl.ds(pl.multiple_of(k * chunk, chunk), chunk)
        lanes = slice(h * NOPE, (h + 1) * NOPE)
        both = jnp.dot(
            packed[rows, :rank],
            jnp.concatenate([w_key[:, lanes], w_value[:, lanes]], axis=1),
            preferred_element_type=jnp.float32,
        ).astype(jnp.bfloat16)
        vals[h % 2, rows, :] = both[:, NOPE:]
        keys = jnp.concatenate([both[:, :NOPE], packed[rows, rank:]], axis=1)
        value = lax.dot_general(
            queries[h], keys, (((1,), (1,)), ((), ())), preferred_element_type=jnp.float32
        )
        scores[h % 2, k] = value
        most = top_ref[...]
        for j in range(chunk // LANES):
            most = jnp.maximum(most, value[:, j * LANES : (j + 1) * LANES])
        top_ref[...] = most

    def weigh_chunk(h, k, top):
        rows = pl.ds(pl.multiple_of(k * chunk, chunk), chunk)
        weights = jnp.exp2((scores[h % 2, k] - top) * scale)
        denom = den_ref[...]
        for j in range(chunk // LANES):
            denom = denom + weights[:, j * LANES : (j + 1) * LANES]
        den_ref[...] = denom
        acc_ref[...] += jnp.dot(
            weights.astype(jnp.bfloat16), vals[h % 2, rows, :], preferred_element_type=jnp.float32
        )

    tp_mates = [c_mate, x_mate, diagonal]
    tp_of = [x * CORES + 1 - c, (1 - x) * CORES + c, (1 - x) * CORES + 1 - c]

    def head_piece(h, i):
        lanes = slice(h * VD, (h + 1) * VD)
        rows = pl.ds(pl.multiple_of(tp_of[i] * quarter, quarter), quarter)
        return remote(
            attended.at[rows, lanes], head_rows.at[tp, :, lanes], tp_s.at[0], tp_r.at[0], tp_mates[i]
        )

    def heads_all():
        return remote(
            attended.at[pl.ds(0, tok - quarter), :],
            head_rows.at[pl.ds(0, tp_count - 1)],
            tp_s.at[0],
            tp_r.at[0],
            c_mate,
        )

    for h in range(heads + 1):
        top = None
        if h > 0:
            top = jnp.max(top_ref[...], axis=1, keepdims=True)
            den_ref[...] = jnp.zeros_like(den_ref)
            acc_ref[...] = jnp.zeros_like(acc_ref)
        if h < heads:
            top_ref[...] = jnp.full_like(top_ref, -3.0e38)

        def one_chunk(k, carry, h=h, top=top):
            if h > 0:
                weigh_chunk(h - 1, k, top)
            if h < heads:
                score_chunk(h, k)
            return carry

        lax.fori_loop(0, chunks, one_chunk, 0)
        if h > 0:
            denom = jnp.sum(den_ref[...], axis=1, keepdims=True)
            attended[:, (h - 1) * VD : h * VD] = (acc_ref[...] / denom).astype(jnp.bfloat16)
            for i in (2, 1, 0):
                begin(head_piece(h - 1, i))

    head_rows[tp] = attended[pl.ds(pl.multiple_of(tp * quarter, quarter), quarter), :]
    for n in range(10, len(local)):
        local[n].wait()
    heads_all().wait_recv()
    span = head_rows.shape[2]
    mixed = resid_alpha * own_resid[...].astype(jnp.float32)
    for t in range(tp_count):
        mixed = mixed + jnp.dot(
            head_rows[t], out_weights[t * span : (t + 1) * span, :], preferred_element_type=jnp.float32
        )
    rows_all[z, x, c] = layer_scaled(mixed, mix_gain[...]).astype(jnp.bfloat16)

    kept = jnp.where(is_short(z), wide - LANES, wide) if missing else wide

    pieces = z_r.shape[1]
    halves = [slice(n * model // pieces, (n + 1) * model // pieces) for n in range(pieces)]

    def z_sends(zz, n):
        block = rows_all.at[zz, x, c, :, halves[n]]
        arrives = z_r.at[zz, n]
        return (
            (
                jnp.logical_and(zz <= z, z < nz - 1),
                remote(block, block, up_s.at[zz], arrives, at(zz=jnp.minimum(z + 1, nz - 1))),
            ),
            (
                jnp.logical_and(zz >= z, z > 0),
                remote(block, block, dn_s.at[zz], arrives, at(zz=jnp.maximum(z - 1, 0))),
            ),
        )

    def x_send(zz, n):
        block = rows_all.at[zz, x, c, :, halves[n]]
        return remote(block, block, x_s.at[0], x_r.at[zz, n], x_mate)

    def c_send(zz, xx, n):
        block = rows_all.at[zz, xx, c, :, halves[n]]
        return remote(block, block, c_s.at[0], c_r.at[zz, xx], c_mate)

    def arrive_x(zz, n):
        block = rows_all.at[zz, 1 - x, c, :, halves[n]]
        remote(block, block, x_s.at[0], x_r.at[zz, n], x_mate).wait_recv()

    def arrive_c(zz, xx):
        block = rows_all.at[zz, xx, 1 - c]
        remote(block, block, c_s.at[0], c_r.at[zz, xx], c_mate).wait_recv()

    bend = x_stage.shape[2]

    def core_send(zz, xx):
        return remote(
            part.at[zz, xx, 1 - c], core_part.at[zz, xx], crs_s.at[0], crs_r.at[zz, xx], c_mate
        )

    middle = -(-bend // (2 * LANES)) * LANES
    cuts = [slice(0, middle), slice(middle, bend)]

    def x_sum_send(zz, n):
        cols = cuts[n]
        return remote(
            x_stage.at[zz, :, cols], x_part.at[zz, :, cols], xrs_s.at[0], xrs_r.at[zz, n], x_mate
        )

    def last_send():
        return remote(last_stage, last_part, last_sem.at[0], last_sem.at[1], x_mate)

    def beyond(way):
        return at(zz=jnp.clip(jnp.where(way == 0, z + 1, z - 1), 0, nz - 1))

    def sum_send(zz, n, way):
        cols = cuts[n]
        return remote(
            z_stage.at[zz, :, cols],
            z_part.at[way, zz, :, cols],
            zch_s.at[0],
            zch_r.at[way, zz, n],
            beyond(way),
        )

    def late_send(zz, way):
        return remote(
            late_stage.at[zz], late_part.at[way, zz], late_s.at[0], late_r.at[way, zz], beyond(way)
        )

    def pair_sum(zz, xx, cols):
        return part[zz, xx, c, :, cols].astype(jnp.float32) + core_part[zz, xx, :, cols].astype(
            jnp.float32
        )

    late_cols = slice(bend, model)

    def gather_step(step):
        zz = near_order(step, z, nz)
        for n in range(pieces):

            @pl.when(step > 0)
            def _(n=n):
                block = rows_all.at[zz, x, c, :, halves[n]]
                remote(block, block, up_s.at[zz], z_r.at[zz, n], x_mate).wait_recv()

            for wanted, copy in z_sends(zz, n):
                pl.when(wanted)(copy.start)
            x_send(zz, n).start()
            c_send(zz, x, n).start()

    def across_step(step):
        zz = near_order(step, z, nz)
        for n in range(pieces):
            arrive_x(zz, n)
            c_send(zz, 1 - x, n).start()

    def mix_half(turn, step):
        zz = near_order(jnp.where(step == 0, 0, nz - step), z, nz)
        late_rows = step == 1
        xx = jnp.where((turn == 0) == late_rows, x, 1 - x)
        pl.when(jnp.logical_and(late_rows, turn == 1))(lambda: across_step(nz - 1))
        arrive_c(zz, xx)
        rows = CORES * quarter
        lanes = lax.broadcasted_iota(jnp.int32, (1, wide), 1)
        unit = rows_all[zz, xx].reshape(rows, model)
        gate = jnp.dot(unit, gate_w[...], preferred_element_type=jnp.float32)
        up = jnp.dot(unit, up_w[...], preferred_element_type=jnp.float32)
        inner = jax.nn.silu(gate) * up
        hidden[...] = jnp.where(lanes < kept, inner, 0.0).astype(jnp.bfloat16)
        cut = 512
        for n in range(model // cut):
            piece = jnp.dot(
                hidden[...], down_w[:, n * cut : (n + 1) * cut], preferred_element_type=jnp.float32
            ).astype(jnp.bfloat16)
            part[zz, xx, :, :, n * cut : (n + 1) * cut] = piece.reshape(CORES, quarter, cut)
        core_send(zz, xx).start()
        return step

    inside = jnp.logical_and(z > 0, z < nz - 1)

    def send_x_sum(zz, n):
        x_stage[zz, :, cuts[n]] = pair_sum(zz, 1 - x, cuts[n]).astype(jnp.bfloat16)
        x_sum_send(zz, n).start()

    def mix_step(step):
        zz = near_order(jnp.where(step == 0, 0, nz - step), z, nz)
        lax.fori_loop(0, 2, mix_half, step)
        core_send(zz, 1 - x).wait_recv()
        send_x_sum(zz, 0)
        pl.when(jnp.logical_or(step > 0, inside))(lambda: send_x_sum(zz, 1))
        pl.when(jnp.logical_and(step == nz - 1, jnp.logical_not(inside)))(lambda: send_x_sum(z, 1))

    def ready_sum(zz, n):
        x_sum_send(zz, n).wait_recv()
        return pair_sum(zz, x, cuts[n]) + x_part[zz, :, cuts[n]].astype(jnp.float32)

    def handed_on(step):
        for turn in range(2):
            way = jnp.where(z < nz // 2, 1 - turn, turn)
            place = jnp.where(way == 0, z, nz - 1 - z)
            owner = nz - 1 - step + place
            wanted = jnp.logical_and(owner > place, owner < nz)
            yield way, jnp.where(way == 0, owner, nz - 1 - owner), wanted, place > 0

    def chain_step(step):
        for way, zz, wanted, relayed in handed_on(step):

            @pl.when(wanted)
            def _(way=way, zz=zz, relayed=relayed):
                for n in range(2):
                    cols = cuts[n]
                    z_stage[zz, :, cols] = ready_sum(zz, n).astype(jnp.bfloat16)

                    @pl.when(relayed)
                    def _(n=n, cols=cols):
                        sum_send(zz, n, way).wait_recv()
                        z_stage[zz, :, cols] = (
                            z_stage[zz, :, cols].astype(jnp.float32)
                            + z_part[way, zz, :, cols].astype(jnp.float32)
                        ).astype(jnp.bfloat16)

                    sum_send(zz, n, way).start()

    def late_step(step):
        for way, zz, wanted, relayed in handed_on(step):

            @pl.when(wanted)
            def _(way=way, zz=zz, relayed=relayed):
                core_send(zz, x).wait_recv()
                for xx in range(2):
                    late_stage[zz, xx] = pair_sum(zz, xx, late_cols).astype(jnp.bfloat16)

                @pl.when(relayed)
                def _():
                    late_send(zz, way).wait_recv()
                    late_stage[zz] = (
                        late_stage[zz].astype(jnp.float32) + late_part[way, zz].astype(jnp.float32)
                    ).astype(jnp.bfloat16)

                late_send(zz, way).start()

    def late_total(xx):
        got = pair_sum(z, xx, late_cols)
        got = got + jnp.where(z > 0, late_part[0, z, xx].astype(jnp.float32), 0.0)
        return got + jnp.where(z < nz - 1, late_part[1, z, xx].astype(jnp.float32), 0.0)

    gather_step(jnp.int32(0))
    pass_weights(0)
    for step in range(1, nz):
        if step < 3:
            pass_weights(step)
        gather_step(jnp.int32(step))
        across_step(jnp.int32(step - 1))
    for m in range(3):
        when_wait_recv(weight_y_all(m))

    def one_step(step, carry):
        mix_step(step)
        pl.when(step > 0)(lambda: late_step(step - 1))
        pl.when(step > 1)(lambda: chain_step(step - 2))
        return carry

    lax.fori_loop(0, nz, one_step, 0)
    core_send(z, x).wait_recv()
    pl.when(z > 0)(late_send(z, 0).wait_recv)
    pl.when(z < nz - 1)(late_send(z, 1).wait_recv)
    last_stage[...] = late_total(1 - x).astype(jnp.bfloat16)
    last_send().start()
    late_sum = late_total(x)
    chain_step(nz - 2)

    totals = []
    for n in range(2):
        cols = cuts[n]
        got = ready_sum(z, n)
        pl.when(z > 0)(sum_send(z, n, 0).wait_recv)
        pl.when(z < nz - 1)(sum_send(z, n, 1).wait_recv)
        got = got + jnp.where(z > 0, z_part[0, z, :, cols].astype(jnp.float32), 0.0)
        totals.append(got + jnp.where(z < nz - 1, z_part[1, z, :, cols].astype(jnp.float32), 0.0))
    last_send().wait_recv()
    late_sum = late_sum + last_part[...].astype(jnp.float32)
    part_sum = jnp.concatenate(totals + [late_sum], axis=1)
    out_ref[...] = layer_scaled(
        resid_alpha * rows_all[z, x, c].astype(jnp.float32) + 0.5 * part_sum, out_gain[...]
    ).astype(jnp.bfloat16)

    latent_bytes(nz - 1, kvz_s.at[0], kvz_r.at[0]).wait_send()
    latent_bytes(nz, kvy_s.at[0], kvy_r.at[0]).wait_send()
    latent_bytes(len(foreign), kvx_s.at[0], kvx_r.at[0]).wait_send()
    latent_bytes(2 * len(foreign), kvc_s.at[0], kvc_r.at[0]).wait_send()
    heads_all().wait_send()
    for m in range(3):
        pairs = weight_y_all(m)
        for s in range(1, nz):
            pairs = pairs + weight_z(s, m)
        for wanted, copy in pairs:
            pl.when(wanted)(copy.wait_send)

    last_send().wait_send()

    everywhere = rows_all.at[:, x, c]
    remote(everywhere, everywhere, x_s.at[0], x_r.at[0, 0], x_mate).wait_send()
    everywhere = rows_all.at[:, :, c]
    remote(everywhere, everywhere, c_s.at[0], c_r.at[0, 0], c_mate).wait_send()
    remote(part.at[:, :, 1 - c], core_part, crs_s.at[0], crs_r.at[0, 0], c_mate).wait_send()
    remote(x_stage, x_part, xrs_s.at[0], xrs_r.at[0, 0], x_mate).wait_send()
    others = pl.ds(0, nz - 1)
    remote(
        z_stage.at[others], z_part.at[0, others], zch_s.at[0], zch_r.at[0, 0, 0], x_mate
    ).wait_send()
    remote(
        late_stage.at[others], late_part.at[0, others], late_s.at[0], late_r.at[0, 0], x_mate
    ).wait_send()

    def drain(zz, carry):
        block = rows_all.at[zz, x, c]
        for wanted, sem in (
            (jnp.logical_and(zz <= z, z < nz - 1), up_s),
            (jnp.logical_and(zz >= z, z > 0), dn_s),
        ):
            pl.when(wanted)(remote(block, block, sem.at[zz], z_r.at[0, 0], x_mate).wait_send)
        return carry

    lax.fori_loop(0, nz, drain, 0)


def fused_layer(
    sp_count,
    tp_count,
    resid_stream,
    q_latent,
    kv_latent,
    rope_key,
    doc_ids,
    q_gain,
    kv_gain,
    w_query,
    w_key,
    w_value,
    w_out,
    mix_gain,
    w_gate,
    w_up,
    w_down,
    out_gain,
):
    ny = tp_count // CORES
    nz = sp_count // ny
    tok = q_latent.shape[0]
    total = tok * sp_count
    quarter = tok // tp_count
    model = resid_stream.shape[1]
    heads = w_key.shape[1] // NOPE
    rank = kv_latent.shape[1]
    ff = w_gate.shape[1]
    wide = -(-ff // (LANES * nz)) * LANES
    chunk = 1024
    pieces = 4
    bend = model - model // 8
    hbm = pl.BlockSpec(memory_space=pl.ANY)
    bf16, f32 = jnp.bfloat16, jnp.float32
    dma = pltpu.SemaphoreType.DMA
    table = turn_table(total)
    scratch = [
        pltpu.VMEM(q_latent.shape, bf16),
        pltpu.VMEM(kv_latent.shape, bf16),
        pltpu.VMEM((RD, tok), bf16),
        pltpu.VMEM((tok,), jnp.int32),
        pltpu.VMEM((RD, tok), f32),
        pltpu.VMEM((1, q_latent.shape[1]), f32),
        pltpu.VMEM((1, rank), f32),
        pltpu.VMEM((1, model), f32),
        pltpu.VMEM((1, model), f32),
        pltpu.VMEM(w_query.shape, bf16),
        pltpu.VMEM(w_key.shape, bf16),
        pltpu.VMEM(w_value.shape, bf16),
        pltpu.VMEM((total, rank + 2 * RD), bf16),
        pltpu.VMEM((heads, tok, NOPE + 2 * RD), bf16),
        pltpu.VMEM((2, total, VD), bf16),
        pltpu.VMEM((2, total // chunk, tok, chunk), f32),
        pltpu.VMEM((tok, LANES), f32),
        pltpu.VMEM((tok, LANES), f32),
        pltpu.VMEM((tok, VD), f32),
        pltpu.VMEM((tok, heads * VD), bf16),
        pltpu.VMEM((tp_count, quarter, heads * VD), bf16),
        pltpu.VMEM(w_out.shape, bf16),
        pltpu.VMEM((quarter, model), bf16),
        pltpu.VMEM((model, wide), bf16),
        pltpu.VMEM((model, wide), bf16),
        pltpu.VMEM((wide, model), bf16),
        pltpu.VMEM((nz, 2, CORES, quarter, model), bf16),
        pltpu.VMEM((CORES * quarter, wide), bf16),
        pltpu.VMEM((nz, 2, CORES, quarter, model), bf16),
        pltpu.VMEM((nz, 2, quarter, model), bf16),
        pltpu.VMEM((nz, quarter, bend), bf16),
        pltpu.VMEM((nz, quarter, bend), bf16),
        pltpu.VMEM((nz, quarter, bend), bf16),
        pltpu.VMEM((2, nz, quarter, bend), bf16),
        pltpu.VMEM((nz, 2, quarter, model - bend), bf16),
        pltpu.VMEM((2, nz, 2, quarter, model - bend), bf16),
        pltpu.VMEM((quarter, model - bend), bf16),
        pltpu.VMEM((quarter, model - bend), bf16),
        dma((14,)),
        dma((3,)),
        dma((1,)),
        dma((nz - 1,)),
        dma((1,)),
        dma((nz,)),
        dma((1,)),
        dma((2 * nz - 1,)),
        dma((1,)),
        dma((1,)),
        dma((nz - 1, 3)),
        dma((nz - 1, 3)),
        dma((3,)),
        dma((3,)),
        dma((1,)),
        dma((1,)),
        dma((nz,)),
        dma((nz,)),
        dma((nz, pieces)),
        dma((1,)),
        dma((nz, pieces)),
        dma((1,)),
        dma((nz, 2)),
        dma((1,)),
        dma((nz, 2)),
        dma((1,)),
        dma((nz, 2)),
        dma((1,)),
        dma((2, nz, 2)),
        dma((1,)),
        dma((2, nz)),
        dma((2,)),
    ]
    return pl.pallas_call(
        functools.partial(layer_kernel, nz, ny, heads),
        out_shape=pltpu.VMEM((quarter, model), bf16),
        in_specs=[hbm] * 17,
        out_specs=pl.BlockSpec(memory_space=pltpu.VMEM),
        scratch_shapes=scratch,
        compiler_params=pltpu.CompilerParams(
            collective_id=0, has_side_effects=True, vmem_limit_bytes=64 * 1000 * 1000
        ),
    )(
        q_latent,
        kv_latent,
        rope_key.T,
        doc_ids,
        table,
        q_gain[None, :],
        kv_gain[None, :],
        mix_gain[None, :],
        out_gain[None, :],
        w_query,
        w_key,
        w_value,
        resid_stream,
        w_out,
        w_gate,
        w_up,
        w_down,
    )


def solution(mesh):
    in_specs = (
        P("sp", None),
        P("sp", None),
        P("sp", None),
        P("sp", None),
        P("sp"),
        P(),
        P(),
        P(None, "tp"),
        P(None, "tp"),
        P(None, "tp"),
        P(),
        P(),
        P("sp", "tp"),
        P("sp", "tp"),
        P("tp", "sp"),
        P(),
    )
    out_specs = P(("sp", "tp"), None)
    if mesh.shape["tp"] == 2 * CORES:
        return jax.shard_map(
            functools.partial(fused_layer, mesh.shape["sp"], mesh.shape["tp"]),
            mesh=mesh,
            in_specs=in_specs,
            out_specs=out_specs,
            check_vma=False,
        )
    return jax.shard_map(body, mesh=mesh, in_specs=in_specs, out_specs=out_specs, check_vma=False)
```
